32 devices in a mesh: sp: 16 (over z, y, x), tp: 2 (over core).
Axes of the slice: x: 2, y: 2, z: 4, core: 2. Of those that a mesh axis runs over, the one named last changes fastest.
Arguments:
- tokens: bfloat16 [4096, 2048], P('sp', 'tp'), may hold values from -6 to 6
- norm_gain: float32 [2048], replicated, may hold values from 0.1 to 1.9
- glu_value: bfloat16 [2048, 2048], P('sp', 'tp'), may hold values from -0.125 to 0.125
- glu_gate: bfloat16 [2048, 2048], P('sp', 'tp'), may hold values from -0.125 to 0.125
- conv_taps: float32 [31, 2048], P(None, 'tp'), may hold values from -11 to 11
- ln_gain: float32 [2048], P('tp'), may hold values from 0.1 to 1.9
- ln_bias: float32 [2048], P('tp'), may hold values from -3 to 3
- query_weight: bfloat16 [2048, 2048], P('sp', 'tp'), may hold values from -0.125 to 0.125
- key_weight: bfloat16 [2048, 2048], P('sp', 'tp'), may hold values from -0.125 to 0.125
- value_weight: bfloat16 [2048, 2048], P('sp', 'tp'), may hold values from -0.125 to 0.125
- gate_weight: bfloat16 [2048, 32], replicated, may hold values from -0.125 to 0.125
- gate_bias: float32 [32], replicated, may hold values from -1 to 110
- log_decay_extra: float32 [4096, 16], P('sp'), may hold values from -1.3 to 0
- mem_gain: float32 [2048], P('tp'), may hold values from 0.1 to 1.9
- out_conv: bfloat16 [2048, 2048], P('tp'), may hold values from -0.125 to 0.125
- out_mem: bfloat16 [2048, 2048], P('tp'), may hold values from -0.125 to 0.125
Outputs:
- mixed: bfloat16 [4096, 2048], P(('sp', 'tp'))
The draws below stay inside these ranges and needn't reach their ends.
All inputs are finite; a program needn't handle non-finite values.
Results may differ from the reference program's by a relative error of at most 0.015.
Values may be sent and summed in bfloat16 or wider, within the bound.
A program may use at most 128 MiB of HBM per device.

```python
import math
import jax
import jax.numpy as jnp
from jax import lax

D = 2048
CONV = 2048
MEMORY_HEADS = 8
HEAD = 256
KW = 31
BLOCK = 128
MEM = 2048
SEQUENCE_TOKENS = 4096
N_TP = 2


def draw_conv_taps(key, part):
    base_key, rough_key = jax.random.split(jax.random.fold_in(key, 11))
    base = jnp.clip(jax.random.normal(base_key, (KW, CONV), jnp.float32), -4.0, 4.0)
    rising = 10.0 ** (jnp.arange(CONV, dtype=jnp.float32) / CONV)
    rough = jax.random.uniform(rough_key, (1, CONV), jnp.float32, 0.5, 1.5)
    return base * rising[None, :] * rough * KW ** (-0.5)


def draw_gate_bias(key, part):
    input_key, pick_key, fast_key, slow_key = jax.random.split(jax.random.fold_in(key, 23), 4)
    inputs = jax.random.uniform(input_key, (2, MEMORY_HEADS), jnp.float32, -1.0, 1.0)
    share = 0.5
    fast = jax.random.uniform(pick_key, (2, MEMORY_HEADS), jnp.float32) < share
    fast_bias = jax.random.uniform(fast_key, (2, MEMORY_HEADS), jnp.float32, 3.4, 4.6)
    slow_bias = math.log(SEQUENCE_TOKENS) + 1.0 + jax.random.uniform(slow_key, (2, MEMORY_HEADS), jnp.float32, 0.0, 1.0)
    forget = jnp.where(fast, fast_bias, slow_bias)
    return jnp.stack([inputs[0], forget[0], inputs[1], forget[1]]).reshape(4 * MEMORY_HEADS)


def draw_log_decay_extra(key, part):
    rate_key, place_key, loss_key = jax.random.split(jax.random.fold_in(key, 37), 3)
    blocks = SEQUENCE_TOKENS // BLOCK
    rate_low = 0.25
    rate_high = 1.0
    rates = jnp.exp(jax.random.uniform(rate_key, (blocks, 2 * MEMORY_HEADS), jnp.float32, math.log(rate_low), math.log(rate_high)))
    stable_level = jnp.repeat(rates, BLOCK, axis=0) / SEQUENCE_TOKENS
    slot_places = jax.random.randint(place_key, (3, 2 * MEMORY_HEADS), 0, SEQUENCE_TOKENS)
    loss_values = jax.random.uniform(loss_key, (3, 2 * MEMORY_HEADS), jnp.float32, 0.22, 0.41)
    token_positions = jnp.arange(SEQUENCE_TOKENS, dtype=jnp.int32)[:, None]
    spike_values = jnp.zeros((SEQUENCE_TOKENS, 2 * MEMORY_HEADS), jnp.float32)
    for spike_value in range(3):
        spike_values = spike_values + jnp.where(token_positions == slot_places[spike_value][None, :], loss_values[spike_value][None, :], 0.0)
    return -(stable_level + spike_values)


def level_of(key, extent, cuts, smallest, high):
    gain = 1.0
    for axis_at, blocks in cuts:
        steps = jax.random.uniform(jax.random.fold_in(jax.random.fold_in(key, 6), axis_at), (blocks,), jnp.float32, smallest / len(cuts), high / len(cuts))
        gain = gain * jnp.repeat(jnp.exp(steps), extent[axis_at] // blocks).reshape((-1,) + (1,) * (len(extent) - 1 - axis_at))
    return gain


def gaussian(key, extent, spread, most, cuts=(), kind=jnp.bfloat16):
    array = jax.random.normal(key, extent, jnp.float32) * spread
    if len(cuts) > 0:
        array = level_of(key, extent, cuts, -0.22, 0.18) * array
    return jnp.clip(array, min=-most, max=most).astype(kind)


def setup_inputs(seed: int = 0) -> dict:
    seeds = jax.random.split(jax.random.key(seed), 17)
    return {
        "tokens": gaussian(seeds[0], (SEQUENCE_TOKENS, D), 1.0, 6.0, ((0, 16), (1, 2))),
        "norm_gain": jnp.clip(1.0 + 0.18 * jax.random.normal(seeds[1], (D,), jnp.float32), 0.1, 1.9),
        "glu_value": gaussian(seeds[2], (D, CONV), D ** -0.5, 0.125, ((0, 16), (1, 2))),
        "glu_gate": gaussian(seeds[3], (D, CONV), D ** -0.5, 0.125, ((0, 16), (1, 2))),
        "conv_taps": draw_conv_taps(jax.random.fold_in(seeds[16], 71), 0),
        "ln_gain": jnp.clip(1.0 + 0.18 * jax.random.normal(seeds[5], (CONV,), jnp.float32), 0.1, 1.9),
        "ln_bias": gaussian(seeds[6], (CONV,), 0.5, 3.0, ((0, 2),), jnp.float32),
        "query_weight": gaussian(seeds[7], (D, MEM), D ** -0.5, 0.125, ((0, 16), (1, 2))),
        "key_weight": gaussian(seeds[8], (D, MEM), D ** -0.5, 0.125, ((0, 16), (1, 2))),
        "value_weight": gaussian(seeds[9], (D, MEM), D ** -0.5, 0.125, ((0, 16), (1, 2))),
        "gate_weight": gaussian(seeds[10], (D, 4 * MEMORY_HEADS), D ** -0.5, 0.125),
        "gate_bias": draw_gate_bias(jax.random.fold_in(seeds[16], 71), 0),
        "log_decay_extra": draw_log_decay_extra(jax.random.fold_in(seeds[16], 71), 0),
        "mem_gain": jnp.clip(1.0 + 0.18 * jax.random.normal(seeds[13], (MEM,), jnp.float32), 0.1, 1.9),
        "out_conv": gaussian(seeds[14], (CONV, D), CONV ** -0.5, 0.125, ((0, 2),)),
        "out_mem": gaussian(seeds[15], (MEM, D), MEM ** -0.5, 0.125, ((0, 2),)),
    }


EPS = 1e-06
LOW_START = -1e+30
PRECISE = lax.Precision.HIGHEST

def block_step(carried_state, block_data):
    state_mat, state_vec, stabilizer = carried_state
    queries, key_rows, value_rows, input_gate, log_forget = block_data
    key_scale = HEAD ** (-0.5)
    length = log_forget.shape[-1]
    causal = jnp.tril(jnp.ones((length, length), dtype=bool))
    decay_sum = jnp.cumsum(log_forget, axis=-1)
    log_weight = jnp.where(causal, decay_sum[:, :, None] - decay_sum[:, None, :] + input_gate[:, None, :], -jnp.inf)
    carried = decay_sum + stabilizer[:, None]
    running = jnp.maximum(carried, lax.optimization_barrier(jnp.max(log_weight, axis=-1)))
    inner_weight = jnp.exp(log_weight - running[:, :, None])
    carry_weight = jnp.exp(carried - running)
    raw_scores = jnp.einsum('htd,hsd->hts', queries, key_rows, preferred_element_type=jnp.float32)
    scores = raw_scores * key_scale * inner_weight
    query_wide = queries.astype(jnp.float32)
    numerator = carry_weight[:, :, None] * jnp.einsum('htd,hde->hte', query_wide, state_mat, precision=PRECISE)
    numerator = numerator + jnp.einsum('hts,hse->hte', scores.astype(jnp.bfloat16), value_rows, preferred_element_type=jnp.float32)
    denominator = carry_weight * jnp.einsum('htd,hd->ht', query_wide, state_vec, precision=PRECISE) + lax.optimization_barrier(jnp.sum(scores, axis=-1))
    to_end = decay_sum[:, -1:] - decay_sum + input_gate
    carried_end = decay_sum[:, -1] + stabilizer
    new_stabilizer = jnp.maximum(carried_end, lax.optimization_barrier(jnp.max(to_end, axis=-1)))
    end_weight = jnp.exp(to_end - new_stabilizer[:, None]) * key_scale
    keep_weight = jnp.exp(carried_end - new_stabilizer)
    weighted = key_rows.astype(jnp.float32) * end_weight[:, :, None]
    new_mat = keep_weight[:, None, None] * state_mat + jnp.einsum('hsd,hse->hde', weighted.astype(jnp.bfloat16), value_rows, preferred_element_type=jnp.float32)
    new_vec = keep_weight[:, None] * state_vec + lax.optimization_barrier(jnp.sum(weighted, axis=1))
    return ((new_mat, new_vec, new_stabilizer), (numerator, denominator, running, decay_sum))

def one_direction(queries, key_proj, value_proj, input_gate, log_forget):
    count = SEQUENCE_TOKENS // BLOCK

    def heads_first(tensor):
        return jnp.transpose(tensor.reshape(BLOCK, MEMORY_HEADS, HEAD), (1, 0, 2))

    def step(carried_state, block_data):
        query_blk, key_blk, value_blk, input_blk, forget_blk = block_data
        new_state, results = block_step(carried_state, (heads_first(query_blk), heads_first(key_blk), heads_first(value_blk), input_blk.T, forget_blk.T))
        numerator, denominator, running, _ = results
        return (new_state, numerator / jnp.maximum(jnp.abs(denominator), jnp.exp(-running))[:, :, None])
    start = (jnp.zeros((MEMORY_HEADS, HEAD, HEAD), jnp.float32), jnp.zeros((MEMORY_HEADS, HEAD), jnp.float32), jnp.full((MEMORY_HEADS,), LOW_START, jnp.float32))
    inputs = (queries.reshape(count, BLOCK, MEM), key_proj.reshape(count, BLOCK, MEM), value_proj.reshape(count, BLOCK, MEM), input_gate.reshape(count, BLOCK, MEMORY_HEADS), log_forget.reshape(count, BLOCK, MEMORY_HEADS))
    _, outputs = lax.scan(step, start, inputs)
    return jnp.transpose(outputs, (0, 2, 1, 3)).reshape(SEQUENCE_TOKENS, MEMORY_HEADS, HEAD)

def reference(tokens, norm_gain, glu_value, glu_gate, conv_taps, ln_gain, ln_bias, query_weight, key_weight, value_weight, gate_weight, gate_bias, log_decay_extra, mem_gain, out_conv, out_mem):
    wide = tokens.astype(jnp.float32)
    normed = (wide * lax.rsqrt(lax.optimization_barrier(jnp.mean(wide * wide, axis=-1, keepdims=True)) + EPS) * norm_gain).astype(jnp.bfloat16)
    value_sum = jnp.dot(normed, glu_value, preferred_element_type=jnp.float32)
    gate_sum = jnp.dot(normed, glu_gate, preferred_element_type=jnp.float32)
    glu = (value_sum * jax.nn.sigmoid(gate_sum)).astype(jnp.bfloat16)
    reach = KW // 2
    padded = jnp.pad(glu.astype(jnp.float32), ((reach, reach), (0, 0)))
    conv = jnp.zeros((SEQUENCE_TOKENS, CONV), jnp.float32)
    for offset in range(KW):
        conv = conv + conv_taps[offset] * padded[offset:offset + SEQUENCE_TOKENS]
    chan_mean = lax.optimization_barrier(jnp.mean(conv, axis=-1, keepdims=True))
    chan_var = lax.optimization_barrier(jnp.mean(conv * conv, axis=-1, keepdims=True)) - chan_mean * chan_mean
    normal = (conv - chan_mean) * lax.rsqrt(chan_var + EPS) * ln_gain + ln_bias
    act = (normal * jax.nn.sigmoid(normal)).astype(jnp.bfloat16)
    queries = jnp.dot(normed, query_weight, preferred_element_type=jnp.float32).astype(jnp.bfloat16)
    key_proj = jnp.dot(normed, key_weight, preferred_element_type=jnp.float32).astype(jnp.bfloat16)
    value_proj = jnp.dot(normed, value_weight, preferred_element_type=jnp.float32).astype(jnp.bfloat16)
    gates = (jnp.dot(normed, gate_weight, preferred_element_type=jnp.float32) + gate_bias).reshape(SEQUENCE_TOKENS, 4, MEMORY_HEADS)
    extra = log_decay_extra.reshape(SEQUENCE_TOKENS, 2, MEMORY_HEADS)
    forget_fwd = jax.nn.log_sigmoid(gates[:, 1]) + extra[:, 0]
    forget_bwd = jax.nn.log_sigmoid(gates[:, 3]) + extra[:, 1]
    forward_out = one_direction(queries, key_proj, value_proj, gates[:, 0], forget_fwd)
    backward_out = jnp.flip(one_direction(jnp.flip(queries, 0), jnp.flip(key_proj, 0), jnp.flip(value_proj, 0), jnp.flip(gates[:, 2], 0), jnp.flip(forget_bwd, 0)), 0)
    summed = forward_out + backward_out
    head_norm = summed * lax.rsqrt(lax.optimization_barrier(jnp.mean(summed * summed, axis=-1, keepdims=True)) + EPS)
    memory = (head_norm * mem_gain.reshape(MEMORY_HEADS, HEAD)).reshape(SEQUENCE_TOKENS, MEM).astype(jnp.bfloat16)
    conv_group = CONV // N_TP
    mem_group = MEM // N_TP
    total = jnp.zeros((SEQUENCE_TOKENS, D), jnp.float32)
    for channel_group in range(N_TP):
        conv_cols = act[:, channel_group * conv_group:(channel_group + 1) * conv_group]
        mem_cols = memory[:, channel_group * mem_group:(channel_group + 1) * mem_group]
        partial_sum = jnp.dot(conv_cols, out_conv[channel_group * conv_group:(channel_group + 1) * conv_group], preferred_element_type=jnp.float32)
        partial_sum = partial_sum + jnp.dot(mem_cols, out_mem[channel_group * mem_group:(channel_group + 1) * mem_group], preferred_element_type=jnp.float32)
        total = total + lax.optimization_barrier(partial_sum.astype(jnp.bfloat16)).astype(jnp.float32)
    return total.astype(jnp.bfloat16)
```

```python
import functools
import math
import types

import jax
import jax.numpy as jnp
from jax import lax
from jax.experimental import pallas as pl
from jax.experimental.pallas import tpu as pltpu
from jax.sharding import Mesh, PartitionSpec as P

MEMORY_HEADS = 8
HEAD = 256
KW = 31

EPS = 1e-06
PRECISE = lax.Precision.HIGHEST


def parts_of(x):
    first = lax.reduce_precision(x, 8, 7)
    rest = x - first
    second = lax.reduce_precision(rest, 8, 7)
    third = rest - second
    return [p.astype(jnp.bfloat16) for p in (first, second, third)]


def whole_of(a, b, c):
    return a.astype(jnp.float32) + b.astype(jnp.float32) + c.astype(jnp.float32)


MESH = pl.DeviceIdType.MESH


def layer_kernel(outer, inner, tp, names, *refs):
    r = types.SimpleNamespace(**dict(zip(names, refs)))
    tokens, norm_gain = r.tokens, r.norm_gain
    weights = [r.glu_value, r.glu_gate, r.key_weight, r.value_weight, r.query_weight]
    count = len(weights)
    o, i, t = lax.axis_index("outer"), lax.axis_index("inner"), lax.axis_index("tp")
    block, half = tokens.shape
    depth = weights[0].shape[0]
    hb = block // tp
    quarter = inner * block
    groups = outer // tp
    model = half * tp
    channels = MEMORY_HEADS * HEAD
    scale = HEAD ** (-0.5)
    f32, bf16 = jnp.float32, jnp.bfloat16

    par, grp = lax.rem(o, tp), lax.div(o, tp)
    mate = 1 - t
    twin = o + 1 - 2 * par
    primary = t == par
    place = grp * tp + t
    last = outer - 1
    x, y = lax.rem(i, 2), lax.div(i, 2)
    near = [i, y * 2 + 1 - x, (1 - y) * 2 + x, (1 - y) * 2 + 1 - x]
    head = par * inner + i

    nq, nsrc, xin, wst, wfull, ow = r.nq, r.nsrc, r.xin, r.wst, r.wfull, r.ow

    def span(index, size):
        return pl.ds(pl.multiple_of(index * size, size), size)

    def remote(src, dst, send, recv, device):
        return pltpu.make_async_remote_copy(
            src_ref=src, dst_ref=dst, send_sem=send, recv_sem=recv,
            device_id=device, device_id_type=MESH,
        )

    sends = []

    def start(copy, when=None):
        if when is None:
            copy.start()
        else:
            pl.when(when)(copy.start)
        sends.append((copy, when))

    def guarded(when, action):
        pl.when(when)(action)

    local = pltpu.make_async_copy

    own_rows = [local(weights[j], wst.at[j, o], r.own_s.at[j]) for j in range(count)]
    tok_own = local(tokens.at[span(t, hb), :], xin.at[t], r.loc_s.at[0])
    tok_own.start()

    @pl.when(primary)
    def _():
        for copy in own_rows:
            copy.start()

    gate_in = local(r.gate_weight, r.gwp.at[pl.ds(0, r.gate_weight.shape[0]), :], r.loc_s.at[1])
    out_in = [
        local(source, ow.at[k], r.loc_s.at[2 + k]) for k, source in enumerate((r.out_conv, r.out_mem))
    ]

    barrier = pltpu.get_barrier_semaphore()
    greeted = []
    for dz in range(tp):
        for k in range(inner):
            for c in range(tp):
                if (dz, k, c) != (0, 0, 0):
                    greeted.append((o if dz == 0 else twin, near[k], t if c == 0 else mate))
    for step in range(1, groups):
        away = lax.rem(grp + step, groups) * tp
        for dz in range(tp):
            for c in range(tp):
                greeted.append((away + dz, i, c))
    for device in greeted:
        pl.semaphore_signal(barrier, inc=1, device_id=device, device_id_type=MESH)
    pl.semaphore_wait(barrier, len(greeted))

    start(remote(tokens.at[span(mate, hb), :], xin.at[t], r.xin_s, r.xin_r, (o, i, mate)))

    def spread(j, step):
        target = lax.rem(grp + step, groups) * tp + t
        return remote(
            weights[j], wst.at[j, o], r.w1_s.at[j, step], r.w1_r.at[j, o], (target, i, t)
        )

    def spread_all(j):
        for step in range(groups):
            start(spread(j, step), None if step else jnp.logical_not(primary))

    def arrived(j, plane):
        remote(wst.at[j, plane], wst.at[j, plane], r.w1_s.at[j, 0], r.w1_r.at[j, plane], (o, i, mate)).wait_recv()

    small = ((r.conv_taps, r.taps), (r.ln_gain, r.lng), (r.ln_bias, r.lnb), (r.mem_gain, r.mgn))
    own_small = [
        local(a.at[:, span(i, HEAD)], b, r.sml_s.at[k]) for k, (a, b) in enumerate(small)
    ]
    mate_small = [
        remote(a.at[:, span(i, HEAD)], b, r.prm_s.at[k], r.prm_r.at[k], (o, i, mate))
        for k, (a, b) in enumerate(small)
    ]
    spread_all(0)

    @pl.when(primary)
    def _():
        for copy in own_small:
            copy.start()
        for copy in mate_small:
            copy.start()

    ext = r.ext
    plane = jnp.where(primary, o, twin)
    own_ext = local(r.extra, ext.at[i], r.loc_s.at[4])
    guarded(primary, own_ext.start)
    for k in range(inner):
        copy = remote(r.extra, ext.at[i], r.ext_s.at[k], r.ext_r.at[i], (plane, near[k], par))
        start(copy, None if k else jnp.logical_not(primary))

    gate_in.start()
    for copy in out_in:
        copy.start()

    tok_own.wait()
    remote(xin.at[mate], xin.at[mate], r.xin_s, r.xin_r, (o, i, mate)).wait_recv()
    norm_rows = 32

    def norm_step(m, carry):
        at = span(m, norm_rows)
        parts = [xin[f, at, :].astype(f32) for f in range(tp)]
        square = sum(jnp.sum(p * p, axis=-1, keepdims=True) for p in parts)
        level = lax.rsqrt(square * (1.0 / model) + EPS)
        for f in range(tp):
            row = (parts[f] * level * norm_gain[:, pl.ds(f * half, half)]).astype(bf16)
            nsrc[at, pl.ds(f * half, half)] = row

            @pl.when(primary)
            def _():
                nq[pl.ds(pl.multiple_of(i * block + t * hb + m * norm_rows, norm_rows), norm_rows), pl.ds(f * half, half)] = row
        return carry

    lax.fori_loop(0, hb // norm_rows, norm_step, 0)

    def rows_of(b, c):
        return nq.at[pl.ds(pl.multiple_of(b * block + c * hb, hb), hb), :]

    def tok_wait(b, c):
        remote(rows_of(b, c), rows_of(b, c), r.tok_s.at[0], r.tok_r.at[b, c], (o, i, mate)).wait_recv()

    start(remote(nsrc, rows_of(i, t), r.tok_s.at[0], r.tok_r.at[i, t], (o, i, mate)), jnp.logical_not(primary))
    start(remote(nsrc, rows_of(i, t), r.tok_s.at[1], r.tok_r.at[i, t], (twin, i, par)))

    def row_block(owner_plane, owner):
        return pl.ds(pl.multiple_of((owner_plane * inner + owner) * depth, depth), depth)

    def deal(j, plane_at, k):
        return remote(
            wst.at[j, plane_at, :, span(near[k], HEAD)],
            wfull.at[j, row_block(plane_at, i), :],
            r.w2_s.at[j, plane_at, k - 1], r.w2_r.at[j, plane_at, k - 1], (o, near[k], t),
        )

    def keep(j, plane_at):
        return local(
            wst.at[j, plane_at, :, span(i, HEAD)], wfull.at[j, row_block(plane_at, i), :],
            r.keep_s.at[j, plane_at],
        )

    def plane_of(step):
        return lax.rem(grp + step, groups) * tp

    def deal_planes(j):
        planes = [o, twin]
        for step in range(1, groups):
            planes += [plane_of(step), plane_of(step) + 1]
        return planes

    def deal_all(j, which=None):
        @pl.when(primary)
        def _():
            for index, plane_at in enumerate(deal_planes(j)):
                if which is not None and index not in which:
                    continue
                if index == 0:
                    own_rows[j].wait()
                else:
                    arrived(j, plane_at)
                for k in range(1, inner):
                    deal(j, plane_at, k).start()
                keep(j, plane_at).start()

    def share(j, plane_at):
        rows = pl.ds(pl.multiple_of(plane_at * inner * depth, inner * depth), inner * depth)
        return remote(
            wfull.at[j, rows, :], wfull.at[j, rows, :],
            r.fw_s.at[j, plane_at], r.fw_r.at[j, plane_at], (o, i, mate),
        )

    def collect(j):
        @pl.when(primary)
        def _():
            for plane_at in deal_planes(j):
                keep(j, plane_at).wait()
                for k in range(1, inner):
                    rows = wfull.at[j, row_block(plane_at, near[k]), :]
                    remote(rows, rows, r.w2_s.at[j, plane_at, k - 1], r.w2_r.at[j, plane_at, k - 1], (o, i, mate)).wait_recv()
                share(j, plane_at).start()

        @pl.when(jnp.logical_not(primary))
        def _():
            for plane_at in deal_planes(j):
                share(j, plane_at).wait_recv()

    deal_all(0, (0,))

    def pass_on(b_from, c, k, slot):
        return remote(
            rows_of(b_from, c), rows_of(b_from, c), r.pas_s.at[slot], r.tok_r.at[b_from, c], (o, near[k], t)
        )

    def own_half(c):
        @pl.when(jnp.logical_not(jnp.logical_and(primary, t == c)))
        def _():
            tok_wait(i, c)

    first, second = t, mate
    for index, c in enumerate((first, second)):
        own_half(c)
        start(pass_on(i, c, 1, 2 * index))
        start(pass_on(i, c, 2, 2 * index + 1))
    for j in range(1, count):
        spread_all(j)
    deal_all(0, range(1, outer))
    tok_wait(near[1], 0)
    start(pass_on(near[1], 0, 2, 4))
    tok_wait(near[2], 1)
    start(pass_on(near[2], 1, 1, 5))
    deal_all(1)
    tok_wait(near[1], 1)
    tok_wait(near[2], 0)
    tok_wait(near[3], 0)
    tok_wait(near[3], 1)

    gwp, gt, rowsv, colsv = r.gwp, r.gt, r.rowsv, r.colsv
    gate_in.wait()

    def chunk(n):
        return span(n, block)

    def gate_step(n, carry):
        got = lax.dot_general(
            nq[chunk(n), :], gwp[...], (((1,), (1,)), ((), ())), preferred_element_type=f32
        )
        gt[:, chunk(n)] = got.T[: gt.shape[0]]
        return carry

    lax.fori_loop(0, inner, gate_step, 0)
    guarded(primary, own_ext.wait)
    for k in range(inner):
        def hear(k=k):
            remote(r.extra, ext.at[near[k]], r.ext_s.at[0], r.ext_r.at[near[k]], (o, i, mate)).wait_recv()
        if k:
            hear()
        else:
            guarded(jnp.logical_not(primary), hear)

    mine = lax.broadcasted_iota(jnp.int32, (MEMORY_HEADS, quarter), 0) == head
    mine_block = lax.broadcasted_iota(jnp.int32, (MEMORY_HEADS, block), 0) == head

    def gate_row(g):
        rows = gt[pl.ds(g * MEMORY_HEADS, MEMORY_HEADS), :]
        return jnp.sum(jnp.where(mine, rows, 0.0), axis=0, keepdims=True) + r.gate_bias[g * MEMORY_HEADS + head]

    def extra_row(d):
        pieces = [
            jnp.sum(jnp.where(mine_block, ext[b, pl.ds(d * MEMORY_HEADS, MEMORY_HEADS), :], 0.0), axis=0, keepdims=True)
            for b in range(inner)
        ]
        return jnp.concatenate(pieces, axis=1)

    def log_sigmoid(v):
        return jnp.minimum(v, 0.0) - jnp.log1p(jnp.exp(-jnp.abs(v)))

    within = lax.rem(lax.broadcasted_iota(jnp.int32, (1, quarter), 1), block)

    def scan(v, forward, join, empty):
        step = 1
        while step < block:
            if forward:
                v = join(v, jnp.where(within >= step, pltpu.roll(v, step, 1), empty))
            else:
                v = join(v, jnp.where(within < block - step, pltpu.roll(v, quarter - step, 1), empty))
            step *= 2
        return v

    table = []
    for d in range(2):
        gate_in_row = gate_row(2 * d)
        forget = log_sigmoid(gate_row(2 * d + 1)) + extra_row(d)
        decay = scan(forget, d == 0, jnp.add, 0.0)
        shifted = gate_in_row - decay
        running = scan(shifted, d == 0, jnp.maximum, -jnp.inf)
        table += [shifted, running, decay]
    table += [jnp.zeros((1, quarter), f32)] * 2
    rowsv[...] = jnp.concatenate(table, axis=0)

    def turn_step(n, carry):
        piece = rowsv[:, chunk(n)]
        wide = jnp.concatenate([piece, jnp.zeros((LANES - piece.shape[0], block), f32)], axis=0)
        colsv[chunk(n), :] = wide.T
        return carry

    lax.fori_loop(0, inner, turn_step, 0)

    gpad, conv, hsend, hrecv = r.gpad, r.conv, r.hsend, r.hrecv
    pad = hsend.shape[1]
    reach = KW // 2

    def project(n, j):
        return jnp.dot(nq[chunk(n), :], wfull[j], preferred_element_type=f32)

    collect(0)
    deal_all(2)
    collect(1)

    def glu_step(n, carry):
        glu = (project(n, 0) * jax.nn.sigmoid(project(n, 1))).astype(bf16)
        gpad[pl.ds(pl.multiple_of(n * block + pad, pad), block), :] = glu.astype(f32)

        @pl.when(n == 0)
        def _():
            hsend[0] = glu[:pad]

        @pl.when(n == inner - 1)
        def _():
            hsend[1] = glu[block - pad :]

        return carry

    lax.fori_loop(0, inner, glu_step, 0)
    has_before, has_after = place > 0, place < last

    def device_of(q):
        return (lax.div(q, tp) * tp + par, i, lax.rem(q, tp))

    start(remote(hsend.at[0], hrecv.at[1], r.hal_s.at[0], r.hal_r.at[1], device_of(jnp.maximum(place - 1, 0))), has_before)
    start(remote(hsend.at[1], hrecv.at[0], r.hal_s.at[1], r.hal_r.at[0], device_of(jnp.minimum(place + 1, last))), has_after)
    deal_all(3)

    @pl.when(primary)
    def _():
        for copy in own_small:
            copy.wait()

    @pl.when(jnp.logical_not(primary))
    def _():
        for copy in mate_small:
            copy.wait_recv()

    for side, present, at in ((0, has_before, 0), (1, has_after, pad + quarter)):
        @pl.when(present)
        def _():
            remote(hrecv.at[side], hrecv.at[side], r.hal_s.at[0], r.hal_r.at[side], (o, i, mate)).wait_recv()
            gpad[pl.ds(at, pad), :] = hrecv[side].astype(f32)

        @pl.when(jnp.logical_not(present))
        def _():
            gpad[pl.ds(at, pad), :] = jnp.zeros((pad, HEAD), f32)

    taps, statc, stbuf = r.taps, r.statc, r.stbuf
    conv_rows = 64
    lane = lax.broadcasted_iota(jnp.int32, (conv_rows, LANES), 1)
    shift = pad - reach

    def conv_step(m, carry):
        window = gpad[pl.ds(pl.multiple_of(m * conv_rows, conv_rows), conv_rows + 2 * pad), :]
        total = jnp.zeros((conv_rows, HEAD), f32)
        for residue in range(8):
            moved = window[residue : residue + conv_rows + 2 * pad - 8] if residue else window
            for j in range(KW):
                at = j + shift
                if at % 8 == residue:
                    total = total + taps[pl.ds(j, 1), :] * moved[at - residue : at - residue + conv_rows]
        conv[span(m, conv_rows), :] = total
        s1 = jnp.sum(total, axis=-1, keepdims=True)
        s2 = jnp.sum(total * total, axis=-1, keepdims=True)
        statc[span(m, conv_rows), :] = jnp.where(lane == 0, s1, jnp.where(lane == 1, s2, 0.0))
        return carry

    lax.fori_loop(0, quarter // conv_rows, conv_step, 0)
    sums = r.sums

    def sums_step(n, carry):
        sums[:, chunk(n)] = statc[chunk(n), :].T[: sums.shape[0]]
        return carry

    lax.fori_loop(0, inner, sums_step, 0)
    peers = []
    for dz in range(tp):
        for k in range(inner):
            if (dz, k) != (0, 0):
                peers.append((o if dz == 0 else twin, near[k]))
    for index, (plane_to, chip) in enumerate(peers):
        start(remote(sums, stbuf.at[head], r.sta_s.at[index], r.sta_r.at[head], (plane_to, chip, t)))
    deal_all(4)

    kb, vb, cm, cv = r.kb, r.vb, r.cm, r.cv
    smat, sinfo, matx, infox = r.smat, r.sinfo, r.matx, r.infox

    def key_step(n, carry):
        kb[chunk(n), :] = project(n, 2).astype(bf16)
        return carry

    def state_step(n, carry):
        values = project(n, 3).astype(bf16)
        vb[chunk(n), :] = values
        keys = kb[chunk(n), :].astype(f32)
        cols = colsv[chunk(n), :]
        for d in range(2):
            end = block - 1 if d == 0 else 0
            top = cols[end : end + 1, 3 * d + 1 : 3 * d + 2]
            weighted = keys * (jnp.exp(cols[:, 3 * d : 3 * d + 1] - top) * scale)
            cm[d, n] = lax.dot_general(
                weighted.astype(bf16), values, (((0,), (0,)), ((), ())), preferred_element_type=f32
            )
            cv[d, n] = jnp.broadcast_to(jnp.sum(weighted, axis=0, keepdims=True), (8, HEAD))
        return carry

    collect(2)
    lax.fori_loop(0, inner, key_step, 0)
    collect(3)
    lax.fori_loop(0, inner, state_step, 0)

    def corner(n, d, column):
        end = block - 1 if d == 0 else 0
        at = n * block + end
        return colsv[pl.ds(at, 1), :][:, column : column + 1]

    totals = [[corner(n, d, 3 * d + 2) for n in range(inner)] for d in range(2)]
    levels = [[corner(n, d, 3 * d + 1) + totals[d][n] for n in range(inner)] for d in range(2)]
    for d in range(2):
        reaches = []
        for n in range(inner):
            later = range(n + 1, inner) if d == 0 else range(n)
            value = levels[d][n]
            for m in later:
                value = value + totals[d][m]
            reaches.append(value)
        top = functools.reduce(jnp.maximum, reaches)
        shares = [jnp.exp(v - top) for v in reaches]
        matx[d] = sum(shares[n] * cm[d, n] for n in range(inner)).astype(bf16)
        vec = sum(shares[n] * cv[d, n] for n in range(inner))
        row = lax.broadcasted_iota(jnp.int32, (8, HEAD), 0)
        decay = functools.reduce(jnp.add, totals[d])
        infox[d] = jnp.where(row == 0, vec, jnp.where(row == 1, top, decay))

    for d in range(2):
        for slot in range(outer):
            empty = place <= slot if d == 0 else place >= slot

            @pl.when(empty)
            def _():
                row = lax.broadcasted_iota(jnp.int32, (8, HEAD), 0)
                smat[d, slot] = jnp.zeros((HEAD, HEAD), bf16)
                sinfo[d, slot] = jnp.where(row == 1, LOW_START, 0.0)

    for step in range(1, outer):
        for d in range(2):
            target = place + step if d == 0 else place - step
            present = target <= last if d == 0 else target >= 0
            device = device_of(jnp.clip(target, 0, last))
            start(remote(matx.at[d], smat.at[d, place], r.mat_s.at[d, step - 1], r.mat_r.at[d, place], device), present)
            start(remote(infox.at[d], sinfo.at[d, place], r.inf_s.at[d, step - 1], r.inf_r.at[d, place], device), present)

    for plane_from, chip in peers:
        other = lax.rem(plane_from, tp) * inner + chip
        remote(sums, stbuf.at[other], r.sta_s.at[0], r.sta_r.at[other], (o, i, mate)).wait_recv()
    stbuf[head] = sums[...]

    def stat_step(n, carry):
        whole = stbuf[0, :, chunk(n)]
        for k in range(1, MEMORY_HEADS):
            whole = whole + stbuf[k, :, chunk(n)]
        whole = whole * (1.0 / channels)
        mean = whole[0:1]
        rstd = lax.rsqrt(whole[1:2] - mean * mean + EPS)
        wide = jnp.concatenate([mean, rstd, jnp.zeros((LANES - 2, block), f32)], axis=0)
        statc[chunk(n), :] = wide.T
        return carry

    lax.fori_loop(0, inner, stat_step, 0)
    actb, memb, cin = r.actb, r.memb, r.cin

    def give(which, source, b):
        return remote(
            source.at[chunk(b), :], cin.at[which, i], r.ret_s.at[which, b], r.ret_r.at[which, i],
            (plane, b, par),
        )

    def give_own(which, source):
        return local(source.at[chunk(i), :], cin.at[which, i], r.rel_s.at[which])

    def give_rows(which, source, b):
        to_self = jnp.logical_and(primary, b == i)
        guarded(to_self, give_own(which, source).start)
        guarded(jnp.logical_not(to_self), give(which, source, b).start)

    def act_step(n, carry):
        for half_at in range(2):
            rows = pl.ds(pl.multiple_of(n * block + half_at * (block // 2), block // 2), block // 2)
            cols = statc[rows, :]
            normal = (conv[rows, :] - cols[:, 0:1]) * cols[:, 1:2] * r.lng[...] + r.lnb[...]
            actb[rows, :] = (normal * jax.nn.sigmoid(normal)).astype(bf16)
        give_rows(0, actb, n)
        return carry

    lax.fori_loop(0, inner, act_step, 0)

    for d in range(2):
        for slot in range(outer):
            present = slot < place if d == 0 else slot > place

            @pl.when(present)
            def _():
                remote(matx.at[d], smat.at[d, slot], r.mat_s.at[d, 0], r.mat_r.at[d, slot], (o, i, mate)).wait_recv()
                remote(infox.at[d], sinfo.at[d, slot], r.inf_s.at[d, 0], r.inf_r.at[d, slot], (o, i, mate)).wait_recv()

    chi, clo, nvs, levs = r.chi, r.clo, r.nvs, r.levs
    for d in range(2):
        reaches = []
        for slot in range(outer):
            value = sinfo[d, slot][1:2, 0:1]
            for m in (range(slot + 1, outer) if d == 0 else range(slot)):
                value = value + sinfo[d, m][2:3, 0:1]
            reaches.append(value)
        level = functools.reduce(jnp.maximum, reaches)
        shares = [jnp.exp(v - level) for v in reaches]
        mat = sum(shares[s] * smat[d, s].astype(f32) for s in range(outer))
        vec = sum(shares[s] * sinfo[d, s][0:1] for s in range(outer))
        for n in (range(inner) if d == 0 else range(inner - 1, -1, -1)):
            high = mat.astype(bf16)
            chi[d, n] = high
            clo[d, n] = (mat - high.astype(f32)).astype(bf16)
            nvs[d, n] = jnp.broadcast_to(vec, (8, HEAD))
            levs[d, n] = jnp.broadcast_to(level, (8, LANES))
            carried = level + totals[d][n]
            new_level = jnp.maximum(carried, levels[d][n])
            kept, added = jnp.exp(carried - new_level), jnp.exp(levels[d][n] - new_level)
            mat = kept * mat + added * cm[d, n]
            vec = kept * vec + added * cv[d, n][0:1]
            level = new_level

    acc, pbuf = r.acc, r.pbuf
    tile = 512
    tiles = model // tile

    def own_sender(which):
        return local(actb.at[chunk(i), :], cin.at[which, i], r.rel_s.at[which])

    def take(which):
        for k in range(inner):
            def hear(k=k):
                remote(actb.at[chunk(0), :], cin.at[which, near[k]], r.ret_s.at[which, 0], r.ret_r.at[which, near[k]], (o, i, mate)).wait_recv()
            if k:
                hear()
            else:
                guarded(jnp.logical_not(primary), hear)
                guarded(primary, own_sender(which).wait)

    def part(which, n):
        return sum(
            jnp.dot(cin[which, k], ow[which, pl.ds(k * HEAD, HEAD), span(n, tile)], preferred_element_type=f32)
            for k in range(inner)
        )

    def conv_out_step(n, carry):
        acc[:, span(n, tile)] = part(0, n)
        return carry

    for copy in out_in:
        copy.wait()
    take(0)
    lax.fori_loop(0, tiles, conv_out_step, 0)

    collect(4)
    earlier = lax.broadcasted_iota(jnp.int32, (block, block), 0) >= lax.broadcasted_iota(jnp.int32, (block, block), 1)
    later = lax.broadcasted_iota(jnp.int32, (block, block), 0) <= lax.broadcasted_iota(jnp.int32, (block, block), 1)

    def memory_step(n, carry):
        queries = project(n, 4).astype(bf16)
        wide = queries.astype(f32)
        scores = lax.dot_general(
            queries, kb[chunk(n), :], (((1,), (1,)), ((), ())), preferred_element_type=f32
        ) * scale
        values = vb[chunk(n), :]
        cols = colsv[chunk(n), :]
        rows = rowsv[:, chunk(n)]
        out = jnp.zeros((block, HEAD), f32)
        for d in range(2):
            running, decay = cols[:, 3 * d + 1 : 3 * d + 2], cols[:, 3 * d + 2 : 3 * d + 3]
            level = levs[d, n][0:1, 0:1]
            top = jnp.maximum(running, level)
            carry_weight = jnp.exp(level - top)
            weight = jnp.where(
                earlier if d == 0 else later, jnp.exp(jnp.minimum(rows[3 * d : 3 * d + 1] - top, 0.0)), 0.0
            )
            inner_part = scores * weight
            num = jnp.dot(inner_part.astype(bf16), values, preferred_element_type=f32)
            far = jnp.dot(queries, chi[d, n], preferred_element_type=f32)
            far = far + jnp.dot(queries, clo[d, n], preferred_element_type=f32)
            num = num + carry_weight * far
            den = jnp.sum(inner_part + wide * (carry_weight * nvs[d, n][0:1]), axis=-1, keepdims=True)
            out = out + num / jnp.maximum(jnp.abs(den), jnp.exp(-top - decay))
        level = lax.rsqrt(jnp.mean(out * out, axis=-1, keepdims=True) + EPS)
        memb[chunk(n), :] = (out * level * r.mgn[...]).astype(bf16)
        give_rows(1, memb, n)
        return carry

    lax.fori_loop(0, inner, memory_step, 0)
    take(1)

    out_own, out_mate = r.out_own, r.out_mate

    def piece(n):
        return remote(
            pbuf.at[span(mate, hb), span(n, tile)], out_mate.at[:, span(n, tile)],
            r.fin_s.at[n], r.fin_r.at[n], (o, i, mate),
        )

    def stay(n):
        return local(pbuf.at[span(t, hb), span(n, tile)], out_own.at[:, span(n, tile)], r.fil_s.at[n])

    def mem_out_step(n, carry):
        pbuf[:, span(n, tile)] = (acc[:, span(n, tile)] + part(1, n)).astype(bf16)
        piece(n).start()
        stay(n).start()
        return carry

    lax.fori_loop(0, tiles, mem_out_step, 0)

    for copy, when in sends:
        if when is None:
            copy.wait_send()
        else:
            pl.when(when)(copy.wait_send)

    @pl.when(primary)
    def _():
        for copy in mate_small:
            copy.wait_send()
        for j in range(count):
            for plane_at in deal_planes(j):
                for k in range(1, inner):
                    deal(j, plane_at, k).wait_send()
                share(j, plane_at).wait_send()

    for which, source in ((0, actb), (1, memb)):
        for b in range(inner):
            guarded(jnp.logical_not(jnp.logical_and(primary, i == b)), give(which, source, b).wait_send)
    for n in range(tiles):
        stay(n).wait()
        piece(n).wait()


LANES = 128
LOW_START = -1e30


def whole_layer(outer, inner, tp, args):
    tokens = args.tokens
    block, half = tokens.shape
    depth = args.glu_value.shape[0]
    count = 5
    quarter, model = inner * block, half * tp
    hb = block // tp
    pad = 16
    f32, bf16 = jnp.float32, jnp.bfloat16
    dma = pltpu.SemaphoreType.DMA
    tiles = model // 512
    extra = args.log_decay_extra.T
    operands = dict(
        tokens=tokens, norm_gain=args.norm_gain[None],
        glu_value=args.glu_value, glu_gate=args.glu_gate,
        key_weight=args.key_weight, value_weight=args.value_weight, query_weight=args.query_weight,
        conv_taps=args.conv_taps, ln_gain=args.ln_gain[None], ln_bias=args.ln_bias[None],
        gate_weight=args.gate_weight.T, gate_bias=args.gate_bias,
        extra=extra, mem_gain=args.mem_gain[None],
        out_conv=args.out_conv, out_mem=args.out_mem,
    )
    scratch = dict(
        nq=pltpu.VMEM((quarter, model), bf16),
        nsrc=pltpu.VMEM((hb, model), bf16),
        xin=pltpu.VMEM((tp, hb, half), bf16),
        wst=pltpu.VMEM((count, outer, depth, half), bf16),
        wfull=pltpu.VMEM((count, model, HEAD), bf16),
        ow=pltpu.VMEM((2,) + args.out_conv.shape, bf16),
        taps=pltpu.VMEM((KW, HEAD), f32), lng=pltpu.VMEM((1, HEAD), f32),
        lnb=pltpu.VMEM((1, HEAD), f32), mgn=pltpu.VMEM((1, HEAD), f32),
        ext=pltpu.VMEM((inner,) + extra.shape, f32),
        gwp=pltpu.VMEM((LANES, model), bf16),
        gt=pltpu.VMEM((4 * MEMORY_HEADS, quarter), f32),
        rowsv=pltpu.VMEM((8, quarter), f32), colsv=pltpu.VMEM((quarter, LANES), f32),
        gpad=pltpu.VMEM((quarter + 2 * pad, HEAD), f32), conv=pltpu.VMEM((quarter, HEAD), f32),
        hsend=pltpu.VMEM((2, pad, HEAD), bf16), hrecv=pltpu.VMEM((2, pad, HEAD), bf16),
        statc=pltpu.VMEM((quarter, LANES), f32), sums=pltpu.VMEM((8, quarter), f32),
        stbuf=pltpu.VMEM((MEMORY_HEADS, 8, quarter), f32),
        kb=pltpu.VMEM((quarter, HEAD), bf16), vb=pltpu.VMEM((quarter, HEAD), bf16),
        cm=pltpu.VMEM((2, inner, HEAD, HEAD), f32), cv=pltpu.VMEM((2, inner, 8, HEAD), f32),
        matx=pltpu.VMEM((2, HEAD, HEAD), bf16), infox=pltpu.VMEM((2, 8, HEAD), f32),
        smat=pltpu.VMEM((2, outer, HEAD, HEAD), bf16), sinfo=pltpu.VMEM((2, outer, 8, HEAD), f32),
        chi=pltpu.VMEM((2, inner, HEAD, HEAD), bf16), clo=pltpu.VMEM((2, inner, HEAD, HEAD), bf16),
        nvs=pltpu.VMEM((2, inner, 8, HEAD), f32), levs=pltpu.VMEM((2, inner, 8, LANES), f32),
        actb=pltpu.VMEM((quarter, HEAD), bf16), memb=pltpu.VMEM((quarter, HEAD), bf16),
        cin=pltpu.VMEM((2, inner, block, HEAD), bf16),
        acc=pltpu.VMEM((block, model), f32), pbuf=pltpu.VMEM((block, model), bf16),
        own_s=dma((count,)), loc_s=dma((5,)), xin_s=dma, xin_r=dma,
        w1_s=dma((count, outer // tp)), w1_r=dma((count, outer)),
        sml_s=dma((4,)), prm_s=dma((4,)), prm_r=dma((4,)),
        ext_s=dma((inner,)), ext_r=dma((inner,)),
        tok_s=dma((2,)), tok_r=dma((inner, tp)), pas_s=dma((6,)),
        w2_s=dma((count, outer, inner - 1)), w2_r=dma((count, outer, inner - 1)),
        keep_s=dma((count, outer)), fw_s=dma((count, outer)), fw_r=dma((count, outer)),
        hal_s=dma((2,)), hal_r=dma((2,)),
        sta_s=dma((MEMORY_HEADS,)), sta_r=dma((MEMORY_HEADS,)),
        mat_s=dma((2, outer)), mat_r=dma((2, outer)), inf_s=dma((2, outer)), inf_r=dma((2, outer)),
        ret_s=dma((2, inner)), ret_r=dma((2, inner)), rel_s=dma((2,)),
        fin_s=dma((tiles,)), fin_r=dma((tiles,)), fil_s=dma((tiles,)),
    )
    any_space = pl.BlockSpec(memory_space=pl.ANY)
    spaces = {n: any_space for n in operands}
    spaces.update(
        gate_bias=pl.BlockSpec(memory_space=pltpu.SMEM), norm_gain=pl.BlockSpec(memory_space=pltpu.VMEM)
    )
    names = list(operands) + ["out_own", "out_mate"] + list(scratch)
    shape = jax.ShapeDtypeStruct((hb, model), bf16)
    own, mate = pl.pallas_call(
        functools.partial(layer_kernel, outer, inner, tp, names),
        out_shape=(shape, shape),
        in_specs=[spaces[n] for n in operands],
        out_specs=(any_space, any_space),
        scratch_shapes=list(scratch.values()),
        compiler_params=pltpu.CompilerParams(
            collective_id=0, has_side_effects=True, vmem_limit_bytes=60 * 2**20
        ),
    )(*operands.values())
    return (own.astype(f32) + mate.astype(f32)).astype(bf16)


def gather_inputs(tokens, weights, extra, inner):
    rows, half = tokens.shape
    gathered = lax.all_gather(tokens, ("inner", "tp"), axis=0)
    tp = gathered.shape[0] // inner
    whole = jnp.transpose(gathered.reshape(inner, tp, rows, half), (0, 2, 1, 3))
    whole = whole.reshape(inner * rows, tp * half)
    depth, columns = weights[0].shape
    width = columns // inner
    packed = jnp.stack([w.reshape(depth, inner, width) for w in weights], axis=2)
    packed = jnp.transpose(packed, (1, 0, 2, 3)).reshape(inner, depth, len(weights) * width)
    if inner > 1:
        packed = lax.all_to_all(packed, "inner", split_axis=0, concat_axis=0, tiled=True)
    pieces = lax.all_gather(packed.reshape(inner * depth, -1), "outer", axis=0, tiled=True)
    pieces = pieces.reshape(-1, len(weights), width).transpose(1, 0, 2)
    extras = lax.all_gather(extra, "inner", axis=0, tiled=True) if inner > 1 else extra
    return whole, pieces, extras.T


def local_state(keys, values, shifted, level, total, scale):
    weight = jnp.exp(shifted - level[:, None]) * scale
    weighted = keys.astype(jnp.float32) * weight[:, :, None]
    mat = jnp.einsum(
        "hsd,hse->hde", weighted.astype(jnp.bfloat16), values, preferred_element_type=jnp.float32
    )
    return mat, jnp.sum(weighted, axis=1), level + total, total


def packed_state(mat, vec, level, decay):
    spread = lambda x: jnp.broadcast_to(x[:, None], vec.shape)
    rows = parts_of(vec) + parts_of(spread(level)) + parts_of(spread(decay))
    pad = [jnp.zeros_like(rows[0])] * 7
    return jnp.concatenate([mat.astype(jnp.bfloat16), jnp.stack(rows + pad, axis=1)], axis=1)


def incoming(states, reverse):
    count = states.shape[0]
    mats = states[:, :, :HEAD]
    rows = states[:, :, HEAD:]
    vecs = whole_of(rows[:, :, 0], rows[:, :, 1], rows[:, :, 2])
    levels = whole_of(rows[:, :, 3, 0], rows[:, :, 4, 0], rows[:, :, 5, 0])
    decays = whole_of(rows[:, :, 6, 0], rows[:, :, 7, 0], rows[:, :, 8, 0])
    place = lax.axis_index("outer")
    order = jnp.arange(count)
    if reverse:
        ahead = (order > place)[:, None]
        between = (order[None, :] < order[:, None]) & (order[None, :] > place)
    else:
        ahead = (order < place)[:, None]
        between = (order[None, :] > order[:, None]) & (order[None, :] < place)
    lost = jnp.sum(jnp.where(between[:, :, None], decays[None], 0.0), axis=1)
    reach = jnp.where(ahead, levels + lost, -1e30)
    level = jnp.max(reach, axis=0)
    share = jnp.where(ahead, jnp.exp(reach - level[None]), 0.0)
    mat = jnp.sum(share[:, :, None, None] * mats.astype(jnp.float32), axis=0)
    vec = jnp.sum(share[:, :, None] * vecs, axis=0)
    return mat, vec, level


def finish(query_wide, num, den, running, decay, state):
    mat, vec, level = state
    top = jnp.maximum(running, level[:, None])
    local_weight = jnp.exp(running - top)
    carry_weight = jnp.exp(level[:, None] - top)
    num = local_weight[:, :, None] * num + carry_weight[:, :, None] * jnp.einsum(
        "htd,hde->hte", query_wide, mat, precision=PRECISE
    )
    den = local_weight * den + carry_weight * jnp.einsum(
        "htd,hd->ht", query_wide, vec, precision=PRECISE
    )
    return num / jnp.maximum(jnp.abs(den), jnp.exp(-top - decay))[:, :, None]


def make_shards(inner, outer, tp):
    def own(array, dim):
        size = array.shape[dim] // inner
        return lax.dynamic_slice_in_dim(array, lax.axis_index("inner") * size, size, dim)

    def shards(
        tokens,
        norm_gain,
        glu_value,
        glu_gate,
        conv_taps,
        ln_gain,
        ln_bias,
        query_weight,
        key_weight,
        value_weight,
        gate_weight,
        gate_bias,
        log_decay_extra,
        mem_gain,
        out_conv,
        out_mem,
    ):
        fits = tp == 2 and inner == 4 and outer % tp == 0 and inner * tp == MEMORY_HEADS
        if fits and tokens.shape[1] == inner * HEAD and conv_taps.shape[1] == inner * HEAD:
            return whole_layer(outer, inner, tp, types.SimpleNamespace(
                tokens=tokens, norm_gain=norm_gain, glu_value=glu_value, glu_gate=glu_gate,
                conv_taps=conv_taps, ln_gain=ln_gain, ln_bias=ln_bias, query_weight=query_weight,
                key_weight=key_weight, value_weight=value_weight, gate_weight=gate_weight,
                gate_bias=gate_bias, log_decay_extra=log_decay_extra, mem_gain=mem_gain,
                out_conv=out_conv, out_mem=out_mem,
            ))
        taps, gain, bias, mgain = own(conv_taps, 1), own(ln_gain, 0), own(ln_bias, 0), own(mem_gain, 0)
        channels = conv_taps.shape[1] * tp
        width = gain.shape[0]
        heads = mgain.shape[0] // HEAD
        first = (lax.axis_index("tp") * inner + lax.axis_index("inner")) * heads
        stacked = (query_weight, key_weight, value_weight, glu_value, glu_gate)
        whole, weights, extras = gather_inputs(tokens, stacked, log_decay_extra, inner)
        rows = whole.shape[0]
        wide = whole.astype(jnp.float32)
        normed = (
            wide * lax.rsqrt(jnp.mean(wide * wide, axis=-1, keepdims=True) + EPS) * norm_gain
        ).astype(jnp.bfloat16)
        own_gate = lax.dynamic_slice_in_dim(
            gate_weight.reshape(-1, 4, MEMORY_HEADS), first, heads, 2
        )
        own_bias = lax.dynamic_slice_in_dim(gate_bias.reshape(4, MEMORY_HEADS), first, heads, 1)
        gates = lax.dot_general(
            own_gate.reshape(-1, 4 * heads), normed, (((0,), (1,)), ((), ())),
            preferred_element_type=jnp.float32,
        ).reshape(4, heads, rows) + own_bias[:, :, None]
        own_extra = lax.dynamic_slice_in_dim(
            extras.reshape(2, MEMORY_HEADS, rows), first, heads, 1
        )
        lf = jax.nn.log_sigmoid(gates[1::2]) + own_extra
        at = jnp.arange(rows)
        causal = at[:, None] >= at[None, :]
        anti = at[:, None] <= at[None, :]

        def total(x, mask):
            return jnp.sum(jnp.where(mask, x[:, None, :], 0.0), axis=-1)

        def highest(x, mask):
            return jnp.max(jnp.where(mask, x[:, None, :], -jnp.inf), axis=-1)

        decay_f = total(lf[0], causal)
        decay_b = total(lf[1], anti)
        shifted_f = gates[0] - decay_f
        shifted_b = gates[2] - decay_b
        running_f = highest(shifted_f, causal)
        running_b = highest(shifted_b, anti)

        def project(i):
            return jnp.dot(normed, weights[i], preferred_element_type=jnp.float32)

        def heads_first(x):
            return jnp.transpose(x.reshape(rows, heads, HEAD), (1, 0, 2)).astype(jnp.bfloat16)

        keys = heads_first(project(1))
        values = heads_first(project(2))
        scale = HEAD ** (-0.5)
        state_f = local_state(
            keys, values, shifted_f, running_f[:, -1], decay_f[:, -1], scale
        )
        state_b = local_state(keys, values, shifted_b, running_b[:, 0], decay_b[:, 0], scale)
        sent = jnp.stack([packed_state(*state_f), packed_state(*state_b)])
        states = lax.all_gather(sent, "outer", axis=0)

        glu = (project(3) * jax.nn.sigmoid(project(4))).astype(jnp.bfloat16)
        reach = KW // 2
        before = lax.ppermute(glu[rows - reach :], "outer", [(i, i + 1) for i in range(outer - 1)])
        after = lax.ppermute(glu[:reach], "outer", [(i + 1, i) for i in range(outer - 1)])
        queries = heads_first(project(0))

        scores = jnp.einsum("htd,hsd->hts", queries, keys, preferred_element_type=jnp.float32) * scale

        def local_out(shifted, running, mask):
            weight = jnp.where(
                mask, jnp.exp(jnp.minimum(shifted[:, None, :] - running[:, :, None], 0.0)), 0.0
            )
            part = scores * weight
            num = jnp.einsum(
                "hts,hse->hte", part.astype(jnp.bfloat16), values,
                preferred_element_type=jnp.float32,
            )
            return num, jnp.sum(part, axis=-1)

        num_f, den_f = local_out(shifted_f, running_f, causal)
        num_b, den_b = local_out(shifted_b, running_b, anti)

        padded = jnp.concatenate([before, glu, after], axis=0).astype(jnp.float32)
        conv = jnp.zeros(glu.shape, jnp.float32)
        for offset in range(KW):
            conv = conv + taps[offset] * padded[offset : offset + rows]
        sums = jnp.stack([jnp.sum(conv, axis=-1), jnp.sum(conv * conv, axis=-1)])
        sums = lax.psum(sums, ("inner", "tp")) / channels
        chan_mean = sums[0]
        chan_var = sums[1] - chan_mean * chan_mean
        normal = (conv - chan_mean[:, None]) * lax.rsqrt(chan_var + EPS)[:, None] * gain + bias
        act = (normal * jax.nn.sigmoid(normal)).astype(jnp.bfloat16)

        query_wide = queries.astype(jnp.float32)
        forward = finish(query_wide, num_f, den_f, running_f, decay_f, incoming(states[:, 0], False))
        backward = finish(query_wide, num_b, den_b, running_b, decay_b, incoming(states[:, 1], True))
        summed = forward + backward
        head_norm = summed * lax.rsqrt(jnp.mean(summed * summed, axis=-1, keepdims=True) + EPS)
        head_norm = head_norm * mgain.reshape(heads, HEAD)[:, None, :]
        memory = jnp.transpose(head_norm, (1, 0, 2)).reshape(rows, heads * HEAD).astype(jnp.bfloat16)

        def back(x):
            if inner == 1:
                return x
            return lax.all_to_all(x, "inner", split_axis=0, concat_axis=1, tiled=True)

        result = jnp.dot(back(act), out_conv, preferred_element_type=jnp.float32)
        result = result + jnp.dot(back(memory), out_mem, preferred_element_type=jnp.float32)
        return lax.psum_scatter(
            result.astype(jnp.bfloat16), "tp", scatter_dimension=0, tiled=True
        )

    return shards


def solution(mesh):
    sp, tp = mesh.shape["sp"], mesh.shape["tp"]
    inner = math.gcd(sp, max(MEMORY_HEADS // tp, 1))
    outer = sp // inner
    fine = Mesh(mesh.devices.reshape(outer, inner, tp), ("outer", "inner", "tp"))
    rows = ("outer", "inner")
    in_specs = (
        P(rows, "tp"),
        P(),
        P(rows, "tp"),
        P(rows, "tp"),
        P(None, "tp"),
        P("tp"),
        P("tp"),
        P(rows, "tp"),
        P(rows, "tp"),
        P(rows, "tp"),
        P(),
        P(),
        P(rows, None),
        P("tp"),
        P("tp", None),
        P("tp", None),
    )
    return jax.shard_map(
        make_shards(inner, outer, tp), mesh=fine, in_specs=in_specs,
        out_specs=P(("outer", "inner", "tp"), None), check_vma=False,
    )
```

```python
import functools
import math
import types

import jax
import jax.numpy as jnp
from jax import lax
from jax.experimental import pallas as pl
from jax.experimental.pallas import tpu as pltpu
from jax.sharding import Mesh, PartitionSpec as P

MEMORY_HEADS = 8
HEAD = 256
KW = 31

EPS = 1e-06
PRECISE = lax.Precision.HIGHEST


def parts_of(x):
    first = lax.reduce_precision(x, 8, 7)
    rest = x - first
    second = lax.reduce_precision(rest, 8, 7)
    third = rest - second
    return [p.astype(jnp.bfloat16) for p in (first, second, third)]


def whole_of(a, b, c):
    return a.astype(jnp.float32) + b.astype(jnp.float32) + c.astype(jnp.float32)


MESH = pl.DeviceIdType.MESH


def layer_kernel(outer, inner, tp, names, *refs):
    r = types.SimpleNamespace(**dict(zip(names, refs)))
    tokens, norm_gain = r.tokens, r.norm_gain
    weights = [r.key_weight, r.value_weight, r.glu_value, r.glu_gate, r.query_weight]
    count = len(weights)
    o, i, t = lax.axis_index("outer"), lax.axis_index("inner"), lax.axis_index("tp")
    block, half = tokens.shape
    depth = weights[0].shape[0]
    hb = block // tp
    quarter = inner * block
    groups = outer // tp
    model = half * tp
    channels = MEMORY_HEADS * HEAD
    scale = HEAD ** (-0.5)
    f32, bf16 = jnp.float32, jnp.bfloat16

    par, grp = lax.rem(o, tp), lax.div(o, tp)
    mate = 1 - t
    twin = o + 1 - 2 * par
    primary = t == par
    place = grp * tp + t
    last = outer - 1
    x, y = lax.rem(i, 2), lax.div(i, 2)
    near = [i, y * 2 + 1 - x, (1 - y) * 2 + x, (1 - y) * 2 + 1 - x]
    head = par * inner + i

    nq, nsrc, xin, wst, wfull, ow = r.nq, r.nsrc, r.xin, r.wst, r.wfull, r.ow

    def span(index, size):
        return pl.ds(pl.multiple_of(index * size, size), size)

    def remote(src, dst, send, recv, device):
        return pltpu.make_async_remote_copy(
            src_ref=src, dst_ref=dst, send_sem=send, recv_sem=recv,
            device_id=device, device_id_type=MESH,
        )

    sends = []

    def start(copy, when=None):
        if when is None:
            copy.start()
        else:
            pl.when(when)(copy.start)
        sends.append((copy, when))

    def guarded(when, action):
        pl.when(when)(action)

    local = pltpu.make_async_copy

    own_rows = [local(weights[j], wst.at[j, o], r.own_s.at[j]) for j in range(count)]
    tok_own = local(tokens.at[span(t, hb), :], xin.at[t], r.loc_s.at[0])
    tok_own.start()

    for copy in own_rows:
        copy.start()

    gate_in = local(r.gate_weight, r.gwp.at[pl.ds(0, r.gate_weight.shape[0]), :], r.loc_s.at[1])
    out_in = [
        local(source, ow.at[k], r.loc_s.at[2 + k]) for k, source in enumerate((r.out_conv, r.out_mem))
    ]

    barrier = pltpu.get_barrier_semaphore()
    greeted = []
    for dz in range(tp):
        for k in range(inner):
            for c in range(tp):
                if (dz, k, c) != (0, 0, 0):
                    greeted.append((o if dz == 0 else twin, near[k], t if c == 0 else mate))
    for step in range(1, groups):
        away = lax.rem(grp + step, groups) * tp
        for dz in range(tp):
            for c in range(tp):
                greeted.append((away + dz, i, c))
    for device in greeted:
        pl.semaphore_signal(barrier, inc=1, device_id=device, device_id_type=MESH)
    pl.semaphore_wait(barrier, len(greeted))

    start(remote(tokens.at[span(mate, hb), :], xin.at[t], r.xin_s, r.xin_r, (o, i, mate)))

    def spread(j, step):
        target = lax.rem(grp + step, groups) * tp + t
        return remote(
            wst.at[j, o], wst.at[j, o], r.w1_s.at[j, step], r.w1_r.at[j, o], (target, i, t)
        )

    moved = (1, 3)

    def plane_of(step):
        return lax.rem(grp + step, groups) * tp

    def hand_over(j):
        at = moved.index(j)
        return remote(wst.at[j, o], r.wmv.at[at], r.mov_s.at[at], r.mov_r.at[at], (o, i, mate))

    def spread_all(j, phase):
        for step in range(groups):
            target = lax.rem(grp + step, groups) * tp + t
            apart = (target - o) * (twin - o) < 0
            if phase == 0:
                when = jnp.logical_and(apart, jnp.logical_not(primary))
            elif phase == 1:
                when = jnp.logical_not(apart)
                if step == 0:
                    when = jnp.logical_and(when, jnp.logical_not(primary))
            else:
                when = jnp.logical_and(apart, primary)
            if step and phase == 1 and j in moved:
                start(spread(j, step), jnp.logical_and(when, primary))
                other = plane_of(step) + mate
                at_end = jnp.logical_and(primary, (other - o) * (twin - o) > 0)

                @pl.when(at_end)
                def _():
                    hand_over(j).wait_recv()

                start(remote(
                    r.wmv.at[moved.index(j)], wst.at[j, o], r.mvd_s.at[moved.index(j)], r.w1_r.at[j, o], (other, i, mate)
                ), at_end)
            elif step or phase == 1:
                start(spread(j, step), when)

    def arrived(j, plane):
        remote(wst.at[j, plane], wst.at[j, plane], r.w1_s.at[j, 0], r.w1_r.at[j, plane], (o, i, mate)).wait_recv()

    small = ((r.conv_taps, r.taps), (r.ln_gain, r.lng), (r.ln_bias, r.lnb), (r.mem_gain, r.mgn))
    own_small = [
        local(a.at[:, span(i, HEAD)], b, r.sml_s.at[k]) for k, (a, b) in enumerate(small)
    ]
    mate_small = [
        remote(a.at[:, span(i, HEAD)], b, r.prm_s.at[k], r.prm_r.at[k], (o, i, mate))
        for k, (a, b) in enumerate(small)
    ]
    for j in range(count):
        own_rows[j].wait()
        spread_all(j, 0)
        if j in moved:
            at_end = (plane_of(1) + t - o) * (twin - o) > 0
            start(hand_over(j), jnp.logical_and(jnp.logical_not(primary), at_end))

    @pl.when(primary)
    def _():
        for copy in own_small:
            copy.start()
        for copy in mate_small:
            copy.start()

    ext = r.ext
    plane = jnp.where(primary, o, twin)
    own_ext = local(r.extra, ext.at[i], r.loc_s.at[4])
    guarded(primary, own_ext.start)
    for k in range(inner):
        copy = remote(r.extra, ext.at[i], r.ext_s.at[k], r.ext_r.at[i], (plane, near[k], par))
        start(copy, None if k else jnp.logical_not(primary))

    gate_in.start()
    for copy in out_in:
        copy.start()

    tok_own.wait()
    remote(xin.at[mate], xin.at[mate], r.xin_s, r.xin_r, (o, i, mate)).wait_recv()
    norm_rows = 32
    pieces = 2
    piece_rows = hb // pieces

    def norm_step(m, carry):
        at = span(m, norm_rows)
        parts = [xin[f, at, :].astype(f32) for f in range(tp)]
        square = sum(jnp.sum(p * p, axis=-1, keepdims=True) for p in parts)
        level = lax.rsqrt(square * (1.0 / model) + EPS)
        for f in range(tp):
            row = (parts[f] * level * norm_gain[:, pl.ds(f * half, half)]).astype(bf16)
            nsrc[at, pl.ds(f * half, half)] = row

            @pl.when(primary)
            def _():
                nq[pl.ds(pl.multiple_of(i * block + t * hb + m * norm_rows, norm_rows), norm_rows), pl.ds(f * half, half)] = row
        return carry

    def rows_of(b, c, s):
        return nq.at[pl.ds(pl.multiple_of(b * block + c * hb + s * piece_rows, piece_rows), piece_rows), :]

    def tok_wait(b, c, s):
        rows = rows_of(b, c, s)
        remote(rows, rows, r.tok_s.at[0, 0], r.tok_r.at[b, c, s], (o, i, mate)).wait_recv()

    steps = piece_rows // norm_rows
    for s in range(pieces):
        lax.fori_loop(s * steps, (s + 1) * steps, norm_step, 0)
        source = nsrc.at[pl.ds(s * piece_rows, piece_rows), :]
        start(remote(source, rows_of(i, t, s), r.tok_s.at[1, s], r.tok_r.at[i, t, s], (twin, i, par)))
        start(remote(source, rows_of(i, t, s), r.tok_s.at[0, s], r.tok_r.at[i, t, s], (o, i, mate)), jnp.logical_not(primary))
    for j in range(count):
        spread_all(j, 1)

    def row_block(owner_plane, owner):
        return pl.ds(pl.multiple_of((owner_plane * inner + owner) * depth, depth), depth)

    def deal(j, plane_at, k):
        return remote(
            wst.at[j, plane_at, :, span(near[k], HEAD)],
            wfull.at[j, row_block(plane_at, i), :],
            r.w2_s.at[j, plane_at, k - 1], r.w2_r.at[j, plane_at, k - 1], (o, near[k], t),
        )

    def keep(j, plane_at):
        return local(
            wst.at[j, plane_at, :, span(i, HEAD)], wfull.at[j, row_block(plane_at, i), :],
            r.keep_s.at[j, plane_at],
        )

    def deal_planes(j):
        bases = [plane_of(step) for step in range(1, groups)]
        nearer = [base + jnp.where(base < o, 1, 0) for base in bases]
        farther = [base + jnp.where(base < o, 0, 1) for base in bases]
        return [o] + nearer + [twin] + farther

    def deal_all(j, which=None):
        @pl.when(primary)
        def _():
            for index, plane_at in enumerate(deal_planes(j)):
                if which is not None and index not in which:
                    continue
                if index:
                    arrived(j, plane_at)
                for k in range(1, inner):
                    deal(j, plane_at, k).start()
                keep(j, plane_at).start()

    def share(j, plane_at):
        rows = pl.ds(pl.multiple_of(plane_at * inner * depth, inner * depth), inner * depth)
        return remote(
            wfull.at[j, rows, :], wfull.at[j, rows, :],
            r.fw_s.at[j, plane_at], r.fw_r.at[j, plane_at], (o, i, mate),
        )

    def collect(j):
        @pl.when(primary)
        def _():
            for plane_at in deal_planes(j):
                keep(j, plane_at).wait()
                for k in range(1, inner):
                    rows = wfull.at[j, row_block(plane_at, near[k]), :]
                    remote(rows, rows, r.w2_s.at[j, plane_at, k - 1], r.w2_r.at[j, plane_at, k - 1], (o, i, mate)).wait_recv()
                share(j, plane_at).start()

        @pl.when(jnp.logical_not(primary))
        def _():
            for plane_at in deal_planes(j):
                share(j, plane_at).wait_recv()

    def pass_on(b_from, c, s, k, slot):
        rows = rows_of(b_from, c, s)
        return remote(rows, rows, r.pas_s.at[slot, s], r.tok_r.at[b_from, c, s], (o, near[k], t))

    @pl.when(primary)
    def _():
        for s in range(pieces):
            for c, slot in ((t, 0), (mate, 2)):
                if slot:
                    tok_wait(i, c, s)
                pass_on(i, c, s, 1, slot).start()
                pass_on(i, c, s, 2, slot + 1).start()

    @pl.when(jnp.logical_not(primary))
    def _():
        for s in range(pieces):
            for c, slot in ((t, 0), (mate, 2)):
                tok_wait(i, c, s)
                pass_on(i, c, s, 1, slot).start()
                pass_on(i, c, s, 2, slot + 1).start()

    for s in range(pieces):
        tok_wait(near[1], 0, s)
        start(pass_on(near[1], 0, s, 2, 4))
        tok_wait(near[2], 1, s)
        start(pass_on(near[2], 1, s, 1, 5))
    for j in range(count):
        spread_all(j, 2)
    for s in range(pieces):
        tok_wait(near[1], 1, s)
        tok_wait(near[2], 0, s)
        tok_wait(near[3], 0, s)
        tok_wait(near[3], 1, s)

    deal_all(0)
    deal_all(1)

    gwp, gt, rowsv, colsv = r.gwp, r.gt, r.rowsv, r.colsv
    gate_in.wait()

    def chunk(n):
        return span(n, block)

    def gate_step(n, carry):
        got = lax.dot_general(
            nq[chunk(n), :], gwp[...], (((1,), (1,)), ((), ())), preferred_element_type=f32
        )
        gt[:, chunk(n)] = got.T[: gt.shape[0]]
        return carry

    lax.fori_loop(0, inner, gate_step, 0)
    guarded(primary, own_ext.wait)
    for k in range(inner):
        def hear(k=k):
            remote(r.extra, ext.at[near[k]], r.ext_s.at[0], r.ext_r.at[near[k]], (o, i, mate)).wait_recv()
        if k:
            hear()
        else:
            guarded(jnp.logical_not(primary), hear)

    mine = lax.broadcasted_iota(jnp.int32, (MEMORY_HEADS, quarter), 0) == head
    mine_block = lax.broadcasted_iota(jnp.int32, (MEMORY_HEADS, block), 0) == head

    def gate_row(g):
        rows = gt[pl.ds(g * MEMORY_HEADS, MEMORY_HEADS), :]
        return jnp.sum(jnp.where(mine, rows, 0.0), axis=0, keepdims=True) + r.gate_bias[g * MEMORY_HEADS + head]

    def extra_row(d):
        pieces = [
            jnp.sum(jnp.where(mine_block, ext[b, pl.ds(d * MEMORY_HEADS, MEMORY_HEADS), :], 0.0), axis=0, keepdims=True)
            for b in range(inner)
        ]
        return jnp.concatenate(pieces, axis=1)

    def log_sigmoid(v):
        return jnp.minimum(v, 0.0) - jnp.log1p(jnp.exp(-jnp.abs(v)))

    within = lax.rem(lax.broadcasted_iota(jnp.int32, (1, quarter), 1), block)

    def scan(v, forward, join, empty):
        step = 1
        while step < block:
            if forward:
                v = join(v, jnp.where(within >= step, pltpu.roll(v, step, 1), empty))
            else:
                v = join(v, jnp.where(within < block - step, pltpu.roll(v, quarter - step, 1), empty))
            step *= 2
        return v

    table = []
    for d in range(2):
        gate_in_row = gate_row(2 * d)
        forget = log_sigmoid(gate_row(2 * d + 1)) + extra_row(d)
        decay = scan(forget, d == 0, jnp.add, 0.0)
        shifted = gate_in_row - decay
        running = scan(shifted, d == 0, jnp.maximum, -jnp.inf)
        table += [shifted, running, decay]
    table += [jnp.zeros((1, quarter), f32)] * 2
    rowsv[...] = jnp.concatenate(table, axis=0)

    def turn_step(n, carry):
        piece = rowsv[:, chunk(n)]
        wide = jnp.concatenate([piece, jnp.zeros((LANES - piece.shape[0], block), f32)], axis=0)
        colsv[chunk(n), :] = wide.T
        return carry

    lax.fori_loop(0, inner, turn_step, 0)

    def project(n, j):
        return jnp.dot(nq[chunk(n), :], wfull[j], preferred_element_type=f32)

    kb, vb, cm, cv = r.kb, r.vb, r.cm, r.cv
    smat, sinfo, matx, infox = r.smat, r.sinfo, r.matx, r.infox
    gmat, ginfo, gin, gininfo = r.gmat, r.ginfo, r.gin, r.gininfo

    def key_step(n, carry):
        kb[chunk(n), :] = project(n, 0).astype(bf16)
        return carry

    def state_step(n, carry):
        values = project(n, 1).astype(bf16)
        vb[chunk(n), :] = values
        keys = kb[chunk(n), :].astype(f32)
        cols = colsv[chunk(n), :]
        for d in range(2):
            end = block - 1 if d == 0 else 0
            top = cols[end : end + 1, 3 * d + 1 : 3 * d + 2]
            weighted = keys * (jnp.exp(cols[:, 3 * d : 3 * d + 1] - top) * scale)
            cm[d, n] = lax.dot_general(
                weighted.astype(bf16), values, (((0,), (0,)), ((), ())), preferred_element_type=f32
            )
            cv[d, n] = jnp.broadcast_to(jnp.sum(weighted, axis=0, keepdims=True), (8, HEAD))
        return carry

    collect(0)
    lax.fori_loop(0, inner, key_step, 0)
    deal_all(2)
    collect(1)
    lax.fori_loop(0, inner, state_step, 0)

    def corner(n, d, column):
        end = block - 1 if d == 0 else 0
        at = n * block + end
        return colsv[pl.ds(at, 1), :][:, column : column + 1]

    def device_of(q):
        return (lax.div(q, tp) * tp + par, i, lax.rem(q, tp))

    totals = [[corner(n, d, 3 * d + 2) for n in range(inner)] for d in range(2)]
    levels = [[corner(n, d, 3 * d + 1) + totals[d][n] for n in range(inner)] for d in range(2)]
    for d in range(2):
        reaches = []
        for n in range(inner):
            later = range(n + 1, inner) if d == 0 else range(n)
            value = levels[d][n]
            for m in later:
                value = value + totals[d][m]
            reaches.append(value)
        top = functools.reduce(jnp.maximum, reaches)
        shares = [jnp.exp(v - top) for v in reaches]
        matx[d] = sum(shares[n] * cm[d, n] for n in range(inner)).astype(bf16)
        vec = sum(shares[n] * cv[d, n] for n in range(inner))
        row = lax.broadcasted_iota(jnp.int32, (8, HEAD), 0)
        decay = functools.reduce(jnp.add, totals[d])
        infox[d] = jnp.where(row == 0, vec, jnp.where(row == 1, top, decay))

    start(remote(matx, smat, r.mat_s.at[0], r.mat_r.at[0], (o, i, mate)))
    start(remote(infox, sinfo, r.inf_s.at[0], r.inf_r.at[0], (o, i, mate)))
    gpad, conv, hsend, hrecv = r.gpad, r.conv, r.hsend, r.hrecv
    pad = hsend.shape[1]
    reach = KW // 2
    sides = HEAD // LANES

    def value_step(n, carry):
        r.gval[chunk(n), :] = project(n, 2)
        return carry

    deal_all(3, range(2))
    mat_rows = gin.at[span(t, HEAD // tp), :]
    mate_rows = gin.at[span(mate, HEAD // tp), :]
    remote(matx, smat, r.mat_s.at[0], r.mat_r.at[0], (o, i, mate)).wait_recv()
    remote(infox, sinfo, r.inf_s.at[0], r.inf_r.at[0], (o, i, mate)).wait_recv()
    ours, theirs = infox[grp], sinfo[grp]
    is_far = t == grp
    our_reach = ours[1:2, 0:1] + jnp.where(is_far, theirs[2:3, 0:1], 0.0)
    their_reach = theirs[1:2, 0:1] + jnp.where(is_far, 0.0, ours[2:3, 0:1])
    group_level = jnp.maximum(our_reach, their_reach)
    our_share, their_share = jnp.exp(our_reach - group_level), jnp.exp(their_reach - group_level)
    gmat[...] = (our_share * matx[grp].astype(f32) + their_share * smat[grp].astype(f32)).astype(bf16)
    state_row = lax.broadcasted_iota(jnp.int32, (8, HEAD), 0)
    ginfo[...] = jnp.where(state_row == 0, our_share * ours[0:1] + their_share * theirs[0:1], group_level)
    across = ((1 - grp) * tp + par, i, t)
    start(remote(gmat.at[span(t, HEAD // tp), :], mat_rows, r.mat_s.at[1], r.mat_r.at[1], across))
    start(remote(ginfo, gininfo, r.inf_s.at[1], r.inf_r.at[1], across))
    collect(2)
    lax.fori_loop(0, inner, value_step, 0)
    deal_all(3, range(2, outer))
    deal_all(4, range(2))
    collect(3)

    def glu_step(n, carry):
        glu = (r.gval[chunk(n), :] * jax.nn.sigmoid(project(n, 3))).astype(bf16)
        for side in range(sides):
            gpad[side, pl.ds(pl.multiple_of(n * block + pad, pad), block), :] = glu[:, side * LANES : (side + 1) * LANES].astype(f32)

        @pl.when(n == 0)
        def _():
            hsend[0] = glu[:pad]

        @pl.when(n == inner - 1)
        def _():
            hsend[1] = glu[block - pad :]

        return carry

    lax.fori_loop(0, inner, glu_step, 0)
    has_before, has_after = place > 0, place < last
    start(remote(hsend.at[0], hrecv.at[1], r.hal_s.at[0], r.hal_r.at[1], device_of(jnp.maximum(place - 1, 0))), has_before)
    start(remote(hsend.at[1], hrecv.at[0], r.hal_s.at[1], r.hal_r.at[0], device_of(jnp.minimum(place + 1, last))), has_after)

    deal_all(4, (2,))

    @pl.when(primary)
    def _():
        for copy in own_small:
            copy.wait()

    @pl.when(jnp.logical_not(primary))
    def _():
        for copy in mate_small:
            copy.wait_recv()

    for edge, present, at in ((0, has_before, 0), (1, has_after, pad + quarter)):
        @pl.when(present)
        def _():
            remote(hrecv.at[edge], hrecv.at[edge], r.hal_s.at[0], r.hal_r.at[edge], (o, i, mate)).wait_recv()
            for side in range(sides):
                gpad[side, pl.ds(at, pad), :] = hrecv[edge, :, side * LANES : (side + 1) * LANES].astype(f32)

        @pl.when(jnp.logical_not(present))
        def _():
            for side in range(sides):
                gpad[side, pl.ds(at, pad), :] = jnp.zeros((pad, LANES), f32)

    taps, statc, stbuf = r.taps, r.statc, r.stbuf
    conv_rows = 64
    lane = lax.broadcasted_iota(jnp.int32, (conv_rows, LANES), 1)
    shift = pad - reach

    def conv_step(m, carry):
        s1 = s2 = 0.0
        for side in range(sides):
            total = jnp.zeros((conv_rows, LANES), f32)
            for j in range(KW):
                rows = gpad[side, pl.ds(m * conv_rows + (j + shift), conv_rows), :]
                total = total + taps[pl.ds(j, 1), pl.ds(side * LANES, LANES)] * rows
            conv[side, span(m, conv_rows), :] = total
            s1 = s1 + total
            s2 = s2 + total * total
        s1 = jnp.sum(s1, axis=-1, keepdims=True)
        s2 = jnp.sum(s2, axis=-1, keepdims=True)
        statc[span(m, conv_rows), :] = jnp.where(lane == 0, s1, jnp.where(lane == 1, s2, 0.0))
        return carry

    lax.fori_loop(0, quarter // conv_rows, conv_step, 0)
    deal_all(4, range(3, outer))
    sums = r.sums

    def sums_step(n, carry):
        sums[:, chunk(n)] = statc[chunk(n), :].T[: sums.shape[0]]
        return carry

    lax.fori_loop(0, inner, sums_step, 0)
    peers = []
    for dz in range(tp):
        for k in range(inner):
            if (dz, k) != (0, 0):
                peers.append((o if dz == 0 else twin, near[k]))
    for index, (plane_to, chip) in enumerate(peers):
        start(remote(sums, stbuf.at[head], r.sta_s.at[index], r.sta_r.at[head], (plane_to, chip, t)))
    remote(mat_rows, mat_rows, r.mat_s.at[1], r.mat_r.at[1], (o, i, mate)).wait_recv()
    start(remote(mat_rows, mat_rows, r.mat_s.at[2], r.mat_r.at[2], (o, i, mate)))
    remote(ginfo, gininfo, r.inf_s.at[1], r.inf_r.at[1], (o, i, mate)).wait_recv()
    remote(mate_rows, mate_rows, r.mat_s.at[2], r.mat_r.at[2], (o, i, mate)).wait_recv()

    chi, clo, nvs, levs = r.chi, r.clo, r.nvs, r.levs
    for d in range(2):
        by_mate, by_group = t == 1 - d, grp == 1 - d
        near_reach = jnp.where(by_mate, sinfo[d][1:2, 0:1], LOW_START)
        far_reach = gininfo[1:2, 0:1] + jnp.where(by_mate, sinfo[d][2:3, 0:1], 0.0)
        far_reach = jnp.where(by_group, far_reach, LOW_START)
        level = jnp.maximum(near_reach, far_reach)
        near_share = jnp.where(by_mate, jnp.exp(near_reach - level), 0.0)
        far_share = jnp.where(by_group, jnp.exp(far_reach - level), 0.0)
        mat = near_share * smat[d].astype(f32) + far_share * gin[...].astype(f32)
        vec = near_share * sinfo[d][0:1] + far_share * gininfo[0:1]
        for n in (range(inner) if d == 0 else range(inner - 1, -1, -1)):
            high = mat.astype(bf16)
            chi[d, n] = high
            clo[d, n] = (mat - high.astype(f32)).astype(bf16)
            nvs[d, n] = jnp.broadcast_to(vec, (8, HEAD))
            levs[d, n] = jnp.broadcast_to(level, (8, LANES))
            carried = level + totals[d][n]
            new_level = jnp.maximum(carried, levels[d][n])
            kept, added = jnp.exp(carried - new_level), jnp.exp(levels[d][n] - new_level)
            mat = kept * mat + added * cm[d, n]
            vec = kept * vec + added * cv[d, n][0:1]
            level = new_level

    earlier = lax.broadcasted_iota(jnp.int32, (block, block), 0) >= lax.broadcasted_iota(jnp.int32, (block, block), 1)
    later = lax.broadcasted_iota(jnp.int32, (block, block), 0) <= lax.broadcasted_iota(jnp.int32, (block, block), 1)
    lane_at = lax.broadcasted_iota(jnp.int32, (block, LANES), 1)

    def weight_step(n, carry):
        cols = colsv[chunk(n), :]
        rows = rowsv[:, chunk(n)]
        kept = jnp.zeros((block, LANES), f32)
        for d in range(2):
            running, decay = cols[:, 3 * d + 1 : 3 * d + 2], cols[:, 3 * d + 2 : 3 * d + 3]
            level = levs[d, n][0:1, 0:1]
            top = jnp.maximum(running, level)
            r.wgt[d, n] = jnp.where(
                earlier if d == 0 else later,
                jnp.exp(jnp.minimum(rows[3 * d : 3 * d + 1] - top, 0.0)) * scale, 0.0,
            )
            kept = jnp.where(lane_at == 2 * d, jnp.exp(level - top), kept)
            kept = jnp.where(lane_at == 2 * d + 1, jnp.exp(-top - decay), kept)
        r.colw[chunk(n), :] = kept
        return carry

    lax.fori_loop(0, inner, weight_step, 0)
    collect(4)
    for plane_from, chip in peers:
        other = lax.rem(plane_from, tp) * inner + chip
        remote(sums, stbuf.at[other], r.sta_s.at[0], r.sta_r.at[other], (o, i, mate)).wait_recv()
    stbuf[head] = sums[...]

    def stat_step(n, carry):
        whole = stbuf[0, :, chunk(n)]
        for k in range(1, MEMORY_HEADS):
            whole = whole + stbuf[k, :, chunk(n)]
        whole = whole * (1.0 / channels)
        mean = whole[0:1]
        rstd = lax.rsqrt(whole[1:2] - mean * mean + EPS)
        wide = jnp.concatenate([mean, rstd, jnp.zeros((LANES - 2, block), f32)], axis=0)
        statc[chunk(n), :] = wide.T
        return carry

    lax.fori_loop(0, inner, stat_step, 0)
    actb, memb, cin = r.actb, r.memb, r.cin

    def give(which, source, b):
        return remote(
            source.at[chunk(b), :], cin.at[which, i], r.ret_s.at[which, b], r.ret_r.at[which, i],
            (plane, b, par),
        )

    def give_own(which, source):
        return local(source.at[chunk(i), :], cin.at[which, i], r.rel_s.at[which])

    def give_rows(which, source, b):
        to_self = jnp.logical_and(primary, b == i)
        guarded(to_self, give_own(which, source).start)
        guarded(jnp.logical_not(to_self), give(which, source, b).start)

    def turn(step):
        k = inner - 1 - step
        flip_x, flip_y = lax.rem(k, 2), lax.div(k, 2)
        return (y + flip_y - 2 * y * flip_y) * 2 + x + flip_x - 2 * x * flip_x

    def act_step(step, carry):
        n = turn(step)
        for half_at in range(2):
            rows = pl.ds(pl.multiple_of(n * block + half_at * (block // 2), block // 2), block // 2)
            cols = statc[rows, :]
            for side in range(sides):
                lanes = pl.ds(side * LANES, LANES)
                normal = (conv[side, rows, :] - cols[:, 0:1]) * cols[:, 1:2] * r.lng[:, lanes] + r.lnb[:, lanes]
                actb[rows, lanes] = (normal * jax.nn.sigmoid(normal)).astype(bf16)
        give_rows(0, actb, n)
        return carry

    lax.fori_loop(0, inner, act_step, 0)

    def memory_step(step, carry):
        n = turn(step)
        queries = project(n, 4).astype(bf16)
        wide = queries.astype(f32)
        scores = lax.dot_general(
            queries, kb[chunk(n), :], (((1,), (1,)), ((), ())), preferred_element_type=f32
        )
        values = vb[chunk(n), :]
        cols = r.colw[chunk(n), :]
        out = jnp.zeros((block, HEAD), f32)
        for d in range(2):
            carry_weight, floor = cols[:, 2 * d : 2 * d + 1], cols[:, 2 * d + 1 : 2 * d + 2]
            inner_part = scores * r.wgt[d, n]
            num = jnp.dot(inner_part.astype(bf16), values, preferred_element_type=f32)
            far = jnp.dot(queries, chi[d, n], preferred_element_type=f32)
            far = far + jnp.dot(queries, clo[d, n], preferred_element_type=f32)
            den = jnp.sum(inner_part + carry_weight * (wide * nvs[d, n][0:1]), axis=-1, keepdims=True)
            share_of = 1.0 / jnp.maximum(jnp.abs(den), floor)
            out = out + (num * share_of + far * (carry_weight * share_of))
        level = lax.rsqrt(jnp.mean(out * out, axis=-1, keepdims=True) + EPS)
        memb[chunk(n), :] = (out * level * r.mgn[...]).astype(bf16)
        give_rows(1, memb, n)
        return carry

    lax.fori_loop(0, inner, memory_step, 0)
    acc, pbuf = r.acc, r.pbuf
    tile = 512
    tiles = model // tile

    def own_sender(which):
        return local(actb.at[chunk(i), :], cin.at[which, i], r.rel_s.at[which])

    def take(which):
        for k in range(inner):
            def hear(k=k):
                remote(actb.at[chunk(0), :], cin.at[which, near[k]], r.ret_s.at[which, 0], r.ret_r.at[which, near[k]], (o, i, mate)).wait_recv()
            if k:
                hear()
            else:
                guarded(jnp.logical_not(primary), hear)
                guarded(primary, own_sender(which).wait)

    def part(which, n):
        return sum(
            jnp.dot(cin[which, k], ow[which, pl.ds(k * HEAD, HEAD), span(n, tile)], preferred_element_type=f32)
            for k in range(inner)
        )

    def conv_out_step(n, carry):
        acc[:, span(n, tile)] = part(0, n)
        return carry

    for copy in out_in:
        copy.wait()
    take(0)
    lax.fori_loop(0, tiles, conv_out_step, 0)

    take(1)

    out_own, out_mate = r.out_own, r.out_mate

    def piece(n):
        return remote(
            pbuf.at[span(mate, hb), span(n, tile)], out_mate.at[:, span(n, tile)],
            r.fin_s.at[n], r.fin_r.at[n], (o, i, mate),
        )

    def stay(n):
        return local(pbuf.at[span(t, hb), span(n, tile)], out_own.at[:, span(n, tile)], r.fil_s.at[n])

    def mem_out_step(n, carry):
        pbuf[:, span(n, tile)] = (acc[:, span(n, tile)] + part(1, n)).astype(bf16)
        piece(n).start()
        stay(n).start()
        return carry

    lax.fori_loop(0, tiles, mem_out_step, 0)

    for copy, when in sends:
        if when is None:
            copy.wait_send()
        else:
            pl.when(when)(copy.wait_send)

    for s in range(pieces):
        for c, slot in ((t, 0), (mate, 2)):
            pass_on(i, c, s, 1, slot).wait_send()
            pass_on(i, c, s, 2, slot + 1).wait_send()

    @pl.when(primary)
    def _():
        for copy in mate_small:
            copy.wait_send()
        for j in range(count):
            for plane_at in deal_planes(j):
                for k in range(1, inner):
                    deal(j, plane_at, k).wait_send()
                share(j, plane_at).wait_send()

    for which, source in ((0, actb), (1, memb)):
        for b in range(inner):
            guarded(jnp.logical_not(jnp.logical_and(primary, i == b)), give(which, source, b).wait_send)
    for n in range(tiles):
        stay(n).wait()
        piece(n).wait()


LANES = 128
LOW_START = -1e30


def whole_layer(outer, inner, tp, args):
    tokens = args.tokens
    block, half = tokens.shape
    depth = args.glu_value.shape[0]
    count = 5
    quarter, model = inner * block, half * tp
    hb = block // tp
    pad = 16
    f32, bf16 = jnp.float32, jnp.bfloat16
    dma = pltpu.SemaphoreType.DMA
    tiles = model // 512
    extra = args.log_decay_extra.T
    operands = dict(
        tokens=tokens, norm_gain=args.norm_gain[None],
        glu_value=args.glu_value, glu_gate=args.glu_gate,
        key_weight=args.key_weight, value_weight=args.value_weight, query_weight=args.query_weight,
        conv_taps=args.conv_taps, ln_gain=args.ln_gain[None], ln_bias=args.ln_bias[None],
        gate_weight=args.gate_weight.T, gate_bias=args.gate_bias,
        extra=extra, mem_gain=args.mem_gain[None],
        out_conv=args.out_conv, out_mem=args.out_mem,
    )
    scratch = dict(
        nq=pltpu.VMEM((quarter, model), bf16),
        nsrc=pltpu.VMEM((hb, model), bf16),
        xin=pltpu.VMEM((tp, hb, half), bf16),
        wst=pltpu.VMEM((count, outer, depth, half), bf16),
        wfull=pltpu.VMEM((count, model, HEAD), bf16),
        wmv=pltpu.VMEM((2, depth, half), bf16),
        ow=pltpu.VMEM((2,) + args.out_conv.shape, bf16),
        taps=pltpu.VMEM((KW, HEAD), f32), lng=pltpu.VMEM((1, HEAD), f32),
        lnb=pltpu.VMEM((1, HEAD), f32), mgn=pltpu.VMEM((1, HEAD), f32),
        ext=pltpu.VMEM((inner,) + extra.shape, f32),
        gwp=pltpu.VMEM((LANES, model), bf16),
        gt=pltpu.VMEM((4 * MEMORY_HEADS, quarter), f32),
        rowsv=pltpu.VMEM((8, quarter), f32), colsv=pltpu.VMEM((quarter, LANES), f32),
        gpad=pltpu.VMEM((HEAD // LANES, quarter + 2 * pad, LANES), f32),
        conv=pltpu.VMEM((HEAD // LANES, quarter, LANES), f32), gval=pltpu.VMEM((quarter, HEAD), f32),
        hsend=pltpu.VMEM((2, pad, HEAD), bf16), hrecv=pltpu.VMEM((2, pad, HEAD), bf16),
        statc=pltpu.VMEM((quarter, LANES), f32), sums=pltpu.VMEM((8, quarter), f32),
        stbuf=pltpu.VMEM((MEMORY_HEADS, 8, quarter), f32),
        kb=pltpu.VMEM((quarter, HEAD), bf16), vb=pltpu.VMEM((quarter, HEAD), bf16),
        cm=pltpu.VMEM((2, inner, HEAD, HEAD), f32), cv=pltpu.VMEM((2, inner, 8, HEAD), f32),
        matx=pltpu.VMEM((2, HEAD, HEAD), bf16), infox=pltpu.VMEM((2, 8, HEAD), f32),
        smat=pltpu.VMEM((2, HEAD, HEAD), bf16), sinfo=pltpu.VMEM((2, 8, HEAD), f32),
        gmat=pltpu.VMEM((HEAD, HEAD), bf16), ginfo=pltpu.VMEM((8, HEAD), f32),
        gin=pltpu.VMEM((HEAD, HEAD), bf16), gininfo=pltpu.VMEM((8, HEAD), f32),
        chi=pltpu.VMEM((2, inner, HEAD, HEAD), bf16), clo=pltpu.VMEM((2, inner, HEAD, HEAD), bf16),
        wgt=pltpu.VMEM((2, inner, block, block), f32), colw=pltpu.VMEM((quarter, LANES), f32),
        nvs=pltpu.VMEM((2, inner, 8, HEAD), f32), levs=pltpu.VMEM((2, inner, 8, LANES), f32),
        actb=pltpu.VMEM((quarter, HEAD), bf16), memb=pltpu.VMEM((quarter, HEAD), bf16),
        cin=pltpu.VMEM((2, inner, block, HEAD), bf16),
        acc=pltpu.VMEM((block, model), f32), pbuf=pltpu.VMEM((block, model), bf16),
        own_s=dma((count,)), mov_s=dma((2,)), mov_r=dma((2,)), mvd_s=dma((2,)), loc_s=dma((5,)), xin_s=dma, xin_r=dma,
        w1_s=dma((count, outer // tp)), w1_r=dma((count, outer)),
        sml_s=dma((4,)), prm_s=dma((4,)), prm_r=dma((4,)),
        ext_s=dma((inner,)), ext_r=dma((inner,)),
        tok_s=dma((2, 2)), tok_r=dma((inner, tp, 2)), pas_s=dma((6, 2)),
        w2_s=dma((count, outer, inner - 1)), w2_r=dma((count, outer, inner - 1)),
        keep_s=dma((count, outer)), fw_s=dma((count, outer)), fw_r=dma((count, outer)),
        hal_s=dma((2,)), hal_r=dma((2,)),
        sta_s=dma((MEMORY_HEADS,)), sta_r=dma((MEMORY_HEADS,)),
        mat_s=dma((3,)), mat_r=dma((3,)), inf_s=dma((2,)), inf_r=dma((2,)),
        ret_s=dma((2, inner)), ret_r=dma((2, inner)), rel_s=dma((2,)),
        fin_s=dma((tiles,)), fin_r=dma((tiles,)), fil_s=dma((tiles,)),
    )
    any_space = pl.BlockSpec(memory_space=pl.ANY)
    spaces = {n: any_space for n in operands}
    spaces.update(
        gate_bias=pl.BlockSpec(memory_space=pltpu.SMEM), norm_gain=pl.BlockSpec(memory_space=pltpu.VMEM)
    )
    names = list(operands) + ["out_own", "out_mate"] + list(scratch)
    shape = pltpu.VMEM((hb, model), bf16)
    own, mate = pl.pallas_call(
        functools.partial(layer_kernel, outer, inner, tp, names),
        out_shape=(shape, shape),
        in_specs=[spaces[n] for n in operands],
        out_specs=(pl.BlockSpec(memory_space=pltpu.VMEM),) * 2,
        scratch_shapes=list(scratch.values()),
        compiler_params=pltpu.CompilerParams(
            collective_id=0, has_side_effects=True, vmem_limit_bytes=60 * 2**20
        ),
    )(*operands.values())
    return (own.astype(f32) + mate.astype(f32)).astype(bf16)


def gather_inputs(tokens, weights, extra, inner):
    rows, half = tokens.shape
    gathered = lax.all_gather(tokens, ("inner", "tp"), axis=0)
    tp = gathered.shape[0] // inner
    whole = jnp.transpose(gathered.reshape(inner, tp, rows, half), (0, 2, 1, 3))
    whole = whole.reshape(inner * rows, tp * half)
    depth, columns = weights[0].shape
    width = columns // inner
    packed = jnp.stack([w.reshape(depth, inner, width) for w in weights], axis=2)
    packed = jnp.transpose(packed, (1, 0, 2, 3)).reshape(inner, depth, len(weights) * width)
    if inner > 1:
        packed = lax.all_to_all(packed, "inner", split_axis=0, concat_axis=0, tiled=True)
    pieces = lax.all_gather(packed.reshape(inner * depth, -1), "outer", axis=0, tiled=True)
    pieces = pieces.reshape(-1, len(weights), width).transpose(1, 0, 2)
    extras = lax.all_gather(extra, "inner", axis=0, tiled=True) if inner > 1 else extra
    return whole, pieces, extras.T


def local_state(keys, values, shifted, level, total, scale):
    weight = jnp.exp(shifted - level[:, None]) * scale
    weighted = keys.astype(jnp.float32) * weight[:, :, None]
    mat = jnp.einsum(
        "hsd,hse->hde", weighted.astype(jnp.bfloat16), values, preferred_element_type=jnp.float32
    )
    return mat, jnp.sum(weighted, axis=1), level + total, total


def packed_state(mat, vec, level, decay):
    spread = lambda x: jnp.broadcast_to(x[:, None], vec.shape)
    rows = parts_of(vec) + parts_of(spread(level)) + parts_of(spread(decay))
    pad = [jnp.zeros_like(rows[0])] * 7
    return jnp.concatenate([mat.astype(jnp.bfloat16), jnp.stack(rows + pad, axis=1)], axis=1)


def incoming(states, reverse):
    count = states.shape[0]
    mats = states[:, :, :HEAD]
    rows = states[:, :, HEAD:]
    vecs = whole_of(rows[:, :, 0], rows[:, :, 1], rows[:, :, 2])
    levels = whole_of(rows[:, :, 3, 0], rows[:, :, 4, 0], rows[:, :, 5, 0])
    decays = whole_of(rows[:, :, 6, 0], rows[:, :, 7, 0], rows[:, :, 8, 0])
    place = lax.axis_index("outer")
    order = jnp.arange(count)
    if reverse:
        ahead = (order > place)[:, None]
        between = (order[None, :] < order[:, None]) & (order[None, :] > place)
    else:
        ahead = (order < place)[:, None]
        between = (order[None, :] > order[:, None]) & (order[None, :] < place)
    lost = jnp.sum(jnp.where(between[:, :, None], decays[None], 0.0), axis=1)
    reach = jnp.where(ahead, levels + lost, -1e30)
    level = jnp.max(reach, axis=0)
    share = jnp.where(ahead, jnp.exp(reach - level[None]), 0.0)
    mat = jnp.sum(share[:, :, None, None] * mats.astype(jnp.float32), axis=0)
    vec = jnp.sum(share[:, :, None] * vecs, axis=0)
    return mat, vec, level


def finish(query_wide, num, den, running, decay, state):
    mat, vec, level = state
    top = jnp.maximum(running, level[:, None])
    local_weight = jnp.exp(running - top)
    carry_weight = jnp.exp(level[:, None] - top)
    num = local_weight[:, :, None] * num + carry_weight[:, :, None] * jnp.einsum(
        "htd,hde->hte", query_wide, mat, precision=PRECISE
    )
    den = local_weight * den + carry_weight * jnp.einsum(
        "htd,hd->ht", query_wide, vec, precision=PRECISE
    )
    return num / jnp.maximum(jnp.abs(den), jnp.exp(-top - decay))[:, :, None]


def make_shards(inner, outer, tp):
    def own(array, dim):
        size = array.shape[dim] // inner
        return lax.dynamic_slice_in_dim(array, lax.axis_index("inner") * size, size, dim)

    def shards(
        tokens,
        norm_gain,
        glu_value,
        glu_gate,
        conv_taps,
        ln_gain,
        ln_bias,
        query_weight,
        key_weight,
        value_weight,
        gate_weight,
        gate_bias,
        log_decay_extra,
        mem_gain,
        out_conv,
        out_mem,
    ):
        fits = tp == 2 and inner == 4 and outer == 2 * tp and inner * tp == MEMORY_HEADS
        if fits and tokens.shape[1] == inner * HEAD and conv_taps.shape[1] == inner * HEAD:
            return whole_layer(outer, inner, tp, types.SimpleNamespace(
                tokens=tokens, norm_gain=norm_gain, glu_value=glu_value, glu_gate=glu_gate,
                conv_taps=conv_taps, ln_gain=ln_gain, ln_bias=ln_bias, query_weight=query_weight,
                key_weight=key_weight, value_weight=value_weight, gate_weight=gate_weight,
                gate_bias=gate_bias, log_decay_extra=log_decay_extra, mem_gain=mem_gain,
                out_conv=out_conv, out_mem=out_mem,
            ))
        taps, gain, bias, mgain = own(conv_taps, 1), own(ln_gain, 0), own(ln_bias, 0), own(mem_gain, 0)
        channels = conv_taps.shape[1] * tp
        width = gain.shape[0]
        heads = mgain.shape[0] // HEAD
        first = (lax.axis_index("tp") * inner + lax.axis_index("inner")) * heads
        stacked = (query_weight, key_weight, value_weight, glu_value, glu_gate)
        whole, weights, extras = gather_inputs(tokens, stacked, log_decay_extra, inner)
        rows = whole.shape[0]
        wide = whole.astype(jnp.float32)
        normed = (
            wide * lax.rsqrt(jnp.mean(wide * wide, axis=-1, keepdims=True) + EPS) * norm_gain
        ).astype(jnp.bfloat16)
        own_gate = lax.dynamic_slice_in_dim(
            gate_weight.reshape(-1, 4, MEMORY_HEADS), first, heads, 2
        )
        own_bias = lax.dynamic_slice_in_dim(gate_bias.reshape(4, MEMORY_HEADS), first, heads, 1)
        gates = lax.dot_general(
            own_gate.reshape(-1, 4 * heads), normed, (((0,), (1,)), ((), ())),
            preferred_element_type=jnp.float32,
        ).reshape(4, heads, rows) + own_bias[:, :, None]
        own_extra = lax.dynamic_slice_in_dim(
            extras.reshape(2, MEMORY_HEADS, rows), first, heads, 1
        )
        lf = jax.nn.log_sigmoid(gates[1::2]) + own_extra
        at = jnp.arange(rows)
        causal = at[:, None] >= at[None, :]
        anti = at[:, None] <= at[None, :]

        def total(x, mask):
            return jnp.sum(jnp.where(mask, x[:, None, :], 0.0), axis=-1)

        def highest(x, mask):
            return jnp.max(jnp.where(mask, x[:, None, :], -jnp.inf), axis=-1)

        decay_f = total(lf[0], causal)
        decay_b = total(lf[1], anti)
        shifted_f = gates[0] - decay_f
        shifted_b = gates[2] - decay_b
        running_f = highest(shifted_f, causal)
        running_b = highest(shifted_b, anti)

        def project(i):
            return jnp.dot(normed, weights[i], preferred_element_type=jnp.float32)

        def heads_first(x):
            return jnp.transpose(x.reshape(rows, heads, HEAD), (1, 0, 2)).astype(jnp.bfloat16)

        keys = heads_first(project(1))
        values = heads_first(project(2))
        scale = HEAD ** (-0.5)
        state_f = local_state(
            keys, values, shifted_f, running_f[:, -1], decay_f[:, -1], scale
        )
        state_b = local_state(keys, values, shifted_b, running_b[:, 0], decay_b[:, 0], scale)
        sent = jnp.stack([packed_state(*state_f), packed_state(*state_b)])
        states = lax.all_gather(sent, "outer", axis=0)

        glu = (project(3) * jax.nn.sigmoid(project(4))).astype(jnp.bfloat16)
        reach = KW // 2
        before = lax.ppermute(glu[rows - reach :], "outer", [(i, i + 1) for i in range(outer - 1)])
        after = lax.ppermute(glu[:reach], "outer", [(i + 1, i) for i in range(outer - 1)])
        queries = heads_first(project(0))

        scores = jnp.einsum("htd,hsd->hts", queries, keys, preferred_element_type=jnp.float32) * scale

        def local_out(shifted, running, mask):
            weight = jnp.where(
                mask, jnp.exp(jnp.minimum(shifted[:, None, :] - running[:, :, None], 0.0)), 0.0
            )
            part = scores * weight
            num = jnp.einsum(
                "hts,hse->hte", part.astype(jnp.bfloat16), values,
                preferred_element_type=jnp.float32,
            )
            return num, jnp.sum(part, axis=-1)

        num_f, den_f = local_out(shifted_f, running_f, causal)
        num_b, den_b = local_out(shifted_b, running_b, anti)

        padded = jnp.concatenate([before, glu, after], axis=0).astype(jnp.float32)
        conv = jnp.zeros(glu.shape, jnp.float32)
        for offset in range(KW):
            conv = conv + taps[offset] * padded[offset : offset + rows]
        sums = jnp.stack([jnp.sum(conv, axis=-1), jnp.sum(conv * conv, axis=-1)])
        sums = lax.psum(sums, ("inner", "tp")) / channels
        chan_mean = sums[0]
        chan_var = sums[1] - chan_mean * chan_mean
        normal = (conv - chan_mean[:, None]) * lax.rsqrt(chan_var + EPS)[:, None] * gain + bias
        act = (normal * jax.nn.sigmoid(normal)).astype(jnp.bfloat16)

        query_wide = queries.astype(jnp.float32)
        forward = finish(query_wide, num_f, den_f, running_f, decay_f, incoming(states[:, 0], False))
        backward = finish(query_wide, num_b, den_b, running_b, decay_b, incoming(states[:, 1], True))
        summed = forward + backward
        head_norm = summed * lax.rsqrt(jnp.mean(summed * summed, axis=-1, keepdims=True) + EPS)
        head_norm = head_norm * mgain.reshape(heads, HEAD)[:, None, :]
        memory = jnp.transpose(head_norm, (1, 0, 2)).reshape(rows, heads * HEAD).astype(jnp.bfloat16)

        def back(x):
            if inner == 1:
                return x
            return lax.all_to_all(x, "inner", split_axis=0, concat_axis=1, tiled=True)

        result = jnp.dot(back(act), out_conv, preferred_element_type=jnp.float32)
        result = result + jnp.dot(back(memory), out_mem, preferred_element_type=jnp.float32)
        return lax.psum_scatter(
            result.astype(jnp.bfloat16), "tp", scatter_dimension=0, tiled=True
        )

    return shards


def solution(mesh):
    sp, tp = mesh.shape["sp"], mesh.shape["tp"]
    inner = math.gcd(sp, max(MEMORY_HEADS // tp, 1))
    outer = sp // inner
    fine = Mesh(mesh.devices.reshape(outer, inner, tp), ("outer", "inner", "tp"))
    rows = ("outer", "inner")
    in_specs = (
        P(rows, "tp"),
        P(),
        P(rows, "tp"),
        P(rows, "tp"),
        P(None, "tp"),
        P("tp"),
        P("tp"),
        P(rows, "tp"),
        P(rows, "tp"),
        P(rows, "tp"),
        P(),
        P(),
        P(rows, None),
        P("tp"),
        P("tp", None),
        P("tp", None),
    )
    return jax.shard_map(
        make_shards(inner, outer, tp), mesh=fine, in_specs=in_specs,
        out_specs=P(("outer", "inner", "tp"), None), check_vma=False,
    )
```

```python
import functools
import math
import types

import jax
import jax.numpy as jnp
from jax import lax
from jax.experimental import pallas as pl
from jax.experimental.pallas import tpu as pltpu
from jax.sharding import Mesh, PartitionSpec as P

MEMORY_HEADS = 8
HEAD = 256
KW = 31

EPS = 1e-06
PRECISE = lax.Precision.HIGHEST


def parts_of(x):
    first = lax.reduce_precision(x, 8, 7)
    rest = x - first
    second = lax.reduce_precision(rest, 8, 7)
    third = rest - second
    return [p.astype(jnp.bfloat16) for p in (first, second, third)]


def whole_of(a, b, c):
    return a.astype(jnp.float32) + b.astype(jnp.float32) + c.astype(jnp.float32)


MESH = pl.DeviceIdType.MESH


def layer_kernel(outer, inner, tp, names, *refs):
    r = types.SimpleNamespace(**dict(zip(names, refs)))
    tokens, norm_gain = r.tokens, r.norm_gain
    weights = [r.glu_value, r.glu_gate, r.key_weight, r.value_weight, r.query_weight]
    count = len(weights)
    o, i, t = lax.axis_index("outer"), lax.axis_index("inner"), lax.axis_index("tp")
    block, half = tokens.shape
    depth = weights[0].shape[0]
    hb = block // tp
    quarter = inner * block
    groups = outer // tp
    model = half * tp
    channels = MEMORY_HEADS * HEAD
    scale = HEAD ** (-0.5)
    f32, bf16 = jnp.float32, jnp.bfloat16

    par, grp = lax.rem(o, tp), lax.div(o, tp)
    mate = 1 - t
    twin = o + 1 - 2 * par
    primary = t == par
    place = grp * tp + t
    last = outer - 1
    x, y = lax.rem(i, 2), lax.div(i, 2)
    near = [i, y * 2 + 1 - x, (1 - y) * 2 + x, (1 - y) * 2 + 1 - x]
    head = par * inner + i

    nq, nsrc, xin, wst, wfull, ow = r.nq, r.nsrc, r.xin, r.wst, r.wfull, r.ow

    def span(index, size):
        return pl.ds(pl.multiple_of(index * size, size), size)

    def remote(src, dst, send, recv, device):
        return pltpu.make_async_remote_copy(
            src_ref=src, dst_ref=dst, send_sem=send, recv_sem=recv,
            device_id=device, device_id_type=MESH,
        )

    sends = []

    def start(copy, when=None):
        if when is None:
            copy.start()
        else:
            pl.when(when)(copy.start)
        sends.append((copy, when))

    def guarded(when, action):
        pl.when(when)(action)

    local = pltpu.make_async_copy

    own_rows = [local(weights[j], wst.at[j, o], r.own_s.at[j]) for j in range(count)]
    tok_own = local(tokens.at[span(t, hb), :], xin.at[t], r.loc_s.at[0])
    tok_own.start()

    for copy in own_rows:
        copy.start()

    gate_in = local(r.gate_weight, r.gwp.at[pl.ds(0, r.gate_weight.shape[0]), :], r.loc_s.at[1])
    out_in = [
        local(source, ow.at[k], r.loc_s.at[2 + k]) for k, source in enumerate((r.out_conv, r.out_mem))
    ]

    barrier = pltpu.get_barrier_semaphore()
    greeted = []
    for dz in range(tp):
        for k in range(inner):
            for c in range(tp):
                if (dz, k, c) != (0, 0, 0):
                    greeted.append((o if dz == 0 else twin, near[k], t if c == 0 else mate))
    for step in range(1, groups):
        away = lax.rem(grp + step, groups) * tp
        for dz in range(tp):
            for c in range(tp):
                greeted.append((away + dz, i, c))
    for device in greeted:
        pl.semaphore_signal(barrier, inc=1, device_id=device, device_id_type=MESH)
    pl.semaphore_wait(barrier, len(greeted))

    start(remote(tokens.at[span(mate, hb), :], xin.at[t], r.xin_s, r.xin_r, (o, i, mate)))

    def spread(j, step):
        target = lax.rem(grp + step, groups) * tp + t
        return remote(
            wst.at[j, o], wst.at[j, o], r.w1_s.at[j, step], r.w1_r.at[j, o], (target, i, t)
        )

    moved = (1, 3)

    def plane_of(step):
        return lax.rem(grp + step, groups) * tp

    def hand_over(j):
        at = moved.index(j)
        return remote(wst.at[j, o], r.wmv.at[at], r.mov_s.at[at], r.mov_r.at[at], (o, i, mate))

    def spread_all(j, phase):
        for step in range(groups):
            target = lax.rem(grp + step, groups) * tp + t
            apart = (target - o) * (twin - o) < 0
            if phase == 0:
                when = jnp.logical_and(apart, jnp.logical_not(primary))
            elif phase == 1:
                when = jnp.logical_not(apart)
                if step == 0:
                    when = jnp.logical_and(when, jnp.logical_not(primary))
            else:
                when = jnp.logical_and(apart, primary)
            if step and phase == 1 and j in moved:
                start(spread(j, step), jnp.logical_and(when, primary))
                other = plane_of(step) + mate
                at_end = jnp.logical_and(primary, (other - o) * (twin - o) > 0)

                @pl.when(at_end)
                def _():
                    hand_over(j).wait_recv()

                start(remote(
                    r.wmv.at[moved.index(j)], wst.at[j, o], r.mvd_s.at[moved.index(j)], r.w1_r.at[j, o], (other, i, mate)
                ), at_end)
            elif step or phase == 1:
                start(spread(j, step), when)

    def arrived(j, plane):
        remote(wst.at[j, plane], wst.at[j, plane], r.w1_s.at[j, 0], r.w1_r.at[j, plane], (o, i, mate)).wait_recv()

    small = ((r.conv_taps, r.taps), (r.ln_gain, r.lng), (r.ln_bias, r.lnb), (r.mem_gain, r.mgn))
    own_small = [
        local(a.at[:, span(i, HEAD)], b, r.sml_s.at[k]) for k, (a, b) in enumerate(small)
    ]
    mate_small = [
        remote(a.at[:, span(i, HEAD)], b, r.prm_s.at[k], r.prm_r.at[k], (o, i, mate))
        for k, (a, b) in enumerate(small)
    ]
    for j in range(count):
        own_rows[j].wait()
        spread_all(j, 0)
        if j in moved:
            at_end = (plane_of(1) + t - o) * (twin - o) > 0
            start(hand_over(j), jnp.logical_and(jnp.logical_not(primary), at_end))

    @pl.when(primary)
    def _():
        for copy in own_small:
            copy.start()
        for copy in mate_small:
            copy.start()

    ext = r.ext
    plane = jnp.where(primary, o, twin)
    own_ext = local(r.extra, ext.at[i], r.loc_s.at[4])
    guarded(primary, own_ext.start)
    for k in range(inner):
        copy = remote(r.extra, ext.at[i], r.ext_s.at[k], r.ext_r.at[i], (plane, near[k], par))
        start(copy, None if k else jnp.logical_not(primary))

    gate_in.start()
    for copy in out_in:
        copy.start()

    tok_own.wait()
    remote(xin.at[mate], xin.at[mate], r.xin_s, r.xin_r, (o, i, mate)).wait_recv()
    norm_rows = 32
    pieces = 2
    piece_rows = hb // pieces

    def norm_step(m, carry):
        at = span(m, norm_rows)
        parts = [xin[f, at, :].astype(f32) for f in range(tp)]
        square = sum(jnp.sum(p * p, axis=-1, keepdims=True) for p in parts)
        level = lax.rsqrt(square * (1.0 / model) + EPS)
        for f in range(tp):
            row = (parts[f] * level * norm_gain[:, pl.ds(f * half, half)]).astype(bf16)
            nsrc[at, pl.ds(f * half, half)] = row

            @pl.when(primary)
            def _():
                nq[pl.ds(pl.multiple_of(i * block + t * hb + m * norm_rows, norm_rows), norm_rows), pl.ds(f * half, half)] = row
        return carry

    def rows_of(b, c, s):
        return nq.at[pl.ds(pl.multiple_of(b * block + c * hb + s * piece_rows, piece_rows), piece_rows), :]

    def tok_wait(b, c, s):
        rows = rows_of(b, c, s)
        remote(rows, rows, r.tok_s.at[0, 0], r.tok_r.at[b, c, s], (o, i, mate)).wait_recv()

    steps = piece_rows // norm_rows
    for s in range(pieces):
        lax.fori_loop(s * steps, (s + 1) * steps, norm_step, 0)
        source = nsrc.at[pl.ds(s * piece_rows, piece_rows), :]
        start(remote(source, rows_of(i, t, s), r.tok_s.at[1, s], r.tok_r.at[i, t, s], (twin, i, par)))
        start(remote(source, rows_of(i, t, s), r.tok_s.at[0, s], r.tok_r.at[i, t, s], (o, i, mate)), jnp.logical_not(primary))
    for j in range(count):
        spread_all(j, 1)

    def row_block(owner_plane, owner):
        return pl.ds(pl.multiple_of((owner_plane * inner + owner) * depth, depth), depth)

    def deal(j, plane_at, k):
        return remote(
            wst.at[j, plane_at, :, span(near[k], HEAD)],
            wfull.at[j, row_block(plane_at, i), :],
            r.w2_s.at[j, plane_at, k - 1], r.w2_r.at[j, plane_at, k - 1], (o, near[k], t),
        )

    def keep(j, plane_at):
        return local(
            wst.at[j, plane_at, :, span(i, HEAD)], wfull.at[j, row_block(plane_at, i), :],
            r.keep_s.at[j, plane_at],
        )

    def deal_planes(j):
        bases = [plane_of(step) for step in range(1, groups)]
        nearer = [base + jnp.where(base < o, 1, 0) for base in bases]
        farther = [base + jnp.where(base < o, 0, 1) for base in bases]
        return [o] + nearer + [twin] + farther

    def deal_all(j, which=None):
        @pl.when(primary)
        def _():
            for index, plane_at in enumerate(deal_planes(j)):
                if which is not None and index not in which:
                    continue
                if index:
                    arrived(j, plane_at)
                for k in range(1, inner):
                    deal(j, plane_at, k).start()
                keep(j, plane_at).start()

    def share(j, plane_at):
        rows = pl.ds(pl.multiple_of(plane_at * inner * depth, inner * depth), inner * depth)
        return remote(
            wfull.at[j, rows, :], wfull.at[j, rows, :],
            r.fw_s.at[j, plane_at], r.fw_r.at[j, plane_at], (o, i, mate),
        )

    def collect(j):
        @pl.when(primary)
        def _():
            for plane_at in deal_planes(j):
                keep(j, plane_at).wait()
                for k in range(1, inner):
                    rows = wfull.at[j, row_block(plane_at, near[k]), :]
                    remote(rows, rows, r.w2_s.at[j, plane_at, k - 1], r.w2_r.at[j, plane_at, k - 1], (o, i, mate)).wait_recv()
                share(j, plane_at).start()

        @pl.when(jnp.logical_not(primary))
        def _():
            for plane_at in deal_planes(j):
                share(j, plane_at).wait_recv()

    def pass_on(b_from, c, s, k, slot):
        rows = rows_of(b_from, c, s)
        return remote(rows, rows, r.pas_s.at[slot, s], r.tok_r.at[b_from, c, s], (o, near[k], t))

    @pl.when(primary)
    def _():
        for s in range(pieces):
            for c, slot in ((t, 0), (mate, 2)):
                if slot:
                    tok_wait(i, c, s)
                pass_on(i, c, s, 1, slot).start()
                pass_on(i, c, s, 2, slot + 1).start()

    @pl.when(jnp.logical_not(primary))
    def _():
        for s in range(pieces):
            for c, slot in ((t, 0), (mate, 2)):
                tok_wait(i, c, s)
                pass_on(i, c, s, 1, slot).start()
                pass_on(i, c, s, 2, slot + 1).start()

    for s in range(pieces):
        tok_wait(near[1], 0, s)
        start(pass_on(near[1], 0, s, 2, 4))
        tok_wait(near[2], 1, s)
        start(pass_on(near[2], 1, s, 1, 5))
    for j in range(count):
        spread_all(j, 2)
    for s in range(pieces):
        tok_wait(near[1], 1, s)
        tok_wait(near[2], 0, s)
        tok_wait(near[3], 0, s)
        tok_wait(near[3], 1, s)

    deal_all(0)
    deal_all(1)

    gwp, gt, rowsv, colsv = r.gwp, r.gt, r.rowsv, r.colsv
    gate_in.wait()

    def chunk(n):
        return span(n, block)

    def gate_step(n, carry):
        got = lax.dot_general(
            nq[chunk(n), :], gwp[...], (((1,), (1,)), ((), ())), preferred_element_type=f32
        )
        gt[:, chunk(n)] = got.T[: gt.shape[0]]
        return carry

    lax.fori_loop(0, inner, gate_step, 0)
    guarded(primary, own_ext.wait)
    for k in range(inner):
        def hear(k=k):
            remote(r.extra, ext.at[near[k]], r.ext_s.at[0], r.ext_r.at[near[k]], (o, i, mate)).wait_recv()
        if k:
            hear()
        else:
            guarded(jnp.logical_not(primary), hear)

    mine = lax.broadcasted_iota(jnp.int32, (MEMORY_HEADS, quarter), 0) == head
    mine_block = lax.broadcasted_iota(jnp.int32, (MEMORY_HEADS, block), 0) == head

    def gate_row(g):
        rows = gt[pl.ds(g * MEMORY_HEADS, MEMORY_HEADS), :]
        return jnp.sum(jnp.where(mine, rows, 0.0), axis=0, keepdims=True) + r.gate_bias[g * MEMORY_HEADS + head]

    def extra_row(d):
        pieces = [
            jnp.sum(jnp.where(mine_block, ext[b, pl.ds(d * MEMORY_HEADS, MEMORY_HEADS), :], 0.0), axis=0, keepdims=True)
            for b in range(inner)
        ]
        return jnp.concatenate(pieces, axis=1)

    def log_sigmoid(v):
        return jnp.minimum(v, 0.0) - jnp.log1p(jnp.exp(-jnp.abs(v)))

    within = lax.rem(lax.broadcasted_iota(jnp.int32, (1, quarter), 1), block)

    def scan(v, forward, join, empty):
        step = 1
        while step < block:
            if forward:
                v = join(v, jnp.where(within >= step, pltpu.roll(v, step, 1), empty))
            else:
                v = join(v, jnp.where(within < block - step, pltpu.roll(v, quarter - step, 1), empty))
            step *= 2
        return v

    table = []
    for d in range(2):
        gate_in_row = gate_row(2 * d)
        forget = log_sigmoid(gate_row(2 * d + 1)) + extra_row(d)
        decay = scan(forget, d == 0, jnp.add, 0.0)
        shifted = gate_in_row - decay
        running = scan(shifted, d == 0, jnp.maximum, -jnp.inf)
        table += [shifted, running, decay]
    table += [jnp.zeros((1, quarter), f32)] * 2
    rowsv[...] = jnp.concatenate(table, axis=0)

    def turn_step(n, carry):
        piece = rowsv[:, chunk(n)]
        wide = jnp.concatenate([piece, jnp.zeros((LANES - piece.shape[0], block), f32)], axis=0)
        colsv[chunk(n), :] = wide.T
        return carry

    lax.fori_loop(0, inner, turn_step, 0)

    def project(n, j):
        return jnp.dot(nq[chunk(n), :], wfull[j], preferred_element_type=f32)

    kb, vb, cm, cv = r.kb, r.vb, r.cm, r.cv
    smat, sinfo, matx, infox = r.smat, r.sinfo, r.matx, r.infox
    gmat, ginfo, gin, gininfo = r.gmat, r.ginfo, r.gin, r.gininfo

    def key_step(n, carry):
        kb[chunk(n), :] = project(n, 2).astype(bf16)
        return carry

    def state_step(n, carry):
        values = project(n, 3).astype(bf16)
        vb[chunk(n), :] = values
        keys = kb[chunk(n), :].astype(f32)
        cols = colsv[chunk(n), :]
        for d in range(2):
            end = block - 1 if d == 0 else 0
            top = cols[end : end + 1, 3 * d + 1 : 3 * d + 2]
            weighted = keys * (jnp.exp(cols[:, 3 * d : 3 * d + 1] - top) * scale)
            cm[d, n] = lax.dot_general(
                weighted.astype(bf16), values, (((0,), (0,)), ((), ())), preferred_element_type=f32
            )
            cv[d, n] = jnp.broadcast_to(jnp.sum(weighted, axis=0, keepdims=True), (8, HEAD))
        return carry

    earlier = lax.broadcasted_iota(jnp.int32, (block, block), 0) >= lax.broadcasted_iota(jnp.int32, (block, block), 1)
    later = lax.broadcasted_iota(jnp.int32, (block, block), 0) <= lax.broadcasted_iota(jnp.int32, (block, block), 1)

    def weight_step(n, carry):
        cols = colsv[chunk(n), :]
        rows = rowsv[:, chunk(n)]
        for d in range(2):
            gap = jnp.minimum(rows[3 * d : 3 * d + 1] - cols[:, 3 * d + 1 : 3 * d + 2], 0.0)
            r.wgt[d, n] = jnp.where(earlier if d == 0 else later, jnp.exp(gap) * scale, 0.0)
        return carry

    lax.fori_loop(0, inner, weight_step, 0)
    collect(0)
    gpad, conv, hsend, hrecv = r.gpad, r.conv, r.hsend, r.hrecv
    pad = hsend.shape[1]
    reach = KW // 2
    sides = HEAD // LANES

    def value_step(n, carry):
        r.gval[chunk(n), :] = project(n, 0)
        return carry

    lax.fori_loop(0, inner, value_step, 0)
    deal_all(2)
    collect(1)

    def glu_step(n, carry):
        glu = (r.gval[chunk(n), :] * jax.nn.sigmoid(project(n, 1))).astype(bf16)
        for side in range(sides):
            gpad[side, pl.ds(pl.multiple_of(n * block + pad, pad), block), :] = glu[:, side * LANES : (side + 1) * LANES].astype(f32)

        @pl.when(n == 0)
        def _():
            hsend[0] = glu[:pad]

        @pl.when(n == inner - 1)
        def _():
            hsend[1] = glu[block - pad :]

        return carry

    lax.fori_loop(0, inner, glu_step, 0)
    def device_of(q):
        return (lax.div(q, tp) * tp + par, i, lax.rem(q, tp))

    has_before, has_after = place > 0, place < last
    start(remote(hsend.at[0], hrecv.at[1], r.hal_s.at[0], r.hal_r.at[1], device_of(jnp.maximum(place - 1, 0))), has_before)
    start(remote(hsend.at[1], hrecv.at[0], r.hal_s.at[1], r.hal_r.at[0], device_of(jnp.minimum(place + 1, last))), has_after)

    @pl.when(primary)
    def _():
        for copy in own_small:
            copy.wait()

    @pl.when(jnp.logical_not(primary))
    def _():
        for copy in mate_small:
            copy.wait_recv()

    deal_all(3, range(2))
    taps, statc, stbuf = r.taps, r.statc, r.stbuf
    conv_rows = 64
    lane = lax.broadcasted_iota(jnp.int32, (conv_rows, LANES), 1)
    shift = pad - reach

    def conv_step(m, carry):
        s1 = s2 = 0.0
        for side in range(sides):
            total = jnp.zeros((conv_rows, LANES), f32)
            for residue in range(8):
                moved = gpad[side, pl.ds(m * conv_rows + residue, conv_rows + 2 * pad - 8), :]
                for j in range(KW):
                    at = j + shift - residue
                    if at % 8 == 0:
                        tap = taps[pl.ds(j, 1), pl.ds(side * LANES, LANES)]
                        total = total + tap * moved[at : at + conv_rows]
            conv[side, span(m, conv_rows), :] = total
            s1 = s1 + total
            s2 = s2 + total * total
        s1 = jnp.sum(s1, axis=-1, keepdims=True)
        s2 = jnp.sum(s2, axis=-1, keepdims=True)
        statc[span(m, conv_rows), :] = jnp.where(lane == 0, s1, jnp.where(lane == 1, s2, 0.0))
        return carry

    conv_steps = quarter // conv_rows
    lax.fori_loop(1, conv_steps // 2, conv_step, 0)
    collect(2)
    lax.fori_loop(conv_steps // 2, conv_steps - 1, conv_step, 0)
    deal_all(3, range(2, outer))
    for edge, present, at in ((0, has_before, 0), (1, has_after, pad + quarter)):
        @pl.when(present)
        def _():
            remote(hrecv.at[edge], hrecv.at[edge], r.hal_s.at[0], r.hal_r.at[edge], (o, i, mate)).wait_recv()
            for side in range(sides):
                gpad[side, pl.ds(at, pad), :] = hrecv[edge, :, side * LANES : (side + 1) * LANES].astype(f32)

        @pl.when(jnp.logical_not(present))
        def _():
            for side in range(sides):
                gpad[side, pl.ds(at, pad), :] = jnp.zeros((pad, LANES), f32)

    lax.fori_loop(0, 2, lambda m, carry: conv_step(m * (conv_steps - 1), carry), 0)
    sums = r.sums
    two = pl.ds(0, 2)

    def sums_step(n, carry):
        sums[:, chunk(n)] = statc[chunk(n), :].T[: sums.shape[0]]
        return carry

    lax.fori_loop(0, inner, sums_step, 0)
    peers = []
    for dz in range(tp):
        for k in range(inner):
            if (dz, k) != (0, 0):
                peers.append((o if dz == 0 else twin, near[k]))
    for index, (plane_to, chip) in enumerate(peers):
        start(remote(sums.at[two, :], stbuf.at[head, two, :], r.sta_s.at[index], r.sta_r.at[head], (plane_to, chip, t)))
    lax.fori_loop(0, inner, key_step, 0)
    deal_all(4, range(2))
    collect(3)
    deal_all(4, (2,))
    lax.fori_loop(0, inner // 2, state_step, 0)
    deal_all(4, range(3, outer))
    lax.fori_loop(inner // 2, inner, state_step, 0)

    def corner(n, d, column):
        end = block - 1 if d == 0 else 0
        at = n * block + end
        return colsv[pl.ds(at, 1), :][:, column : column + 1]

    totals = [[corner(n, d, 3 * d + 2) for n in range(inner)] for d in range(2)]
    levels = [[corner(n, d, 3 * d + 1) + totals[d][n] for n in range(inner)] for d in range(2)]
    for d in range(2):
        reaches = []
        for n in range(inner):
            later = range(n + 1, inner) if d == 0 else range(n)
            value = levels[d][n]
            for m in later:
                value = value + totals[d][m]
            reaches.append(value)
        top = functools.reduce(jnp.maximum, reaches)
        shares = [jnp.exp(v - top) for v in reaches]
        matx[d] = sum(shares[n] * cm[d, n] for n in range(inner)).astype(bf16)
        vec = sum(shares[n] * cv[d, n] for n in range(inner))
        row = lax.broadcasted_iota(jnp.int32, (8, HEAD), 0)
        decay = functools.reduce(jnp.add, totals[d])
        infox[d] = jnp.where(row == 0, vec, jnp.where(row == 1, top, decay))

    start(remote(matx, smat, r.mat_s.at[0], r.mat_r.at[0], (o, i, mate)))
    start(remote(infox, sinfo, r.inf_s.at[0], r.inf_r.at[0], (o, i, mate)))
    for plane_from, chip in peers:
        other = lax.rem(plane_from, tp) * inner + chip
        remote(sums.at[two, :], stbuf.at[other, two, :], r.sta_s.at[0], r.sta_r.at[other], (o, i, mate)).wait_recv()
    stbuf[head] = sums[...]

    def stat_step(n, carry):
        whole = stbuf[0, :, chunk(n)]
        for k in range(1, MEMORY_HEADS):
            whole = whole + stbuf[k, :, chunk(n)]
        whole = whole * (1.0 / channels)
        mean = whole[0:1]
        rstd = lax.rsqrt(whole[1:2] - mean * mean + EPS)
        wide = jnp.concatenate([mean, rstd, jnp.zeros((LANES - 2, block), f32)], axis=0)
        statc[chunk(n), :] = wide.T
        return carry

    lax.fori_loop(0, inner, stat_step, 0)
    actb, memb, cin = r.actb, r.memb, r.cin

    def give(which, source, b):
        return remote(
            source.at[chunk(b), :], cin.at[which, i], r.ret_s.at[which, b], r.ret_r.at[which, i],
            (plane, b, par),
        )

    def give_own(which, source):
        return local(source.at[chunk(i), :], cin.at[which, i], r.rel_s.at[which])

    def give_rows(which, source, b):
        to_self = jnp.logical_and(primary, b == i)
        guarded(to_self, give_own(which, source).start)
        guarded(jnp.logical_not(to_self), give(which, source, b).start)

    def turn(step):
        k = inner - 1 - step
        flip_x, flip_y = lax.rem(k, 2), lax.div(k, 2)
        return (y + flip_y - 2 * y * flip_y) * 2 + x + flip_x - 2 * x * flip_x

    def act_step(n, carry):
        for half_at in range(2):
            rows = pl.ds(pl.multiple_of(n * block + half_at * (block // 2), block // 2), block // 2)
            cols = statc[rows, :]
            for side in range(sides):
                lanes = pl.ds(side * LANES, LANES)
                normal = (conv[side, rows, :] - cols[:, 0:1]) * cols[:, 1:2] * r.lng[:, lanes] + r.lnb[:, lanes]
                actb[rows, lanes] = (normal * jax.nn.sigmoid(normal)).astype(bf16)
        return carry

    lax.fori_loop(0, inner, act_step, 0)

    mat_rows = gin.at[span(t, HEAD // tp), :]
    mate_rows = gin.at[span(mate, HEAD // tp), :]
    remote(matx, smat, r.mat_s.at[0], r.mat_r.at[0], (o, i, mate)).wait_recv()
    remote(infox, sinfo, r.inf_s.at[0], r.inf_r.at[0], (o, i, mate)).wait_recv()
    ours, theirs = infox[grp], sinfo[grp]
    is_far = t == grp
    our_reach = ours[1:2, 0:1] + jnp.where(is_far, theirs[2:3, 0:1], 0.0)
    their_reach = theirs[1:2, 0:1] + jnp.where(is_far, 0.0, ours[2:3, 0:1])
    group_level = jnp.maximum(our_reach, their_reach)
    our_share, their_share = jnp.exp(our_reach - group_level), jnp.exp(their_reach - group_level)
    gmat[...] = (our_share * matx[grp].astype(f32) + their_share * smat[grp].astype(f32)).astype(bf16)
    state_row = lax.broadcasted_iota(jnp.int32, (8, HEAD), 0)
    ginfo[...] = jnp.where(state_row == 0, our_share * ours[0:1] + their_share * theirs[0:1], group_level)
    across = ((1 - grp) * tp + par, i, t)
    start(remote(gmat.at[span(t, HEAD // tp), :], mat_rows, r.mat_s.at[1], r.mat_r.at[1], across))
    start(remote(ginfo, gininfo, r.inf_s.at[1], r.inf_r.at[1], across))
    for k in range(inner - 1, -1, -1):
        give_rows(0, actb, near[k])
    collect(4)

    def query_step(n, carry):
        r.qb[chunk(n), :] = project(n, 4).astype(bf16)
        return carry

    lax.fori_loop(0, inner, query_step, 0)
    remote(mat_rows, mat_rows, r.mat_s.at[1], r.mat_r.at[1], (o, i, mate)).wait_recv()
    start(remote(mat_rows, mat_rows, r.mat_s.at[2], r.mat_r.at[2], (o, i, mate)))
    remote(ginfo, gininfo, r.inf_s.at[1], r.inf_r.at[1], (o, i, mate)).wait_recv()
    remote(mate_rows, mate_rows, r.mat_s.at[2], r.mat_r.at[2], (o, i, mate)).wait_recv()

    nvs, levs = r.nvs, r.levs
    for d in range(2):
        by_mate, by_group = t == 1 - d, grp == 1 - d
        near_reach = jnp.where(by_mate, sinfo[d][1:2, 0:1], LOW_START)
        far_reach = gininfo[1:2, 0:1] + jnp.where(by_mate, sinfo[d][2:3, 0:1], 0.0)
        far_reach = jnp.where(by_group, far_reach, LOW_START)
        level = jnp.maximum(near_reach, far_reach)
        near_share = jnp.where(by_mate, jnp.exp(near_reach - level), 0.0)
        far_share = jnp.where(by_group, jnp.exp(far_reach - level), 0.0)
        mat = near_share * smat[d].astype(f32) + far_share * gin[...].astype(f32)
        vec = near_share * sinfo[d][0:1] + far_share * gininfo[0:1]
        for n in (range(inner) if d == 0 else range(inner - 1, -1, -1)):
            high = mat.astype(bf16)
            r.cst[d, n, pl.ds(0, HEAD), :] = high
            r.cst[d, n, pl.ds(HEAD, HEAD), :] = (mat - high.astype(f32)).astype(bf16)
            nvs[d, n] = jnp.broadcast_to(vec, (8, HEAD))
            levs[d, n] = jnp.broadcast_to(level, (8, LANES))
            carried = level + totals[d][n]
            new_level = jnp.maximum(carried, levels[d][n])
            kept, added = jnp.exp(carried - new_level), jnp.exp(levels[d][n] - new_level)
            mat = kept * mat + added * cm[d, n]
            vec = kept * vec + added * cv[d, n][0:1]
            level = new_level

    def column_step(n, carry):
        rows = rowsv[:, chunk(n)]
        kept = []
        for d in range(2):
            running, decay = rows[3 * d + 1 : 3 * d + 2], rows[3 * d + 2 : 3 * d + 3]
            level = levs[d, n][0:1, 0:1]
            top = jnp.maximum(running, level)
            kept += [jnp.exp(running - top), jnp.exp(level - top), jnp.exp(-top - decay)]
        kept.append(jnp.zeros((LANES - len(kept), block), f32))
        r.colw[chunk(n), :] = jnp.concatenate(kept, axis=0).T
        return carry

    lax.fori_loop(0, inner, column_step, 0)
    def memory_step(step, carry):
        n = turn(step)
        queries = r.qb[chunk(n), :]
        score = lax.dot_general(
            queries, kb[chunk(n), :], (((1,), (1,)), ((), ())), preferred_element_type=f32
        )
        wide = queries.astype(f32)
        twice = jnp.concatenate([queries, queries], axis=1)
        values = vb[chunk(n), :]
        cols = r.colw[chunk(n), :]
        out = 0.0
        for d in range(2):
            local_weight, carry_weight = cols[:, 3 * d : 3 * d + 1], cols[:, 3 * d + 1 : 3 * d + 2]
            floor = cols[:, 3 * d + 2 : 3 * d + 3]
            inner_part = score * r.wgt[d, n]
            num = jnp.dot(inner_part.astype(bf16), values, preferred_element_type=f32)
            far = jnp.dot(twice, r.cst[d, n], preferred_element_type=f32)
            inner_sum = jnp.sum(inner_part, axis=-1, keepdims=True)
            far_sum = jnp.sum(wide * nvs[d, n][0:1], axis=-1, keepdims=True)
            den = local_weight * inner_sum + carry_weight * far_sum
            share_of = 1.0 / jnp.maximum(jnp.abs(den), floor)
            out = out + (num * (local_weight * share_of) + far * (carry_weight * share_of))
        level = lax.rsqrt(jnp.mean(out * out, axis=-1, keepdims=True) + EPS)
        memb[chunk(n), :] = (out * level * r.mgn[...]).astype(bf16)
        give_rows(1, memb, n)
        return carry

    lax.fori_loop(0, inner, memory_step, 0)
    acc, pbuf = r.acc, r.pbuf
    tile = 512
    tiles = model // tile

    def own_sender(which):
        return local(actb.at[chunk(i), :], cin.at[which, i], r.rel_s.at[which])

    def take(which):
        for k in range(inner):
            def hear(k=k):
                remote(actb.at[chunk(0), :], cin.at[which, near[k]], r.ret_s.at[which, 0], r.ret_r.at[which, near[k]], (o, i, mate)).wait_recv()
            if k:
                hear()
            else:
                guarded(jnp.logical_not(primary), hear)
                guarded(primary, own_sender(which).wait)

    def part(which, n):
        return sum(
            jnp.dot(cin[which, k], ow[which, pl.ds(k * HEAD, HEAD), span(n, tile)], preferred_element_type=f32)
            for k in range(inner)
        )

    def conv_out_step(n, carry):
        acc[:, span(n, tile)] = part(0, n)
        return carry

    for copy in out_in:
        copy.wait()
    take(0)
    lax.fori_loop(0, tiles, conv_out_step, 0)

    take(1)

    out_own, out_mate = r.out_own, r.out_mate

    def piece(n):
        return remote(
            pbuf.at[span(mate, hb), span(n, tile)], out_mate.at[:, span(n, tile)],
            r.fin_s.at[n], r.fin_r.at[n], (o, i, mate),
        )

    def stay(n):
        return local(pbuf.at[span(t, hb), span(n, tile)], out_own.at[:, span(n, tile)], r.fil_s.at[n])

    def mem_out_step(n, carry):
        pbuf[:, span(n, tile)] = (acc[:, span(n, tile)] + part(1, n)).astype(bf16)
        piece(n).start()
        stay(n).start()
        return carry

    lax.fori_loop(0, tiles, mem_out_step, 0)

    for copy, when in sends:
        if when is None:
            copy.wait_send()
        else:
            pl.when(when)(copy.wait_send)

    for s in range(pieces):
        for c, slot in ((t, 0), (mate, 2)):
            pass_on(i, c, s, 1, slot).wait_send()
            pass_on(i, c, s, 2, slot + 1).wait_send()

    @pl.when(primary)
    def _():
        for copy in mate_small:
            copy.wait_send()
        for j in range(count):
            for plane_at in deal_planes(j):
                for k in range(1, inner):
                    deal(j, plane_at, k).wait_send()
                share(j, plane_at).wait_send()

    for which, source in ((0, actb), (1, memb)):
        for b in range(inner):
            guarded(jnp.logical_not(jnp.logical_and(primary, i == b)), give(which, source, b).wait_send)
    for n in range(tiles):
        stay(n).wait()
        piece(n).wait()


LANES = 128
LOW_START = -1e30


def whole_layer(outer, inner, tp, args):
    tokens = args.tokens
    block, half = tokens.shape
    depth = args.glu_value.shape[0]
    count = 5
    quarter, model = inner * block, half * tp
    hb = block // tp
    pad = 16
    f32, bf16 = jnp.float32, jnp.bfloat16
    dma = pltpu.SemaphoreType.DMA
    tiles = model // 512
    extra = args.log_decay_extra.T
    operands = dict(
        tokens=tokens, norm_gain=args.norm_gain[None],
        glu_value=args.glu_value, glu_gate=args.glu_gate,
        key_weight=args.key_weight, value_weight=args.value_weight, query_weight=args.query_weight,
        conv_taps=args.conv_taps, ln_gain=args.ln_gain[None], ln_bias=args.ln_bias[None],
        gate_weight=args.gate_weight.T, gate_bias=args.gate_bias,
        extra=extra, mem_gain=args.mem_gain[None],
        out_conv=args.out_conv, out_mem=args.out_mem,
    )
    scratch = dict(
        nq=pltpu.VMEM((quarter, model), bf16),
        nsrc=pltpu.VMEM((hb, model), bf16),
        xin=pltpu.VMEM((tp, hb, half), bf16),
        wst=pltpu.VMEM((count, outer, depth, half), bf16),
        wfull=pltpu.VMEM((count, model, HEAD), bf16),
        wmv=pltpu.VMEM((2, depth, half), bf16),
        ow=pltpu.VMEM((2,) + args.out_conv.shape, bf16),
        taps=pltpu.VMEM((KW, HEAD), f32), lng=pltpu.VMEM((1, HEAD), f32),
        lnb=pltpu.VMEM((1, HEAD), f32), mgn=pltpu.VMEM((1, HEAD), f32),
        ext=pltpu.VMEM((inner,) + extra.shape, f32),
        gwp=pltpu.VMEM((LANES, model), bf16),
        gt=pltpu.VMEM((4 * MEMORY_HEADS, quarter), f32),
        rowsv=pltpu.VMEM((8, quarter), f32), colsv=pltpu.VMEM((quarter, LANES), f32),
        gpad=pltpu.VMEM((HEAD // LANES, quarter + 2 * pad, LANES), f32),
        conv=pltpu.VMEM((HEAD // LANES, quarter, LANES), f32), gval=pltpu.VMEM((quarter, HEAD), f32),
        hsend=pltpu.VMEM((2, pad, HEAD), bf16), hrecv=pltpu.VMEM((2, pad, HEAD), bf16),
        statc=pltpu.VMEM((quarter, LANES), f32), sums=pltpu.VMEM((8, quarter), f32),
        stbuf=pltpu.VMEM((MEMORY_HEADS, 8, quarter), f32),
        kb=pltpu.VMEM((quarter, HEAD), bf16), vb=pltpu.VMEM((quarter, HEAD), bf16),
        cm=pltpu.VMEM((2, inner, HEAD, HEAD), f32), cv=pltpu.VMEM((2, inner, 8, HEAD), f32),
        matx=pltpu.VMEM((2, HEAD, HEAD), bf16), infox=pltpu.VMEM((2, 8, HEAD), f32),
        smat=pltpu.VMEM((2, HEAD, HEAD), bf16), sinfo=pltpu.VMEM((2, 8, HEAD), f32),
        gmat=pltpu.VMEM((HEAD, HEAD), bf16), ginfo=pltpu.VMEM((8, HEAD), f32),
        gin=pltpu.VMEM((HEAD, HEAD), bf16), gininfo=pltpu.VMEM((8, HEAD), f32),
        cst=pltpu.VMEM((2, inner, 2 * HEAD, HEAD), bf16), qb=pltpu.VMEM((quarter, HEAD), bf16),
        wgt=pltpu.VMEM((2, inner, block, block), f32), colw=pltpu.VMEM((quarter, LANES), f32),
        nvs=pltpu.VMEM((2, inner, 8, HEAD), f32), levs=pltpu.VMEM((2, inner, 8, LANES), f32),
        actb=pltpu.VMEM((quarter, HEAD), bf16), memb=pltpu.VMEM((quarter, HEAD), bf16),
        cin=pltpu.VMEM((2, inner, block, HEAD), bf16),
        acc=pltpu.VMEM((block, model), f32), pbuf=pltpu.VMEM((block, model), bf16),
        own_s=dma((count,)), mov_s=dma((2,)), mov_r=dma((2,)), mvd_s=dma((2,)), loc_s=dma((5,)), xin_s=dma, xin_r=dma,
        w1_s=dma((count, outer // tp)), w1_r=dma((count, outer)),
        sml_s=dma((4,)), prm_s=dma((4,)), prm_r=dma((4,)),
        ext_s=dma((inner,)), ext_r=dma((inner,)),
        tok_s=dma((2, 2)), tok_r=dma((inner, tp, 2)), pas_s=dma((6, 2)),
        w2_s=dma((count, outer, inner - 1)), w2_r=dma((count, outer, inner - 1)),
        keep_s=dma((count, outer)), fw_s=dma((count, outer)), fw_r=dma((count, outer)),
        hal_s=dma((2,)), hal_r=dma((2,)),
        sta_s=dma((MEMORY_HEADS,)), sta_r=dma((MEMORY_HEADS,)),
        mat_s=dma((3,)), mat_r=dma((3,)), inf_s=dma((2,)), inf_r=dma((2,)),
        ret_s=dma((2, inner)), ret_r=dma((2, inner)), rel_s=dma((2,)),
        fin_s=dma((tiles,)), fin_r=dma((tiles,)), fil_s=dma((tiles,)),
    )
    any_space = pl.BlockSpec(memory_space=pl.ANY)
    spaces = {n: any_space for n in operands}
    spaces.update(
        gate_bias=pl.BlockSpec(memory_space=pltpu.SMEM), norm_gain=pl.BlockSpec(memory_space=pltpu.VMEM)
    )
    names = list(operands) + ["out_own", "out_mate"] + list(scratch)
    shape = pltpu.VMEM((hb, model), bf16)
    own, mate = pl.pallas_call(
        functools.partial(layer_kernel, outer, inner, tp, names),
        out_shape=(shape, shape),
        in_specs=[spaces[n] for n in operands],
        out_specs=(pl.BlockSpec(memory_space=pltpu.VMEM),) * 2,
        scratch_shapes=list(scratch.values()),
        compiler_params=pltpu.CompilerParams(
            collective_id=0, has_side_effects=True, vmem_limit_bytes=60 * 2**20
        ),
    )(*operands.values())
    return (own.astype(f32) + mate.astype(f32)).astype(bf16)


def gather_inputs(tokens, weights, extra, inner):
    rows, half = tokens.shape
    gathered = lax.all_gather(tokens, ("inner", "tp"), axis=0)
    tp = gathered.shape[0] // inner
    whole = jnp.transpose(gathered.reshape(inner, tp, rows, half), (0, 2, 1, 3))
    whole = whole.reshape(inner * rows, tp * half)
    depth, columns = weights[0].shape
    width = columns // inner
    packed = jnp.stack([w.reshape(depth, inner, width) for w in weights], axis=2)
    packed = jnp.transpose(packed, (1, 0, 2, 3)).reshape(inner, depth, len(weights) * width)
    if inner > 1:
        packed = lax.all_to_all(packed, "inner", split_axis=0, concat_axis=0, tiled=True)
    pieces = lax.all_gather(packed.reshape(inner * depth, -1), "outer", axis=0, tiled=True)
    pieces = pieces.reshape(-1, len(weights), width).transpose(1, 0, 2)
    extras = lax.all_gather(extra, "inner", axis=0, tiled=True) if inner > 1 else extra
    return whole, pieces, extras.T


def local_state(keys, values, shifted, level, total, scale):
    weight = jnp.exp(shifted - level[:, None]) * scale
    weighted = keys.astype(jnp.float32) * weight[:, :, None]
    mat = jnp.einsum(
        "hsd,hse->hde", weighted.astype(jnp.bfloat16), values, preferred_element_type=jnp.float32
    )
    return mat, jnp.sum(weighted, axis=1), level + total, total


def packed_state(mat, vec, level, decay):
    spread = lambda x: jnp.broadcast_to(x[:, None], vec.shape)
    rows = parts_of(vec) + parts_of(spread(level)) + parts_of(spread(decay))
    pad = [jnp.zeros_like(rows[0])] * 7
    return jnp.concatenate([mat.astype(jnp.bfloat16), jnp.stack(rows + pad, axis=1)], axis=1)


def incoming(states, reverse):
    count = states.shape[0]
    mats = states[:, :, :HEAD]
    rows = states[:, :, HEAD:]
    vecs = whole_of(rows[:, :, 0], rows[:, :, 1], rows[:, :, 2])
    levels = whole_of(rows[:, :, 3, 0], rows[:, :, 4, 0], rows[:, :, 5, 0])
    decays = whole_of(rows[:, :, 6, 0], rows[:, :, 7, 0], rows[:, :, 8, 0])
    place = lax.axis_index("outer")
    order = jnp.arange(count)
    if reverse:
        ahead = (order > place)[:, None]
        between = (order[None, :] < order[:, None]) & (order[None, :] > place)
    else:
        ahead = (order < place)[:, None]
        between = (order[None, :] > order[:, None]) & (order[None, :] < place)
    lost = jnp.sum(jnp.where(between[:, :, None], decays[None], 0.0), axis=1)
    reach = jnp.where(ahead, levels + lost, -1e30)
    level = jnp.max(reach, axis=0)
    share = jnp.where(ahead, jnp.exp(reach - level[None]), 0.0)
    mat = jnp.sum(share[:, :, None, None] * mats.astype(jnp.float32), axis=0)
    vec = jnp.sum(share[:, :, None] * vecs, axis=0)
    return mat, vec, level


def finish(query_wide, num, den, running, decay, state):
    mat, vec, level = state
    top = jnp.maximum(running, level[:, None])
    local_weight = jnp.exp(running - top)
    carry_weight = jnp.exp(level[:, None] - top)
    num = local_weight[:, :, None] * num + carry_weight[:, :, None] * jnp.einsum(
        "htd,hde->hte", query_wide, mat, precision=PRECISE
    )
    den = local_weight * den + carry_weight * jnp.einsum(
        "htd,hd->ht", query_wide, vec, precision=PRECISE
    )
    return num / jnp.maximum(jnp.abs(den), jnp.exp(-top - decay))[:, :, None]


def make_shards(inner, outer, tp):
    def own(array, dim):
        size = array.shape[dim] // inner
        return lax.dynamic_slice_in_dim(array, lax.axis_index("inner") * size, size, dim)

    def shards(
        tokens,
        norm_gain,
        glu_value,
        glu_gate,
        conv_taps,
        ln_gain,
        ln_bias,
        query_weight,
        key_weight,
        value_weight,
        gate_weight,
        gate_bias,
        log_decay_extra,
        mem_gain,
        out_conv,
        out_mem,
    ):
        fits = tp == 2 and inner == 4 and outer == 2 * tp and inner * tp == MEMORY_HEADS
        if fits and tokens.shape[1] == inner * HEAD and conv_taps.shape[1] == inner * HEAD:
            return whole_layer(outer, inner, tp, types.SimpleNamespace(
                tokens=tokens, norm_gain=norm_gain, glu_value=glu_value, glu_gate=glu_gate,
                conv_taps=conv_taps, ln_gain=ln_gain, ln_bias=ln_bias, query_weight=query_weight,
                key_weight=key_weight, value_weight=value_weight, gate_weight=gate_weight,
                gate_bias=gate_bias, log_decay_extra=log_decay_extra, mem_gain=mem_gain,
                out_conv=out_conv, out_mem=out_mem,
            ))
        taps, gain, bias, mgain = own(conv_taps, 1), own(ln_gain, 0), own(ln_bias, 0), own(mem_gain, 0)
        channels = conv_taps.shape[1] * tp
        width = gain.shape[0]
        heads = mgain.shape[0] // HEAD
        first = (lax.axis_index("tp") * inner + lax.axis_index("inner")) * heads
        stacked = (query_weight, key_weight, value_weight, glu_value, glu_gate)
        whole, weights, extras = gather_inputs(tokens, stacked, log_decay_extra, inner)
        rows = whole.shape[0]
        wide = whole.astype(jnp.float32)
        normed = (
            wide * lax.rsqrt(jnp.mean(wide * wide, axis=-1, keepdims=True) + EPS) * norm_gain
        ).astype(jnp.bfloat16)
        own_gate = lax.dynamic_slice_in_dim(
            gate_weight.reshape(-1, 4, MEMORY_HEADS), first, heads, 2
        )
        own_bias = lax.dynamic_slice_in_dim(gate_bias.reshape(4, MEMORY_HEADS), first, heads, 1)
        gates = lax.dot_general(
            own_gate.reshape(-1, 4 * heads), normed, (((0,), (1,)), ((), ())),
            preferred_element_type=jnp.float32,
        ).reshape(4, heads, rows) + own_bias[:, :, None]
        own_extra = lax.dynamic_slice_in_dim(
            extras.reshape(2, MEMORY_HEADS, rows), first, heads, 1
        )
        lf = jax.nn.log_sigmoid(gates[1::2]) + own_extra
        at = jnp.arange(rows)
        causal = at[:, None] >= at[None, :]
        anti = at[:, None] <= at[None, :]

        def total(x, mask):
            return jnp.sum(jnp.where(mask, x[:, None, :], 0.0), axis=-1)

        def highest(x, mask):
            return jnp.max(jnp.where(mask, x[:, None, :], -jnp.inf), axis=-1)

        decay_f = total(lf[0], causal)
        decay_b = total(lf[1], anti)
        shifted_f = gates[0] - decay_f
        shifted_b = gates[2] - decay_b
        running_f = highest(shifted_f, causal)
        running_b = highest(shifted_b, anti)

        def project(i):
            return jnp.dot(normed, weights[i], preferred_element_type=jnp.float32)

        def heads_first(x):
            return jnp.transpose(x.reshape(rows, heads, HEAD), (1, 0, 2)).astype(jnp.bfloat16)

        keys = heads_first(project(1))
        values = heads_first(project(2))
        scale = HEAD ** (-0.5)
        state_f = local_state(
            keys, values, shifted_f, running_f[:, -1], decay_f[:, -1], scale
        )
        state_b = local_state(keys, values, shifted_b, running_b[:, 0], decay_b[:, 0], scale)
        sent = jnp.stack([packed_state(*state_f), packed_state(*state_b)])
        states = lax.all_gather(sent, "outer", axis=0)

        glu = (project(3) * jax.nn.sigmoid(project(4))).astype(jnp.bfloat16)
        reach = KW // 2
        before = lax.ppermute(glu[rows - reach :], "outer", [(i, i + 1) for i in range(outer - 1)])
        after = lax.ppermute(glu[:reach], "outer", [(i + 1, i) for i in range(outer - 1)])
        queries = heads_first(project(0))

        scores = jnp.einsum("htd,hsd->hts", queries, keys, preferred_element_type=jnp.float32) * scale

        def local_out(shifted, running, mask):
            weight = jnp.where(
                mask, jnp.exp(jnp.minimum(shifted[:, None, :] - running[:, :, None], 0.0)), 0.0
            )
            part = scores * weight
            num = jnp.einsum(
                "hts,hse->hte", part.astype(jnp.bfloat16), values,
                preferred_element_type=jnp.float32,
            )
            return num, jnp.sum(part, axis=-1)

        num_f, den_f = local_out(shifted_f, running_f, causal)
        num_b, den_b = local_out(shifted_b, running_b, anti)

        padded = jnp.concatenate([before, glu, after], axis=0).astype(jnp.float32)
        conv = jnp.zeros(glu.shape, jnp.float32)
        for offset in range(KW):
            conv = conv + taps[offset] * padded[offset : offset + rows]
        sums = jnp.stack([jnp.sum(conv, axis=-1), jnp.sum(conv * conv, axis=-1)])
        sums = lax.psum(sums, ("inner", "tp")) / channels
        chan_mean = sums[0]
        chan_var = sums[1] - chan_mean * chan_mean
        normal = (conv - chan_mean[:, None]) * lax.rsqrt(chan_var + EPS)[:, None] * gain + bias
        act = (normal * jax.nn.sigmoid(normal)).astype(jnp.bfloat16)

        query_wide = queries.astype(jnp.float32)
        forward = finish(query_wide, num_f, den_f, running_f, decay_f, incoming(states[:, 0], False))
        backward = finish(query_wide, num_b, den_b, running_b, decay_b, incoming(states[:, 1], True))
        summed = forward + backward
        head_norm = summed * lax.rsqrt(jnp.mean(summed * summed, axis=-1, keepdims=True) + EPS)
        head_norm = head_norm * mgain.reshape(heads, HEAD)[:, None, :]
        memory = jnp.transpose(head_norm, (1, 0, 2)).reshape(rows, heads * HEAD).astype(jnp.bfloat16)

        def back(x):
            if inner == 1:
                return x
            return lax.all_to_all(x, "inner", split_axis=0, concat_axis=1, tiled=True)

        result = jnp.dot(back(act), out_conv, preferred_element_type=jnp.float32)
        result = result + jnp.dot(back(memory), out_mem, preferred_element_type=jnp.float32)
        return lax.psum_scatter(
            result.astype(jnp.bfloat16), "tp", scatter_dimension=0, tiled=True
        )

    return shards


def solution(mesh):
    sp, tp = mesh.shape["sp"], mesh.shape["tp"]
    inner = math.gcd(sp, max(MEMORY_HEADS // tp, 1))
    outer = sp // inner
    fine = Mesh(mesh.devices.reshape(outer, inner, tp), ("outer", "inner", "tp"))
    rows = ("outer", "inner")
    in_specs = (
        P(rows, "tp"),
        P(),
        P(rows, "tp"),
        P(rows, "tp"),
        P(None, "tp"),
        P("tp"),
        P("tp"),
        P(rows, "tp"),
        P(rows, "tp"),
        P(rows, "tp"),
        P(),
        P(),
        P(rows, None),
        P("tp"),
        P("tp", None),
        P("tp", None),
    )
    return jax.shard_map(
        make_shards(inner, outer, tp), mesh=fine, in_specs=in_specs,
        out_specs=P(("outer", "inner", "tp"), None), check_vma=False,
    )
```

```python
import functools
import math
import types

import jax
import jax.numpy as jnp
from jax import lax
from jax.experimental import pallas as pl
from jax.experimental.pallas import tpu as pltpu
from jax.sharding import Mesh, PartitionSpec as P

MEMORY_HEADS = 8
HEAD = 256
KW = 31

EPS = 1e-06
PRECISE = lax.Precision.HIGHEST


def parts_of(x):
    first = lax.reduce_precision(x, 8, 7)
    rest = x - first
    second = lax.reduce_precision(rest, 8, 7)
    third = rest - second
    return [p.astype(jnp.bfloat16) for p in (first, second, third)]


def whole_of(a, b, c):
    return a.astype(jnp.float32) + b.astype(jnp.float32) + c.astype(jnp.float32)


MESH = pl.DeviceIdType.MESH


def layer_kernel(outer, inner, tp, names, *refs):
    r = types.SimpleNamespace(**dict(zip(names, refs)))
    tokens, norm_gain = r.tokens, r.norm_gain
    weights = [r.glu_value, r.glu_gate, r.key_weight, r.value_weight, r.query_weight]
    count = len(weights)
    o, i, t = lax.axis_index("outer"), lax.axis_index("inner"), lax.axis_index("tp")
    block, half = tokens.shape
    depth = weights[0].shape[0]
    hb = block // tp
    quarter = inner * block
    groups = outer // tp
    model = half * tp
    channels = MEMORY_HEADS * HEAD
    scale = HEAD ** (-0.5)
    f32, bf16 = jnp.float32, jnp.bfloat16

    par, grp = lax.rem(o, tp), lax.div(o, tp)
    mate = 1 - t
    twin = o + 1 - 2 * par
    primary = t == par
    place = grp * tp + t
    last = outer - 1
    x, y = lax.rem(i, 2), lax.div(i, 2)
    near = [i, y * 2 + 1 - x, (1 - y) * 2 + x, (1 - y) * 2 + 1 - x]
    head = par * inner + i

    nq, nsrc, xin, wst, wfull, ow = r.nq, r.nsrc, r.xin, r.wst, r.wfull, r.ow

    def span(index, size):
        return pl.ds(pl.multiple_of(index * size, size), size)

    def remote(src, dst, send, recv, device):
        return pltpu.make_async_remote_copy(
            src_ref=src, dst_ref=dst, send_sem=send, recv_sem=recv,
            device_id=device, device_id_type=MESH,
        )

    sends = []

    def start(copy, when=None):
        if when is None:
            copy.start()
        else:
            pl.when(when)(copy.start)
        sends.append((copy, when))

    def guarded(when, action):
        pl.when(when)(action)

    local = pltpu.make_async_copy

    own_rows = [local(weights[j], wst.at[j, o], r.own_s.at[j]) for j in range(count)]
    tok_own = local(tokens.at[span(t, hb), :], xin.at[t], r.loc_s.at[0])
    tok_own.start()
    gain_in = local(norm_gain, r.gain, r.loc_s.at[5])
    bias_in = local(r.gate_bias, r.bias, r.loc_s.at[6])
    gain_in.start()
    bias_in.start()

    for copy in own_rows:
        copy.start()

    gate_in = local(r.gate_weight, r.gwp.at[pl.ds(0, r.gate_weight.shape[0]), :], r.loc_s.at[1])
    out_in = [
        local(source, ow.at[k], r.loc_s.at[2 + k]) for k, source in enumerate((r.out_conv, r.out_mem))
    ]

    barrier = pltpu.get_barrier_semaphore()
    greeted = []
    for dz in range(tp):
        for k in range(inner):
            for c in range(tp):
                if (dz, k, c) != (0, 0, 0):
                    greeted.append((o if dz == 0 else twin, near[k], t if c == 0 else mate))
    for step in range(1, groups):
        away = lax.rem(grp + step, groups) * tp
        for dz in range(tp):
            for c in range(tp):
                greeted.append((away + dz, i, c))
    for device in greeted:
        pl.semaphore_signal(barrier, inc=1, device_id=device, device_id_type=MESH)
    pl.semaphore_wait(barrier, len(greeted))

    start(remote(tokens.at[span(mate, hb), :], xin.at[t], r.xin_s, r.xin_r, (o, i, mate)))

    def spread(j, step):
        target = lax.rem(grp + step, groups) * tp + t
        return remote(
            wst.at[j, o], wst.at[j, o], r.w1_s.at[j, step], r.w1_r.at[j, o], (target, i, t)
        )

    moved = (1, 3)

    def plane_of(step):
        return lax.rem(grp + step, groups) * tp

    def hand_over(j):
        at = moved.index(j)
        return remote(wst.at[j, o], r.wmv.at[at], r.mov_s.at[at], r.mov_r.at[at], (o, i, mate))

    def spread_all(j, phase):
        for step in range(groups):
            target = lax.rem(grp + step, groups) * tp + t
            apart = (target - o) * (twin - o) < 0
            if phase == 0:
                when = jnp.logical_and(apart, jnp.logical_not(primary))
            elif phase == 1:
                when = jnp.logical_not(apart)
                if step == 0:
                    when = jnp.logical_and(when, jnp.logical_not(primary))
            else:
                when = jnp.logical_and(apart, primary)
            if step and phase == 1 and j in moved:
                start(spread(j, step), jnp.logical_and(when, primary))
                other = plane_of(step) + mate
                at_end = jnp.logical_and(primary, (other - o) * (twin - o) > 0)

                @pl.when(at_end)
                def _():
                    hand_over(j).wait_recv()

                start(remote(
                    r.wmv.at[moved.index(j)], wst.at[j, o], r.mvd_s.at[moved.index(j)], r.w1_r.at[j, o], (other, i, mate)
                ), at_end)
            elif step or phase == 1:
                start(spread(j, step), when)

    def arrived(j, plane):
        remote(wst.at[j, plane], wst.at[j, plane], r.w1_s.at[j, 0], r.w1_r.at[j, plane], (o, i, mate)).wait_recv()

    def row_block(owner_plane, owner):
        return pl.ds(pl.multiple_of((owner_plane * inner + owner) * depth, depth), depth)

    by_second = (4,)

    def keep(j, plane_at):
        return local(
            wst.at[j, plane_at, :, span(i, HEAD)], wfull.at[j, row_block(plane_at, i), :], r.keep_s.at[j]
        )

    def deal(j, plane_at, k):
        return remote(
            wst.at[j, plane_at, :, span(near[k], HEAD)],
            wfull.at[j, row_block(plane_at, i), :],
            r.w2_s.at[j], r.w2_r.at[j, plane_at], (o, near[k], mate if j in by_second else t),
        )

    def deal_planes(j):
        base = plane_of(1)
        nearer, farther = base + jnp.where(base < o, 1, 0), base + jnp.where(base < o, 0, 1)
        at_end = (nearer - o) * (twin - o) > 0
        return [o, jnp.where(at_end, twin, nearer), farther, jnp.where(at_end, nearer, twin)]

    def deal_all(j, which=None):
        @pl.when(primary)
        def _():
            for index, plane_at in enumerate(deal_planes(j)):
                if which is not None and index not in which:
                    continue
                if index:
                    arrived(j, plane_at)
                for k in range(0 if j in by_second else 1, inner):
                    deal(j, plane_at, k).start()
                if j not in by_second:
                    keep(j, plane_at).start()

    def share(j, plane_at):
        rows = pl.ds(pl.multiple_of(plane_at * inner * depth, inner * depth), inner * depth)
        return remote(
            wfull.at[j, rows, :], wfull.at[j, rows, :],
            r.fw_s.at[j], r.fw_r.at[j], (o, i, mate),
        )

    def received(ref, semaphore):
        remote(ref, ref, semaphore, semaphore, (o, i, mate)).wait_recv()

    def collect(j):
        second = j in by_second
        collects = jnp.logical_not(primary) if second else primary

        @pl.when(collects)
        def _():
            if not second:
                local(wst.at[j, 0], wst.at[j, 0], r.keep_s.at[j]).wait()
            for plane_at in deal_planes(j):
                start_row = pl.multiple_of(plane_at * inner * depth, depth)
                rows = (inner if second else inner - 1) * depth
                received(wfull.at[j, pl.ds(start_row, rows), :], r.w2_r.at[j, plane_at])
                share(j, plane_at).start()

        @pl.when(jnp.logical_not(collects))
        def _():
            received(wfull.at[j], r.fw_r.at[j])

    small = ((r.conv_taps, r.taps), (r.ln_gain, r.lng), (r.ln_bias, r.lnb), (r.mem_gain, r.mgn))
    own_small = [
        local(a.at[:, span(i, HEAD)], b, r.sml_s.at[k]) for k, (a, b) in enumerate(small)
    ]
    mate_small = [
        remote(a.at[:, span(i, HEAD)], b, r.prm_s.at[k], r.prm_r.at[k], (o, i, mate))
        for k, (a, b) in enumerate(small)
    ]
    for j in range(count):
        own_rows[j].wait()
        spread_all(j, 0)
        if j in moved:
            at_end = (plane_of(1) + t - o) * (twin - o) > 0
            start(hand_over(j), jnp.logical_and(jnp.logical_not(primary), at_end))

    @pl.when(primary)
    def _():
        for copy in own_small:
            copy.start()
        for copy in mate_small:
            copy.start()

    ext = r.ext
    plane = jnp.where(primary, o, twin)
    own_ext = local(r.extra, ext.at[i], r.loc_s.at[4])
    guarded(primary, own_ext.start)
    for k in range(inner):
        copy = remote(r.extra, ext.at[i], r.ext_s.at[k], r.ext_r.at[i], (plane, near[k], par))
        start(copy, None if k else jnp.logical_not(primary))

    early = 2
    for j in range(early):
        deal_all(j, (0,))
    gate_in.start()
    for copy in out_in:
        copy.start()

    tok_own.wait()
    gain_in.wait()
    remote(xin.at[mate], xin.at[mate], r.xin_s, r.xin_r, (o, i, mate)).wait_recv()
    norm_rows = 32
    pieces = 2
    piece_rows = hb // pieces

    def norm_step(m, carry):
        at = span(m, norm_rows)
        parts = [xin[f, at, :].astype(f32) for f in range(tp)]
        square = sum(jnp.sum(p * p, axis=-1, keepdims=True) for p in parts)
        level = lax.rsqrt(square * (1.0 / model) + EPS)
        for f in range(tp):
            row = (parts[f] * level * r.gain[:, pl.ds(f * half, half)]).astype(bf16)
            nsrc[at, pl.ds(f * half, half)] = row

            @pl.when(primary)
            def _():
                nq[pl.ds(pl.multiple_of(i * block + t * hb + m * norm_rows, norm_rows), norm_rows), pl.ds(f * half, half)] = row
        return carry

    def rows_of(b, c, s):
        return nq.at[pl.ds(pl.multiple_of(b * block + c * hb + s * piece_rows, piece_rows), piece_rows), :]

    def tok_wait(b, c, s):
        rows = rows_of(b, c, s)
        remote(rows, rows, r.tok_s.at[0, 0], r.tok_r.at[b, c, s], (o, i, mate)).wait_recv()

    steps = piece_rows // norm_rows
    for s in range(pieces):
        lax.fori_loop(s * steps, (s + 1) * steps, norm_step, 0)
        source = nsrc.at[pl.ds(s * piece_rows, piece_rows), :]
        start(remote(source, rows_of(i, t, s), r.tok_s.at[1, s], r.tok_r.at[i, t, s], (twin, i, par)))
        start(remote(source, rows_of(i, t, s), r.tok_s.at[0, s], r.tok_r.at[i, t, s], (o, i, mate)), jnp.logical_not(primary))
    for j in range(count):
        spread_all(j, 1)

    def pass_on(b_from, c, s, k, slot):
        rows = rows_of(b_from, c, s)
        target = near[k] if isinstance(k, int) else jnp.where(k == 1, near[1], near[2])
        return remote(rows, rows, r.pas_s, r.tok_r.at[b_from, c, s], (o, target, t))

    @pl.when(primary)
    def _():
        for s in range(pieces):
            pass_on(i, t, s, 1 + t, 0).start()
        for s in range(pieces):
            tok_wait(i, mate, s)
            pass_on(i, mate, s, 1 + mate, 1).start()
        for s in range(pieces):
            pass_on(i, t, s, 1 + mate, 2).start()
            pass_on(i, mate, s, 1 + t, 3).start()

    @pl.when(jnp.logical_not(primary))
    def _():
        for s in range(pieces):
            for c, slot in ((0, 0), (1, 1)):
                tok_wait(i, c, s)
                pass_on(i, c, s, 1 + c, slot).start()
        for s in range(pieces):
            for c, slot in ((0, 2), (1, 3)):
                pass_on(i, c, s, 2 - c, slot).start()

    for s in range(pieces):
        tok_wait(near[1], 0, s)
        pass_on(near[1], 0, s, 2, 4).start()
        tok_wait(near[2], 1, s)
        pass_on(near[2], 1, s, 1, 5).start()
    for j in range(count):
        spread_all(j, 2)
    received(nq.at[pl.ds(0, (inner - 1) * block), :], r.pas_s)

    @pl.when(jnp.logical_not(primary))
    def _():
        pl.semaphore_signal(r.clear, inc=1, device_id=(o, i, mate), device_id_type=MESH)

    for s in range(pieces):
        tok_wait(near[1], 1, s)
        tok_wait(near[2], 0, s)
        tok_wait(near[3], 0, s)
        tok_wait(near[3], 1, s)

    gwp, gt, rowsv, colsv = r.gwp, r.gt, r.rowsv, r.colsv
    gate_in.wait()
    bias_in.wait()
    bias_row = jnp.concatenate([r.bias[...], jnp.zeros((1, LANES - r.bias.shape[1]), f32)], axis=1)

    def chunk(n):
        return span(n, block)

    def gate_step(n, carry):
        got = lax.dot_general(
            nq[chunk(n), :], gwp[...], (((1,), (1,)), ((), ())), preferred_element_type=f32
        )
        gt[:, chunk(n)] = (got + bias_row).T[: gt.shape[0]]
        return carry

    lax.fori_loop(0, inner, gate_step, 0)
    guarded(primary, own_ext.wait)
    for k in range(inner):
        def hear(k=k):
            remote(r.extra, ext.at[near[k]], r.ext_s.at[0], r.ext_r.at[near[k]], (o, i, mate)).wait_recv()
        if k:
            hear()
        else:
            guarded(jnp.logical_not(primary), hear)

    mine = lax.broadcasted_iota(jnp.int32, (MEMORY_HEADS, quarter), 0) == head
    mine_block = lax.broadcasted_iota(jnp.int32, (MEMORY_HEADS, block), 0) == head

    def gate_row(g):
        rows = gt[pl.ds(g * MEMORY_HEADS, MEMORY_HEADS), :]
        return jnp.sum(jnp.where(mine, rows, 0.0), axis=0, keepdims=True)

    def extra_row(d):
        pieces = [
            jnp.sum(jnp.where(mine_block, ext[b, pl.ds(d * MEMORY_HEADS, MEMORY_HEADS), :], 0.0), axis=0, keepdims=True)
            for b in range(inner)
        ]
        return jnp.concatenate(pieces, axis=1)

    def log_sigmoid(v):
        return jnp.minimum(v, 0.0) - jnp.log1p(jnp.exp(-jnp.abs(v)))

    within = lax.rem(lax.broadcasted_iota(jnp.int32, (1, quarter), 1), block)

    def scan(v, forward, join, empty):
        step = 1
        while step < block:
            if forward:
                v = join(v, jnp.where(within >= step, pltpu.roll(v, step, 1), empty))
            else:
                v = join(v, jnp.where(within < block - step, pltpu.roll(v, quarter - step, 1), empty))
            step *= 2
        return v

    table = []
    for d in range(2):
        gate_in_row = gate_row(2 * d)
        forget = log_sigmoid(gate_row(2 * d + 1)) + extra_row(d)
        decay = scan(forget, d == 0, jnp.add, 0.0)
        shifted = gate_in_row - decay
        running = scan(shifted, d == 0, jnp.maximum, -jnp.inf)
        table += [shifted, running, decay]
    table += [jnp.zeros((1, quarter), f32)] * 2
    rowsv[...] = jnp.concatenate(table, axis=0)

    def turn_step(n, carry):
        piece = rowsv[:, chunk(n)]
        wide = jnp.concatenate([piece, jnp.zeros((LANES - piece.shape[0], block), f32)], axis=0)
        colsv[chunk(n), :] = wide.T
        return carry

    lax.fori_loop(0, inner, turn_step, 0)

    def project(n, j):
        return jnp.dot(nq[chunk(n), :], wfull[j], preferred_element_type=f32)

    kb, vb, cm, cv = r.kb, r.vb, r.cm, r.cv
    smat, sinfo, matx, infox = r.smat, r.sinfo, r.matx, r.infox
    gmat, ginfo, gin, gininfo = r.gmat, r.ginfo, r.gin, r.gininfo

    def key_step(n, carry):
        keys = project(n, 2)
        kb[chunk(n), :] = keys.astype(bf16)
        wide = keys.astype(bf16).astype(f32)
        cols = colsv[chunk(n), :]
        for d in range(2):
            end = block - 1 if d == 0 else 0
            top = cols[end : end + 1, 3 * d + 1 : 3 * d + 2]
            weighted = wide * (jnp.exp(cols[:, 3 * d : 3 * d + 1] - top) * scale)
            r.kwt[d, :, chunk(n)] = weighted.T.astype(bf16)
            cv[d, n] = jnp.broadcast_to(jnp.sum(weighted, axis=0, keepdims=True), (8, HEAD))
        return carry

    def state_step(m, carry):
        ns = [m * 2 + p for p in range(2)]
        values = [project(n, 3).astype(bf16) for n in ns]
        for n, value in zip(ns, values):
            vb[chunk(n), :] = value
        for n, value in zip(ns, values):
            for d in range(2):
                cm[d, n] = jnp.dot(r.kwt[d, :, chunk(n)], value, preferred_element_type=f32)
        return carry

    earlier = lax.broadcasted_iota(jnp.int32, (block, block), 0) >= lax.broadcasted_iota(jnp.int32, (block, block), 1)
    later = lax.broadcasted_iota(jnp.int32, (block, block), 0) <= lax.broadcasted_iota(jnp.int32, (block, block), 1)

    def weight_step(n, carry):
        cols = colsv[chunk(n), :]
        rows = rowsv[:, chunk(n)]
        for d in range(2):
            gap = jnp.minimum(rows[3 * d : 3 * d + 1] - cols[:, 3 * d + 1 : 3 * d + 2], 0.0)
            r.wgt[d, n] = jnp.where(earlier if d == 0 else later, jnp.exp(gap) * scale, 0.0)
        return carry

    lax.fori_loop(0, inner, weight_step, 0)
    @pl.when(primary)
    def _():
        pl.semaphore_wait(r.clear, 1)

    deal_all(0, range(1, outer))
    deal_all(1, range(1, outer))
    deal_all(2, range(2))

    collect(0)
    gpad, conv, hsend, hrecv = r.gpad, r.conv, r.hsend, r.hrecv
    pad = hsend.shape[1]
    reach = KW // 2
    sides = HEAD // LANES

    def value_step(n, carry):
        r.gval[chunk(n), :] = project(n, 0)
        return carry

    lax.fori_loop(0, inner, value_step, 0)
    deal_all(2, range(2, outer))
    deal_all(3, range(2))
    collect(1)

    def glu_step(n, carry):
        glu = (r.gval[chunk(n), :] * jax.nn.sigmoid(project(n, 1))).astype(bf16)
        for side in range(sides):
            gpad[side, pl.ds(pl.multiple_of(n * block + pad, pad), block), :] = glu[:, side * LANES : (side + 1) * LANES].astype(f32)

        @pl.when(n == 0)
        def _():
            hsend[0] = glu[:pad]

        @pl.when(n == inner - 1)
        def _():
            hsend[1] = glu[block - pad :]

        return carry

    lax.fori_loop(0, inner, glu_step, 0)
    def device_of(q):
        return (lax.div(q, tp) * tp + par, i, lax.rem(q, tp))

    has_before, has_after = place > 0, place < last
    start(remote(hsend.at[0], hrecv.at[1], r.hal_s.at[0], r.hal_r.at[1], device_of(jnp.maximum(place - 1, 0))), has_before)
    start(remote(hsend.at[1], hrecv.at[0], r.hal_s.at[1], r.hal_r.at[0], device_of(jnp.minimum(place + 1, last))), has_after)

    @pl.when(primary)
    def _():
        for copy in own_small:
            copy.wait()

    @pl.when(jnp.logical_not(primary))
    def _():
        for copy in mate_small:
            copy.wait_recv()

    deal_all(3, range(2, outer))
    taps, statc, stbuf = r.taps, r.statc, r.stbuf
    conv_rows = 64
    lane = lax.broadcasted_iota(jnp.int32, (conv_rows, LANES), 1)
    shift = pad - reach

    def conv_step(m, carry):
        s1 = s2 = 0.0
        for side in range(sides):
            total = jnp.zeros((conv_rows, LANES), f32)
            for residue in range(8):
                moved = gpad[side, pl.ds(m * conv_rows + residue, conv_rows + 2 * pad - 8), :]
                for j in range(KW):
                    at = j + shift - residue
                    if at % 8 == 0:
                        tap = taps[pl.ds(j, 1), pl.ds(side * LANES, LANES)]
                        total = total + tap * moved[at : at + conv_rows]
            conv[side, span(m, conv_rows), :] = total
            s1 = s1 + total
            s2 = s2 + total * total
        s1 = jnp.sum(s1, axis=-1, keepdims=True)
        s2 = jnp.sum(s2, axis=-1, keepdims=True)
        statc[span(m, conv_rows), :] = jnp.where(lane == 0, s1, jnp.where(lane == 1, s2, 0.0))
        return carry

    conv_steps = quarter // conv_rows
    lax.fori_loop(1, conv_steps // 2, conv_step, 0)
    deal_all(4, range(2))
    collect(2)
    lax.fori_loop(conv_steps // 2, conv_steps - 1, conv_step, 0)
    for edge, present, at in ((0, has_before, 0), (1, has_after, pad + quarter)):
        @pl.when(present)
        def _():
            remote(hrecv.at[edge], hrecv.at[edge], r.hal_s.at[0], r.hal_r.at[edge], (o, i, mate)).wait_recv()
            for side in range(sides):
                gpad[side, pl.ds(at, pad), :] = hrecv[edge, :, side * LANES : (side + 1) * LANES].astype(f32)

        @pl.when(jnp.logical_not(present))
        def _():
            for side in range(sides):
                gpad[side, pl.ds(at, pad), :] = jnp.zeros((pad, LANES), f32)

    lax.fori_loop(0, 2, lambda m, carry: conv_step(m * (conv_steps - 1), carry), 0)
    sums = r.sums
    two = pl.ds(0, 2)

    def sums_step(n, carry):
        sums[:, chunk(n)] = statc[chunk(n), :].T[: sums.shape[0]]
        return carry

    lax.fori_loop(0, inner, sums_step, 0)
    peers = []
    for dz in range(tp):
        for k in range(inner):
            if (dz, k) != (0, 0):
                peers.append((o if dz == 0 else twin, near[k]))
    for index, (plane_to, chip) in enumerate(peers):
        remote(sums.at[two, :], stbuf.at[head, two, :], r.sta_s, r.sta_r, (plane_to, chip, t)).start()
    deal_all(4, range(2, outer))
    lax.fori_loop(0, inner, key_step, 0)
    collect(3)
    lax.fori_loop(0, inner // 2, state_step, 0)

    def corner(n, d, column):
        end = block - 1 if d == 0 else 0
        at = n * block + end
        return colsv[pl.ds(at, 1), :][:, column : column + 1]

    totals = [[corner(n, d, 3 * d + 2) for n in range(inner)] for d in range(2)]
    levels = [[corner(n, d, 3 * d + 1) + totals[d][n] for n in range(inner)] for d in range(2)]
    for d in range(2):
        reaches = []
        for n in range(inner):
            later = range(n + 1, inner) if d == 0 else range(n)
            value = levels[d][n]
            for m in later:
                value = value + totals[d][m]
            reaches.append(value)
        top = functools.reduce(jnp.maximum, reaches)
        shares = [jnp.exp(v - top) for v in reaches]
        matx[d] = sum(shares[n] * cm[d, n] for n in range(inner)).astype(bf16)
        vec = sum(shares[n] * cv[d, n] for n in range(inner))
        row = lax.broadcasted_iota(jnp.int32, (8, HEAD), 0)
        decay = functools.reduce(jnp.add, totals[d])
        infox[d] = jnp.where(row == 0, vec, jnp.where(row == 1, top, decay))

    start(remote(matx, smat, r.mat_s.at[0], r.mat_r.at[0], (o, i, mate)))
    start(remote(infox, sinfo, r.inf_s.at[0], r.inf_r.at[0], (o, i, mate)))
    received(stbuf.at[pl.ds(0, MEMORY_HEADS - 1), two, :], r.sta_r)
    stbuf[head] = sums[...]

    def stat_step(n, carry):
        whole = stbuf[0, :, chunk(n)]
        for k in range(1, MEMORY_HEADS):
            whole = whole + stbuf[k, :, chunk(n)]
        whole = whole * (1.0 / channels)
        mean = whole[0:1]
        rstd = lax.rsqrt(whole[1:2] - mean * mean + EPS)
        wide = jnp.concatenate([mean, rstd, jnp.zeros((LANES - 2, block), f32)], axis=0)
        statc[chunk(n), :] = wide.T
        return carry

    lax.fori_loop(0, inner, stat_step, 0)
    actb, memb, cin = r.actb, r.memb, r.cin

    def give(which, source, b):
        return remote(
            source.at[chunk(b), :], cin.at[which, i], r.ret_s.at[which, b], r.ret_r.at[which, i],
            (plane, b, par),
        )

    def give_own(which, source):
        return local(source.at[chunk(i), :], cin.at[which, i], r.rel_s.at[which])

    def give_rows(which, source, b):
        to_self = jnp.logical_and(primary, b == i)
        guarded(to_self, give_own(which, source).start)
        guarded(jnp.logical_not(to_self), give(which, source, b).start)

    def turn(step):
        k = inner - 1 - step
        flip_x, flip_y = lax.rem(k, 2), lax.div(k, 2)
        return (y + flip_y - 2 * y * flip_y) * 2 + x + flip_x - 2 * x * flip_x

    def act_step(n, carry):
        for half_at in range(2):
            rows = pl.ds(pl.multiple_of(n * block + half_at * (block // 2), block // 2), block // 2)
            cols = statc[rows, :]
            for side in range(sides):
                lanes = pl.ds(side * LANES, LANES)
                normal = (conv[side, rows, :] - cols[:, 0:1]) * cols[:, 1:2] * r.lng[:, lanes] + r.lnb[:, lanes]
                actb[rows, lanes] = (normal * jax.nn.sigmoid(normal)).astype(bf16)
        return carry

    lax.fori_loop(0, inner, act_step, 0)

    mat_rows = gin.at[span(t, HEAD // tp), :]
    mate_rows = gin.at[span(mate, HEAD // tp), :]
    remote(matx, smat, r.mat_s.at[0], r.mat_r.at[0], (o, i, mate)).wait_recv()
    remote(infox, sinfo, r.inf_s.at[0], r.inf_r.at[0], (o, i, mate)).wait_recv()
    ours, theirs = infox[grp], sinfo[grp]
    is_far = t == grp
    our_reach = ours[1:2, 0:1] + jnp.where(is_far, theirs[2:3, 0:1], 0.0)
    their_reach = theirs[1:2, 0:1] + jnp.where(is_far, 0.0, ours[2:3, 0:1])
    group_level = jnp.maximum(our_reach, their_reach)
    our_share, their_share = jnp.exp(our_reach - group_level), jnp.exp(their_reach - group_level)
    gmat[...] = (our_share * matx[grp].astype(f32) + their_share * smat[grp].astype(f32)).astype(bf16)
    state_row = lax.broadcasted_iota(jnp.int32, (8, HEAD), 0)
    ginfo[...] = jnp.where(state_row == 0, our_share * ours[0:1] + their_share * theirs[0:1], group_level)
    across = ((1 - grp) * tp + par, i, t)
    start(remote(gmat.at[span(t, HEAD // tp), :], mat_rows, r.mat_s.at[1], r.mat_r.at[1], across))
    start(remote(ginfo, gininfo, r.inf_s.at[1], r.inf_r.at[1], across))
    for k in range(inner - 1, -1, -1):
        give_rows(0, actb, near[k])
    nvs, levs = r.nvs, r.levs
    for d in range(2):
        by_mate = t == 1 - d
        level = jnp.where(by_mate, sinfo[d][1:2, 0:1], LOW_START)
        present = jnp.where(by_mate, 1.0, 0.0)
        mat = present * smat[d].astype(f32)
        vec = present * sinfo[d][0:1]
        for n in (range(inner) if d == 0 else range(inner - 1, -1, -1)):
            high = mat.astype(bf16)
            r.cst[d, n, pl.ds(0, HEAD), :] = high
            r.cst[d, n, pl.ds(HEAD, HEAD), :] = (mat - high.astype(f32)).astype(bf16)
            nvs[d, n] = jnp.broadcast_to(vec, (8, HEAD))
            levs[d, n] = jnp.broadcast_to(level, (8, LANES))
            carried = level + totals[d][n]
            new_level = jnp.maximum(carried, levels[d][n])
            kept, added = jnp.exp(carried - new_level), jnp.exp(levels[d][n] - new_level)
            mat = kept * mat + added * cm[d, n]
            vec = kept * vec + added * cv[d, n][0:1]
            level = new_level

    first_group = grp == 0

    def along(values):
        return jnp.concatenate([jnp.broadcast_to(v, (1, block)) for v in values], axis=1)

    kept, tops = [], []
    for d in range(2):
        running, decay = rowsv[pl.ds(3 * d + 1, 1), :], rowsv[pl.ds(3 * d + 2, 1), :]
        level = along([levs[d, n][0:1, 0:1] for n in range(inner)])
        top = jnp.maximum(running, level)
        tops.append((top, decay))
        kept.append([jnp.exp(running - top), jnp.exp(level - top), jnp.exp(-top - decay)])
    alone = [jnp.where(first_group, a, b) for a, b in zip(*kept)]
    joined = [jnp.where(first_group, b, a) for a, b in zip(*kept)]
    joined_top, joined_decay = (jnp.where(first_group, b, a) for a, b in zip(*tops))
    r.colw[:, pl.ds(0, 8)] = jnp.concatenate(alone + joined + [jnp.zeros((2, quarter), f32)], axis=0).T
    collect(4)

    pair = 2

    def query_step(m, carry):
        ns = [m * pair + p for p in range(pair)]
        queries = [project(n, 4).astype(bf16) for n in ns]
        scores = [
            lax.dot_general(q, kb[chunk(n), :], (((1,), (1,)), ((), ())), preferred_element_type=f32)
            for n, q in zip(ns, queries)
        ]
        for n, q in zip(ns, queries):
            r.qb[chunk(n), :] = q
        for role, d in ((0, grp), (1, 1 - grp)):
            for n, q, score in zip(ns, queries, scores):
                cols = r.colw[chunk(n), :]
                local_weight, carry_weight = cols[:, 3 * role : 3 * role + 1], cols[:, 3 * role + 1 : 3 * role + 2]
                part = score * r.wgt[d, n]
                num = jnp.dot(part.astype(bf16), vb[chunk(n), :], preferred_element_type=f32)
                far = jnp.dot(jnp.concatenate([q, q], axis=1), r.cst[d, n], preferred_element_type=f32)
                num = local_weight * num + carry_weight * far
                far_sum = jnp.sum(q.astype(f32) * nvs[d, n][0:1], axis=-1, keepdims=True)
                den = local_weight * jnp.sum(part, axis=-1, keepdims=True) + carry_weight * far_sum
                if role == 0:
                    r.alone[chunk(n), :] = num * (1.0 / jnp.maximum(jnp.abs(den), cols[:, 2:3]))
                else:
                    r.numj[chunk(n), :] = num
                    r.denj[chunk(n), :] = jnp.broadcast_to(den, (block, LANES))
        return carry

    lax.fori_loop(0, inner // pair // 2, query_step, 0)
    remote(mat_rows, mat_rows, r.mat_s.at[1], r.mat_r.at[1], (o, i, mate)).wait_recv()
    start(remote(mat_rows, mat_rows, r.mat_s.at[2], r.mat_r.at[2], (o, i, mate)))
    lax.fori_loop(inner // pair // 2, inner // pair, query_step, 0)
    remote(ginfo, gininfo, r.inf_s.at[1], r.inf_r.at[1], (o, i, mate)).wait_recv()
    remote(mate_rows, mate_rows, r.mat_s.at[2], r.mat_r.at[2], (o, i, mate)).wait_recv()

    arriving = gininfo[1:2, 0:1] + jnp.where(t == grp, sinfo[1 - grp][2:3, 0:1], 0.0)
    group_levels = []
    for n in range(inner):
        lost_f = functools.reduce(jnp.add, totals[0][:n], jnp.zeros((1, 1), f32))
        lost_b = functools.reduce(jnp.add, totals[1][n + 1 :], jnp.zeros((1, 1), f32))
        group_levels.append(arriving + jnp.where(first_group, lost_b, lost_f))
    level = along(group_levels)
    top = jnp.maximum(joined_top, level)
    kept = [jnp.exp(joined_top - top), jnp.exp(level - top), jnp.exp(-top - joined_decay)]
    r.colw[:, pl.ds(0, 8)] = jnp.concatenate(kept + [jnp.zeros((5, quarter), f32)], axis=0).T

    def memory_rows(ns):
        queries = [r.qb[chunk(n), :] for n in ns]
        fars = [jnp.dot(q, gin[...], preferred_element_type=f32) for q in queries]
        far_sums = [jnp.sum(q.astype(f32) * gininfo[0:1], axis=-1, keepdims=True) for q in queries]
        for n, far, far_sum in zip(ns, fars, far_sums):
            cols = r.colw[chunk(n), :]
            den = cols[:, 0:1] * r.denj[chunk(n), pl.ds(0, 1)] + cols[:, 1:2] * far_sum
            share_of = 1.0 / jnp.maximum(jnp.abs(den), cols[:, 2:3])
            out = r.alone[chunk(n), :] + (
                r.numj[chunk(n), :] * (cols[:, 0:1] * share_of) + far * (cols[:, 1:2] * share_of)
            )
            level = lax.rsqrt(jnp.mean(out * out, axis=-1, keepdims=True) + EPS)
            memb[chunk(n), :] = (out * level * r.mgn[...]).astype(bf16)
        for n in ns:
            give_rows(1, memb, n)

    for ns in ([near[3]], [near[2]], [near[1], near[0]]):
        memory_rows(ns)
    acc, pbuf = r.acc, r.pbuf
    tile = 512
    tiles = model // tile

    def take(which, k):
        def hear():
            rows = cin.at[which, near[k]]
            remote(rows, rows, r.ret_s.at[which, 0], r.ret_r.at[which, near[k]], (o, i, mate)).wait_recv()

        if k:
            hear()
        else:
            guarded(jnp.logical_not(primary), hear)
            guarded(primary, give_own(which, actb).wait)

    def part(which, n):
        return sum(
            jnp.dot(cin[which, k], ow[which, pl.ds(k * HEAD, HEAD), span(n, tile)], preferred_element_type=f32)
            for k in range(inner)
        )

    def conv_out_step(n, carry):
        acc[:, span(n, tile)] = part(0, n)
        return carry

    for copy in out_in:
        copy.wait()
    for k in range(inner):
        take(0, k)
    lax.fori_loop(0, tiles, conv_out_step, 0)

    def add_step(k):
        def step(n, carry):
            rows = pl.ds(pl.multiple_of(near[k] * HEAD, HEAD), HEAD)
            acc[:, span(n, tile)] += jnp.dot(
                cin[1, near[k]], ow[1, rows, span(n, tile)], preferred_element_type=f32
            )
            return carry
        return step

    for k in range(inner - 1, 0, -1):
        take(1, k)
        lax.fori_loop(0, tiles, add_step(k), 0)
    take(1, 0)
    out_own, out_mate = r.out_own, r.out_mate

    def piece(n):
        return remote(
            pbuf.at[span(mate, hb), span(n, tile)], out_mate.at[:, span(n, tile)],
            r.fin_s, r.fin_r, (o, i, mate),
        )

    def stay(n):
        return local(pbuf.at[span(t, hb), span(n, tile)], out_own.at[:, span(n, tile)], r.fil_s)

    def mem_out_step(n, carry):
        rows = pl.ds(pl.multiple_of(i * HEAD, HEAD), HEAD)
        rest = jnp.dot(cin[1, i], ow[1, rows, span(n, tile)], preferred_element_type=f32)
        pbuf[:, span(n, tile)] = (acc[:, span(n, tile)] + rest).astype(bf16)
        piece(n).start()
        stay(n).start()
        return carry

    lax.fori_loop(0, tiles, mem_out_step, 0)

    for copy, when in sends:
        if when is None:
            copy.wait_send()
        else:
            pl.when(when)(copy.wait_send)


    received(stbuf.at[pl.ds(0, MEMORY_HEADS - 1), two, :], r.sta_s)

    @pl.when(primary)
    def _():
        for copy in mate_small:
            copy.wait_send()
        for j in range(count):
            received(wst.at[j] if j in by_second else wst.at[j, pl.ds(0, inner - 1)], r.w2_s.at[j])
            if j not in by_second:
                received(wfull.at[j], r.fw_s.at[j])

    @pl.when(jnp.logical_not(primary))
    def _():
        for j in by_second:
            received(wfull.at[j], r.fw_s.at[j])

    for which, source in ((0, actb), (1, memb)):
        for b in range(inner):
            guarded(jnp.logical_not(jnp.logical_and(primary, i == b)), give(which, source, b).wait_send)
    local(out_own, out_own, r.fil_s).wait()
    received(out_mate, r.fin_s)
    received(out_mate, r.fin_r)


LANES = 128
LOW_START = -1e30


def whole_layer(outer, inner, tp, args):
    tokens = args.tokens
    block, half = tokens.shape
    depth = args.glu_value.shape[0]
    count = 5
    quarter, model = inner * block, half * tp
    hb = block // tp
    pad = 16
    f32, bf16 = jnp.float32, jnp.bfloat16
    dma = pltpu.SemaphoreType.DMA
    tiles = model // 512
    extra = args.log_decay_extra.T
    operands = dict(
        tokens=tokens, norm_gain=args.norm_gain[None],
        glu_value=args.glu_value, glu_gate=args.glu_gate,
        key_weight=args.key_weight, value_weight=args.value_weight, query_weight=args.query_weight,
        conv_taps=args.conv_taps, ln_gain=args.ln_gain[None], ln_bias=args.ln_bias[None],
        gate_weight=args.gate_weight.T, gate_bias=args.gate_bias[None],
        extra=extra, mem_gain=args.mem_gain[None],
        out_conv=args.out_conv, out_mem=args.out_mem,
    )
    scratch = dict(
        nq=pltpu.VMEM((quarter, model), bf16),
        nsrc=pltpu.VMEM((hb, model), bf16),
        xin=pltpu.VMEM((tp, hb, half), bf16),
        wst=pltpu.VMEM((count, outer, depth, half), bf16),
        wfull=pltpu.VMEM((count, model, HEAD), bf16),
        wmv=pltpu.VMEM((2, depth, half), bf16),
        ow=pltpu.VMEM((2,) + args.out_conv.shape, bf16),
        taps=pltpu.VMEM((KW, HEAD), f32), lng=pltpu.VMEM((1, HEAD), f32),
        lnb=pltpu.VMEM((1, HEAD), f32), mgn=pltpu.VMEM((1, HEAD), f32),
        ext=pltpu.VMEM((inner,) + extra.shape, f32),
        gwp=pltpu.VMEM((LANES, model), bf16),
        gain=pltpu.VMEM((1, model), f32), bias=pltpu.VMEM((1, 4 * MEMORY_HEADS), f32),
        gt=pltpu.VMEM((4 * MEMORY_HEADS, quarter), f32),
        rowsv=pltpu.VMEM((8, quarter), f32), colsv=pltpu.VMEM((quarter, LANES), f32),
        gpad=pltpu.VMEM((HEAD // LANES, quarter + 2 * pad, LANES), f32),
        conv=pltpu.VMEM((HEAD // LANES, quarter, LANES), f32), gval=pltpu.VMEM((quarter, HEAD), f32),
        hsend=pltpu.VMEM((2, pad, HEAD), bf16), hrecv=pltpu.VMEM((2, pad, HEAD), bf16),
        statc=pltpu.VMEM((quarter, LANES), f32), sums=pltpu.VMEM((8, quarter), f32),
        stbuf=pltpu.VMEM((MEMORY_HEADS, 8, quarter), f32),
        kb=pltpu.VMEM((quarter, HEAD), bf16), vb=pltpu.VMEM((quarter, HEAD), bf16),
        cm=pltpu.VMEM((2, inner, HEAD, HEAD), f32), cv=pltpu.VMEM((2, inner, 8, HEAD), f32),
        matx=pltpu.VMEM((2, HEAD, HEAD), bf16), infox=pltpu.VMEM((2, 8, HEAD), f32),
        smat=pltpu.VMEM((2, HEAD, HEAD), bf16), sinfo=pltpu.VMEM((2, 8, HEAD), f32),
        gmat=pltpu.VMEM((HEAD, HEAD), bf16), ginfo=pltpu.VMEM((8, HEAD), f32),
        gin=pltpu.VMEM((HEAD, HEAD), bf16), gininfo=pltpu.VMEM((8, HEAD), f32),
        cst=pltpu.VMEM((2, inner, 2 * HEAD, HEAD), bf16), qb=pltpu.VMEM((quarter, HEAD), bf16), kwt=pltpu.VMEM((2, HEAD, quarter), bf16),
        alone=pltpu.VMEM((quarter, HEAD), f32), numj=pltpu.VMEM((quarter, HEAD), f32), denj=pltpu.VMEM((quarter, LANES), f32),
        wgt=pltpu.VMEM((2, inner, block, block), f32), colw=pltpu.VMEM((quarter, LANES), f32),
        nvs=pltpu.VMEM((2, inner, 8, HEAD), f32), levs=pltpu.VMEM((2, inner, 8, LANES), f32),
        actb=pltpu.VMEM((quarter, HEAD), bf16), memb=pltpu.VMEM((quarter, HEAD), bf16),
        cin=pltpu.VMEM((2, inner, block, HEAD), bf16),
        acc=pltpu.VMEM((block, model), f32), pbuf=pltpu.VMEM((block, model), bf16),
        own_s=dma((count,)), mov_s=dma((2,)), mov_r=dma((2,)), mvd_s=dma((2,)), loc_s=dma((7,)), xin_s=dma, xin_r=dma,
        w1_s=dma((count, outer // tp)), w1_r=dma((count, outer)),
        sml_s=dma((4,)), prm_s=dma((4,)), prm_r=dma((4,)),
        ext_s=dma((inner,)), ext_r=dma((inner,)),
        tok_s=dma((2, 2)), tok_r=dma((inner, tp, 2)), pas_s=dma, clear=pltpu.SemaphoreType.REGULAR,
        w2_s=dma((count,)), w2_r=dma((count, outer)),
        keep_s=dma((count,)), fw_s=dma((count,)), fw_r=dma((count,)),
        hal_s=dma((2,)), hal_r=dma((2,)),
        sta_s=dma, sta_r=dma,
        mat_s=dma((3,)), mat_r=dma((3,)), inf_s=dma((2,)), inf_r=dma((2,)),
        ret_s=dma((2, inner)), ret_r=dma((2, inner)), rel_s=dma((2,)),
        fin_s=dma, fin_r=dma, fil_s=dma,
    )
    any_space = pl.BlockSpec(memory_space=pl.ANY)
    spaces = {n: any_space for n in operands}
    names = list(operands) + ["out_own", "out_mate"] + list(scratch)
    shape = pltpu.VMEM((hb, model), bf16)
    own, mate = pl.pallas_call(
        functools.partial(layer_kernel, outer, inner, tp, names),
        out_shape=(shape, shape),
        in_specs=[spaces[n] for n in operands],
        out_specs=(any_space, any_space),
        scratch_shapes=list(scratch.values()),
        compiler_params=pltpu.CompilerParams(
            collective_id=0, has_side_effects=True, vmem_limit_bytes=60 * 2**20
        ),
    )(*operands.values())
    return (own.astype(f32) + mate.astype(f32)).astype(bf16)


def gather_inputs(tokens, weights, extra, inner):
    rows, half = tokens.shape
    gathered = lax.all_gather(tokens, ("inner", "tp"), axis=0)
    tp = gathered.shape[0] // inner
    whole = jnp.transpose(gathered.reshape(inner, tp, rows, half), (0, 2, 1, 3))
    whole = whole.reshape(inner * rows, tp * half)
    depth, columns = weights[0].shape
    width = columns // inner
    packed = jnp.stack([w.reshape(depth, inner, width) for w in weights], axis=2)
    packed = jnp.transpose(packed, (1, 0, 2, 3)).reshape(inner, depth, len(weights) * width)
    if inner > 1:
        packed = lax.all_to_all(packed, "inner", split_axis=0, concat_axis=0, tiled=True)
    pieces = lax.all_gather(packed.reshape(inner * depth, -1), "outer", axis=0, tiled=True)
    pieces = pieces.reshape(-1, len(weights), width).transpose(1, 0, 2)
    extras = lax.all_gather(extra, "inner", axis=0, tiled=True) if inner > 1 else extra
    return whole, pieces, extras.T


def local_state(keys, values, shifted, level, total, scale):
    weight = jnp.exp(shifted - level[:, None]) * scale
    weighted = keys.astype(jnp.float32) * weight[:, :, None]
    mat = jnp.einsum(
        "hsd,hse->hde", weighted.astype(jnp.bfloat16), values, preferred_element_type=jnp.float32
    )
    return mat, jnp.sum(weighted, axis=1), level + total, total


def packed_state(mat, vec, level, decay):
    spread = lambda x: jnp.broadcast_to(x[:, None], vec.shape)
    rows = parts_of(vec) + parts_of(spread(level)) + parts_of(spread(decay))
    pad = [jnp.zeros_like(rows[0])] * 7
    return jnp.concatenate([mat.astype(jnp.bfloat16), jnp.stack(rows + pad, axis=1)], axis=1)


def incoming(states, reverse):
    count = states.shape[0]
    mats = states[:, :, :HEAD]
    rows = states[:, :, HEAD:]
    vecs = whole_of(rows[:, :, 0], rows[:, :, 1], rows[:, :, 2])
    levels = whole_of(rows[:, :, 3, 0], rows[:, :, 4, 0], rows[:, :, 5, 0])
    decays = whole_of(rows[:, :, 6, 0], rows[:, :, 7, 0], rows[:, :, 8, 0])
    place = lax.axis_index("outer")
    order = jnp.arange(count)
    if reverse:
        ahead = (order > place)[:, None]
        between = (order[None, :] < order[:, None]) & (order[None, :] > place)
    else:
        ahead = (order < place)[:, None]
        between = (order[None, :] > order[:, None]) & (order[None, :] < place)
    lost = jnp.sum(jnp.where(between[:, :, None], decays[None], 0.0), axis=1)
    reach = jnp.where(ahead, levels + lost, -1e30)
    level = jnp.max(reach, axis=0)
    share = jnp.where(ahead, jnp.exp(reach - level[None]), 0.0)
    mat = jnp.sum(share[:, :, None, None] * mats.astype(jnp.float32), axis=0)
    vec = jnp.sum(share[:, :, None] * vecs, axis=0)
    return mat, vec, level


def finish(query_wide, num, den, running, decay, state):
    mat, vec, level = state
    top = jnp.maximum(running, level[:, None])
    local_weight = jnp.exp(running - top)
    carry_weight = jnp.exp(level[:, None] - top)
    num = local_weight[:, :, None] * num + carry_weight[:, :, None] * jnp.einsum(
        "htd,hde->hte", query_wide, mat, precision=PRECISE
    )
    den = local_weight * den + carry_weight * jnp.einsum(
        "htd,hd->ht", query_wide, vec, precision=PRECISE
    )
    return num / jnp.maximum(jnp.abs(den), jnp.exp(-top - decay))[:, :, None]


def make_shards(inner, outer, tp):
    def own(array, dim):
        size = array.shape[dim] // inner
        return lax.dynamic_slice_in_dim(array, lax.axis_index("inner") * size, size, dim)

    def shards(
        tokens,
        norm_gain,
        glu_value,
        glu_gate,
        conv_taps,
        ln_gain,
        ln_bias,
        query_weight,
        key_weight,
        value_weight,
        gate_weight,
        gate_bias,
        log_decay_extra,
        mem_gain,
        out_conv,
        out_mem,
    ):
        fits = tp == 2 and inner == 4 and outer == 2 * tp and inner * tp == MEMORY_HEADS
        if fits and tokens.shape[1] == inner * HEAD and conv_taps.shape[1] == inner * HEAD:
            return whole_layer(outer, inner, tp, types.SimpleNamespace(
                tokens=tokens, norm_gain=norm_gain, glu_value=glu_value, glu_gate=glu_gate,
                conv_taps=conv_taps, ln_gain=ln_gain, ln_bias=ln_bias, query_weight=query_weight,
                key_weight=key_weight, value_weight=value_weight, gate_weight=gate_weight,
                gate_bias=gate_bias, log_decay_extra=log_decay_extra, mem_gain=mem_gain,
                out_conv=out_conv, out_mem=out_mem,
            ))
        taps, gain, bias, mgain = own(conv_taps, 1), own(ln_gain, 0), own(ln_bias, 0), own(mem_gain, 0)
        channels = conv_taps.shape[1] * tp
        width = gain.shape[0]
        heads = mgain.shape[0] // HEAD
        first = (lax.axis_index("tp") * inner + lax.axis_index("inner")) * heads
        stacked = (query_weight, key_weight, value_weight, glu_value, glu_gate)
        whole, weights, extras = gather_inputs(tokens, stacked, log_decay_extra, inner)
        rows = whole.shape[0]
        wide = whole.astype(jnp.float32)
        normed = (
            wide * lax.rsqrt(jnp.mean(wide * wide, axis=-1, keepdims=True) + EPS) * norm_gain
        ).astype(jnp.bfloat16)
        own_gate = lax.dynamic_slice_in_dim(
            gate_weight.reshape(-1, 4, MEMORY_HEADS), first, heads, 2
        )
        own_bias = lax.dynamic_slice_in_dim(gate_bias.reshape(4, MEMORY_HEADS), first, heads, 1)
        gates = lax.dot_general(
            own_gate.reshape(-1, 4 * heads), normed, (((0,), (1,)), ((), ())),
            preferred_element_type=jnp.float32,
        ).reshape(4, heads, rows) + own_bias[:, :, None]
        own_extra = lax.dynamic_slice_in_dim(
            extras.reshape(2, MEMORY_HEADS, rows), first, heads, 1
        )
        lf = jax.nn.log_sigmoid(gates[1::2]) + own_extra
        at = jnp.arange(rows)
        causal = at[:, None] >= at[None, :]
        anti = at[:, None] <= at[None, :]

        def total(x, mask):
            return jnp.sum(jnp.where(mask, x[:, None, :], 0.0), axis=-1)

        def highest(x, mask):
            return jnp.max(jnp.where(mask, x[:, None, :], -jnp.inf), axis=-1)

        decay_f = total(lf[0], causal)
        decay_b = total(lf[1], anti)
        shifted_f = gates[0] - decay_f
        shifted_b = gates[2] - decay_b
        running_f = highest(shifted_f, causal)
        running_b = highest(shifted_b, anti)

        def project(i):
            return jnp.dot(normed, weights[i], preferred_element_type=jnp.float32)

        def heads_first(x):
            return jnp.transpose(x.reshape(rows, heads, HEAD), (1, 0, 2)).astype(jnp.bfloat16)

        keys = heads_first(project(1))
        values = heads_first(project(2))
        scale = HEAD ** (-0.5)
        state_f = local_state(
            keys, values, shifted_f, running_f[:, -1], decay_f[:, -1], scale
        )
        state_b = local_state(keys, values, shifted_b, running_b[:, 0], decay_b[:, 0], scale)
        sent = jnp.stack([packed_state(*state_f), packed_state(*state_b)])
        states = lax.all_gather(sent, "outer", axis=0)

        glu = (project(3) * jax.nn.sigmoid(project(4))).astype(jnp.bfloat16)
        reach = KW // 2
        before = lax.ppermute(glu[rows - reach :], "outer", [(i, i + 1) for i in range(outer - 1)])
        after = lax.ppermute(glu[:reach], "outer", [(i + 1, i) for i in range(outer - 1)])
        queries = heads_first(project(0))

        scores = jnp.einsum("htd,hsd->hts", queries, keys, preferred_element_type=jnp.float32) * scale

        def local_out(shifted, running, mask):
            weight = jnp.where(
                mask, jnp.exp(jnp.minimum(shifted[:, None, :] - running[:, :, None], 0.0)), 0.0
            )
            part = scores * weight
            num = jnp.einsum(
                "hts,hse->hte", part.astype(jnp.bfloat16), values,
                preferred_element_type=jnp.float32,
            )
            return num, jnp.sum(part, axis=-1)

        num_f, den_f = local_out(shifted_f, running_f, causal)
        num_b, den_b = local_out(shifted_b, running_b, anti)

        padded = jnp.concatenate([before, glu, after], axis=0).astype(jnp.float32)
        conv = jnp.zeros(glu.shape, jnp.float32)
        for offset in range(KW):
            conv = conv + taps[offset] * padded[offset : offset + rows]
        sums = jnp.stack([jnp.sum(conv, axis=-1), jnp.sum(conv * conv, axis=-1)])
        sums = lax.psum(sums, ("inner", "tp")) / channels
        chan_mean = sums[0]
        chan_var = sums[1] - chan_mean * chan_mean
        normal = (conv - chan_mean[:, None]) * lax.rsqrt(chan_var + EPS)[:, None] * gain + bias
        act = (normal * jax.nn.sigmoid(normal)).astype(jnp.bfloat16)

        query_wide = queries.astype(jnp.float32)
        forward = finish(query_wide, num_f, den_f, running_f, decay_f, incoming(states[:, 0], False))
        backward = finish(query_wide, num_b, den_b, running_b, decay_b, incoming(states[:, 1], True))
        summed = forward + backward
        head_norm = summed * lax.rsqrt(jnp.mean(summed * summed, axis=-1, keepdims=True) + EPS)
        head_norm = head_norm * mgain.reshape(heads, HEAD)[:, None, :]
        memory = jnp.transpose(head_norm, (1, 0, 2)).reshape(rows, heads * HEAD).astype(jnp.bfloat16)

        def back(x):
            if inner == 1:
                return x
            return lax.all_to_all(x, "inner", split_axis=0, concat_axis=1, tiled=True)

        result = jnp.dot(back(act), out_conv, preferred_element_type=jnp.float32)
        result = result + jnp.dot(back(memory), out_mem, preferred_element_type=jnp.float32)
        return lax.psum_scatter(
            result.astype(jnp.bfloat16), "tp", scatter_dimension=0, tiled=True
        )

    return shards


def solution(mesh):
    sp, tp = mesh.shape["sp"], mesh.shape["tp"]
    inner = math.gcd(sp, max(MEMORY_HEADS // tp, 1))
    outer = sp // inner
    fine = Mesh(mesh.devices.reshape(outer, inner, tp), ("outer", "inner", "tp"))
    rows = ("outer", "inner")
    in_specs = (
        P(rows, "tp"),
        P(),
        P(rows, "tp"),
        P(rows, "tp"),
        P(None, "tp"),
        P("tp"),
        P("tp"),
        P(rows, "tp"),
        P(rows, "tp"),
        P(rows, "tp"),
        P(),
        P(),
        P(rows, None),
        P("tp"),
        P("tp", None),
        P("tp", None),
    )
    return jax.shard_map(
        make_shards(inner, outer, tp), mesh=fine, in_specs=in_specs,
        out_specs=P(("outer", "inner", "tp"), None), check_vma=False,
    )
```

```python
import functools
import math
import types

import jax
import jax.numpy as jnp
from jax import lax
from jax.experimental import pallas as pl
from jax.experimental.pallas import tpu as pltpu
from jax.sharding import Mesh, PartitionSpec as P

MEMORY_HEADS = 8
HEAD = 256
KW = 31

EPS = 1e-06
PRECISE = lax.Precision.HIGHEST


def parts_of(x):
    first = lax.reduce_precision(x, 8, 7)
    rest = x - first
    second = lax.reduce_precision(rest, 8, 7)
    third = rest - second
    return [p.astype(jnp.bfloat16) for p in (first, second, third)]


def whole_of(a, b, c):
    return a.astype(jnp.float32) + b.astype(jnp.float32) + c.astype(jnp.float32)


MESH = pl.DeviceIdType.MESH


def layer_kernel(outer, inner, tp, names, *refs):
    r = types.SimpleNamespace(**dict(zip(names, refs)))
    tokens, norm_gain = r.tokens, r.norm_gain
    weights = [r.glu_value, r.glu_gate, r.key_weight, r.value_weight, r.query_weight]
    count = len(weights)
    o, i, t = lax.axis_index("outer"), lax.axis_index("inner"), lax.axis_index("tp")
    block, half = tokens.shape
    depth = weights[0].shape[0]
    hb = block // tp
    quarter = inner * block
    groups = outer // tp
    model = half * tp
    channels = MEMORY_HEADS * HEAD
    scale = HEAD ** (-0.5)
    f32, bf16 = jnp.float32, jnp.bfloat16

    par, grp = lax.rem(o, tp), lax.div(o, tp)
    mate = 1 - t
    twin = o + 1 - 2 * par
    primary = t == par
    place = grp * tp + t
    last = outer - 1
    x, y = lax.rem(i, 2), lax.div(i, 2)
    near = [i, y * 2 + 1 - x, (1 - y) * 2 + x, (1 - y) * 2 + 1 - x]
    head = par * inner + i

    nq, nsrc, xin, wst, wfull, ow = r.nq, r.nsrc, r.xin, r.wst, r.wfull, r.ow

    def span(index, size):
        return pl.ds(pl.multiple_of(index * size, size), size)

    def remote(src, dst, send, recv, device):
        return pltpu.make_async_remote_copy(
            src_ref=src, dst_ref=dst, send_sem=send, recv_sem=recv,
            device_id=device, device_id_type=MESH,
        )

    sends = []

    def start(copy, when=None):
        if when is None:
            copy.start()
        else:
            pl.when(when)(copy.start)
        sends.append((copy, when))

    def guarded(when, action):
        pl.when(when)(action)

    local = pltpu.make_async_copy

    own_rows = [local(weights[j], wst.at[j, o], r.own_s.at[j]) for j in range(count)]
    tok_own = local(tokens.at[span(t, hb), :], xin.at[t], r.loc_s.at[0])
    tok_own.start()
    gain_in = local(norm_gain, r.gain, r.loc_s.at[5])
    bias_in = local(r.gate_bias, r.bias, r.loc_s.at[6])
    gain_in.start()
    bias_in.start()

    for copy in own_rows:
        copy.start()

    gate_in = local(r.gate_weight, r.gwp.at[pl.ds(0, r.gate_weight.shape[0]), :], r.loc_s.at[1])
    out_in = [
        local(source, ow.at[k], r.loc_s.at[2 + k]) for k, source in enumerate((r.out_conv, r.out_mem))
    ]

    barrier = pltpu.get_barrier_semaphore()
    greeted = []
    for dz in range(tp):
        for k in range(inner):
            for c in range(tp):
                if (dz, k, c) != (0, 0, 0):
                    greeted.append((o if dz == 0 else twin, near[k], t if c == 0 else mate))
    for step in range(1, groups):
        away = lax.rem(grp + step, groups) * tp
        for dz in range(tp):
            for c in range(tp):
                greeted.append((away + dz, i, c))
    for device in greeted:
        pl.semaphore_signal(barrier, inc=1, device_id=device, device_id_type=MESH)
    pl.semaphore_wait(barrier, len(greeted))

    start(remote(tokens.at[span(mate, hb), :], xin.at[t], r.xin_s, r.xin_r, (o, i, mate)))

    def spread(j, step):
        target = lax.rem(grp + step, groups) * tp + t
        return remote(
            wst.at[j, o], wst.at[j, o], r.w1_s.at[j, step], r.w1_r.at[j, o], (target, i, t)
        )

    moved = (1, 3)

    def plane_of(step):
        return lax.rem(grp + step, groups) * tp

    def hand_over(j):
        at = moved.index(j)
        return remote(wst.at[j, o], r.wmv.at[at], r.mov_s.at[at], r.mov_r.at[at], (o, i, mate))

    def spread_all(j, phase):
        for step in range(groups):
            target = lax.rem(grp + step, groups) * tp + t
            apart = (target - o) * (twin - o) < 0
            if phase == 0:
                when = jnp.logical_and(apart, jnp.logical_not(primary))
            elif phase == 1:
                when = jnp.logical_not(apart)
                if step == 0:
                    when = jnp.logical_and(when, jnp.logical_not(primary))
            else:
                when = jnp.logical_and(apart, primary)
            if step and phase == 1 and j in moved:
                start(spread(j, step), jnp.logical_and(when, primary))
                other = plane_of(step) + mate
                at_end = jnp.logical_and(primary, (other - o) * (twin - o) > 0)

                @pl.when(at_end)
                def _():
                    hand_over(j).wait_recv()

                start(remote(
                    r.wmv.at[moved.index(j)], wst.at[j, o], r.mvd_s.at[moved.index(j)], r.w1_r.at[j, o], (other, i, mate)
                ), at_end)
            elif step or phase == 1:
                start(spread(j, step), when)

    def arrived(j, plane):
        remote(wst.at[j, plane], wst.at[j, plane], r.w1_s.at[j, 0], r.w1_r.at[j, plane], (o, i, mate)).wait_recv()

    def row_block(owner_plane, owner):
        return pl.ds(pl.multiple_of((owner_plane * inner + owner) * depth, depth), depth)

    by_second = (4,)

    def keep(j, plane_at):
        return local(
            wst.at[j, plane_at, :, span(i, HEAD)], wfull.at[j, row_block(plane_at, i), :], r.keep_s.at[j]
        )

    def deal(j, plane_at, k):
        return remote(
            wst.at[j, plane_at, :, span(near[k], HEAD)],
            wfull.at[j, row_block(plane_at, i), :],
            r.w2_s.at[j], r.w2_r.at[j, plane_at], (o, near[k], mate if j in by_second else t),
        )

    def deal_planes(j):
        base = plane_of(1)
        nearer, farther = base + jnp.where(base < o, 1, 0), base + jnp.where(base < o, 0, 1)
        at_end = (nearer - o) * (twin - o) > 0
        return [o, jnp.where(at_end, twin, nearer), farther, jnp.where(at_end, nearer, twin)]

    def deal_all(j, which=None):
        @pl.when(primary)
        def _():
            for index, plane_at in enumerate(deal_planes(j)):
                if which is not None and index not in which:
                    continue
                if index:
                    arrived(j, plane_at)
                for k in range(0 if j in by_second else 1, inner):
                    deal(j, plane_at, k).start()
                if j not in by_second:
                    keep(j, plane_at).start()

    def share(j, plane_at):
        rows = pl.ds(pl.multiple_of(plane_at * inner * depth, inner * depth), inner * depth)
        return remote(
            wfull.at[j, rows, :], wfull.at[j, rows, :],
            r.fw_s.at[j], r.fw_r.at[j], (o, i, mate),
        )

    def received(ref, semaphore):
        remote(ref, ref, semaphore, semaphore, (o, i, mate)).wait_recv()

    def gather(j, which=None):
        second = j in by_second

        @pl.when(jnp.logical_not(primary) if second else primary)
        def _():
            if not second and (which is None or 0 in which):
                local(wst.at[j, 0], wst.at[j, 0], r.keep_s.at[j]).wait()
            for index, plane_at in enumerate(deal_planes(j)):
                if which is not None and index not in which:
                    continue
                start_row = pl.multiple_of(plane_at * inner * depth, depth)
                rows = (inner if second else inner - 1) * depth
                received(wfull.at[j, pl.ds(start_row, rows), :], r.w2_r.at[j, plane_at])
                share(j, plane_at).start()

    def handed(j):
        @pl.when(primary if j in by_second else jnp.logical_not(primary))
        def _():
            received(wfull.at[j], r.fw_r.at[j])

    def collect(j, which=None):
        gather(j, which)
        handed(j)

    small = ((r.conv_taps, r.taps), (r.ln_gain, r.lng), (r.ln_bias, r.lnb), (r.mem_gain, r.mgn))
    own_small = [
        local(a.at[:, span(i, HEAD)], b, r.sml_s.at[k]) for k, (a, b) in enumerate(small)
    ]
    mate_small = [
        remote(a.at[:, span(i, HEAD)], b, r.prm_s.at[k], r.prm_r.at[k], (o, i, mate))
        for k, (a, b) in enumerate(small)
    ]
    for j in range(count):
        own_rows[j].wait()
        spread_all(j, 0)
        if j in moved:
            at_end = (plane_of(1) + t - o) * (twin - o) > 0
            start(hand_over(j), jnp.logical_and(jnp.logical_not(primary), at_end))

    @pl.when(primary)
    def _():
        for copy in own_small:
            copy.start()
        for copy in mate_small:
            copy.start()

    ext = r.ext
    plane = jnp.where(primary, o, twin)
    own_ext = local(r.extra, ext.at[i], r.loc_s.at[4])
    guarded(primary, own_ext.start)
    for k in range(inner):
        copy = remote(r.extra, ext.at[i], r.ext_s.at[k], r.ext_r.at[i], (plane, near[k], par))
        start(copy, None if k else jnp.logical_not(primary))

    early = 2
    for j in range(early):
        deal_all(j, (0,))
    gate_in.start()
    for copy in out_in:
        copy.start()

    tok_own.wait()
    gain_in.wait()
    remote(xin.at[mate], xin.at[mate], r.xin_s, r.xin_r, (o, i, mate)).wait_recv()
    norm_rows = 32
    pieces = 2
    piece_rows = hb // pieces

    def norm_step(m, carry):
        at = span(m, norm_rows)
        parts = [xin[f, at, :].astype(f32) for f in range(tp)]
        square = sum(jnp.sum(p * p, axis=-1, keepdims=True) for p in parts)
        level = lax.rsqrt(square * (1.0 / model) + EPS)
        for f in range(tp):
            row = (parts[f] * level * r.gain[:, pl.ds(f * half, half)]).astype(bf16)
            nsrc[at, pl.ds(f * half, half)] = row

            @pl.when(primary)
            def _():
                nq[pl.ds(pl.multiple_of(i * block + t * hb + m * norm_rows, norm_rows), norm_rows), pl.ds(f * half, half)] = row
        return carry

    def rows_of(b, c, s):
        return nq.at[pl.ds(pl.multiple_of(b * block + c * hb + s * piece_rows, piece_rows), piece_rows), :]

    def tok_wait(b, c, s):
        rows = rows_of(b, c, s)
        remote(rows, rows, r.tok_s.at[0, 0], r.tok_r.at[b, c, s], (o, i, mate)).wait_recv()

    steps = piece_rows // norm_rows
    for s in range(pieces):
        lax.fori_loop(s * steps, (s + 1) * steps, norm_step, 0)
        source = nsrc.at[pl.ds(s * piece_rows, piece_rows), :]
        start(remote(source, rows_of(i, t, s), r.tok_s.at[1, s], r.tok_r.at[i, t, s], (twin, i, par)))
        start(remote(source, rows_of(i, t, s), r.tok_s.at[0, s], r.tok_r.at[i, t, s], (o, i, mate)), jnp.logical_not(primary))
    for j in range(count):
        spread_all(j, 1)

    def pass_on(b_from, c, s, k, slot):
        rows = rows_of(b_from, c, s)
        target = near[k] if isinstance(k, int) else jnp.where(k == 1, near[1], near[2])
        return remote(rows, rows, r.pas_s, r.tok_r.at[b_from, c, s], (o, target, t))

    @pl.when(primary)
    def _():
        for s in range(pieces):
            pass_on(i, t, s, 1 + t, 0).start()
        for s in range(pieces):
            tok_wait(i, mate, s)
            pass_on(i, mate, s, 1 + mate, 1).start()
        for s in range(pieces):
            pass_on(i, t, s, 1 + mate, 2).start()
            pass_on(i, mate, s, 1 + t, 3).start()

    @pl.when(jnp.logical_not(primary))
    def _():
        for s in range(pieces):
            for c, slot in ((0, 0), (1, 1)):
                tok_wait(i, c, s)
                pass_on(i, c, s, 1 + c, slot).start()
        for s in range(pieces):
            for c, slot in ((0, 2), (1, 3)):
                pass_on(i, c, s, 2 - c, slot).start()

    for s in range(pieces):
        tok_wait(near[1], 0, s)
        pass_on(near[1], 0, s, 2, 4).start()
        tok_wait(near[2], 1, s)
        pass_on(near[2], 1, s, 1, 5).start()
    for j in range(count):
        spread_all(j, 2)
    received(nq.at[pl.ds(0, (inner - 1) * block), :], r.pas_s)

    @pl.when(jnp.logical_not(primary))
    def _():
        pl.semaphore_signal(r.clear, inc=1, device_id=(o, i, mate), device_id_type=MESH)

    for s in range(pieces):
        tok_wait(near[1], 1, s)
        tok_wait(near[2], 0, s)
        tok_wait(near[3], 0, s)
        tok_wait(near[3], 1, s)

    gwp, gt, rowsv, colsv = r.gwp, r.gt, r.rowsv, r.colsv
    gate_in.wait()
    bias_in.wait()
    bias_row = jnp.concatenate([r.bias[...], jnp.zeros((1, LANES - r.bias.shape[1]), f32)], axis=1)

    def chunk(n):
        return span(n, block)

    def gate_step(n, carry):
        got = lax.dot_general(
            nq[chunk(n), :], gwp[...], (((1,), (1,)), ((), ())), preferred_element_type=f32
        )
        gt[:, chunk(n)] = (got + bias_row).T[: gt.shape[0]]
        return carry

    lax.fori_loop(0, inner, gate_step, 0)
    guarded(primary, own_ext.wait)
    for k in range(inner):
        def hear(k=k):
            remote(r.extra, ext.at[near[k]], r.ext_s.at[0], r.ext_r.at[near[k]], (o, i, mate)).wait_recv()
        if k:
            hear()
        else:
            guarded(jnp.logical_not(primary), hear)

    mine = lax.broadcasted_iota(jnp.int32, (MEMORY_HEADS, quarter), 0) == head
    mine_block = lax.broadcasted_iota(jnp.int32, (MEMORY_HEADS, block), 0) == head

    def gate_row(g):
        rows = gt[pl.ds(g * MEMORY_HEADS, MEMORY_HEADS), :]
        return jnp.sum(jnp.where(mine, rows, 0.0), axis=0, keepdims=True)

    def extra_row(d):
        pieces = [
            jnp.sum(jnp.where(mine_block, ext[b, pl.ds(d * MEMORY_HEADS, MEMORY_HEADS), :], 0.0), axis=0, keepdims=True)
            for b in range(inner)
        ]
        return jnp.concatenate(pieces, axis=1)

    def log_sigmoid(v):
        return jnp.minimum(v, 0.0) - jnp.log1p(jnp.exp(-jnp.abs(v)))

    within = lax.rem(lax.broadcasted_iota(jnp.int32, (1, quarter), 1), block)

    def scan(v, forward, join, empty):
        step = 1
        while step < block:
            if forward:
                v = join(v, jnp.where(within >= step, pltpu.roll(v, step, 1), empty))
            else:
                v = join(v, jnp.where(within < block - step, pltpu.roll(v, quarter - step, 1), empty))
            step *= 2
        return v

    table = []
    for d in range(2):
        gate_in_row = gate_row(2 * d)
        forget = log_sigmoid(gate_row(2 * d + 1)) + extra_row(d)
        decay = scan(forget, d == 0, jnp.add, 0.0)
        shifted = gate_in_row - decay
        running = scan(shifted, d == 0, jnp.maximum, -jnp.inf)
        table += [shifted, running, decay]
    table += [jnp.zeros((1, quarter), f32)] * 2
    rowsv[...] = jnp.concatenate(table, axis=0)

    def turn_step(n, carry):
        piece = rowsv[:, chunk(n)]
        wide = jnp.concatenate([piece, jnp.zeros((LANES - piece.shape[0], block), f32)], axis=0)
        colsv[chunk(n), :] = wide.T
        return carry

    lax.fori_loop(0, inner, turn_step, 0)

    def project(n, j):
        return jnp.dot(nq[chunk(n), :], wfull[j], preferred_element_type=f32)

    kb, vb, cm, cv = r.kb, r.vb, r.cm, r.cv
    smat, sinfo, matx, infox = r.smat, r.sinfo, r.matx, r.infox
    gmat, ginfo, gin, gininfo = r.gmat, r.ginfo, r.gin, r.gininfo

    def key_step(n, carry):
        keys = project(n, 2)
        kb[chunk(n), :] = keys.astype(bf16)
        wide = keys.astype(bf16).astype(f32)
        cols = colsv[chunk(n), :]
        for d in range(2):
            end = block - 1 if d == 0 else 0
            top = cols[end : end + 1, 3 * d + 1 : 3 * d + 2]
            weighted = wide * (jnp.exp(cols[:, 3 * d : 3 * d + 1] - top) * scale)
            r.kwt[d, :, chunk(n)] = weighted.T.astype(bf16)
            cv[d, n] = jnp.broadcast_to(jnp.sum(weighted, axis=0, keepdims=True), (8, HEAD))
        return carry

    def state_step(m, carry):
        ns = [m * 2 + p for p in range(2)]
        values = [project(n, 3).astype(bf16) for n in ns]
        for n, value in zip(ns, values):
            vb[chunk(n), :] = value
        for n, value in zip(ns, values):
            for d in range(2):
                cm[d, n] = jnp.dot(r.kwt[d, :, chunk(n)], value, preferred_element_type=f32)
        return carry

    earlier = lax.broadcasted_iota(jnp.int32, (block, block), 0) >= lax.broadcasted_iota(jnp.int32, (block, block), 1)
    later = lax.broadcasted_iota(jnp.int32, (block, block), 0) <= lax.broadcasted_iota(jnp.int32, (block, block), 1)

    def weight_step(n, carry):
        cols = colsv[chunk(n), :]
        rows = rowsv[:, chunk(n)]
        for d in range(2):
            gap = jnp.minimum(rows[3 * d : 3 * d + 1] - cols[:, 3 * d + 1 : 3 * d + 2], 0.0)
            r.wgt[d, n] = jnp.where(earlier if d == 0 else later, jnp.exp(gap) * scale, 0.0)
        return carry

    lax.fori_loop(0, inner, weight_step, 0)
    @pl.when(primary)
    def _():
        pl.semaphore_wait(r.clear, 1)

    deal_all(0, range(1, outer))
    deal_all(1, range(1, outer))
    deal_all(2, range(2))

    collect(0)
    gpad, conv, hsend, hrecv = r.gpad, r.conv, r.hsend, r.hrecv
    pad = hsend.shape[1]
    reach = KW // 2
    sides = HEAD // LANES

    def value_step(n, carry):
        r.gval[chunk(n), :] = project(n, 0)
        return carry

    lax.fori_loop(0, inner, value_step, 0)
    deal_all(2, range(2, outer))
    deal_all(3, range(2))
    collect(1)

    def glu_step(n, carry):
        glu = (r.gval[chunk(n), :] * jax.nn.sigmoid(project(n, 1))).astype(bf16)
        for side in range(sides):
            gpad[side, pl.ds(pl.multiple_of(n * block + pad, pad), block), :] = glu[:, side * LANES : (side + 1) * LANES].astype(f32)

        @pl.when(n == 0)
        def _():
            hsend[0] = glu[:pad]

        @pl.when(n == inner - 1)
        def _():
            hsend[1] = glu[block - pad :]

        return carry

    lax.fori_loop(0, inner, glu_step, 0)
    def device_of(q):
        return (lax.div(q, tp) * tp + par, i, lax.rem(q, tp))

    has_before, has_after = place > 0, place < last
    start(remote(hsend.at[0], hrecv.at[1], r.hal_s.at[0], r.hal_r.at[1], device_of(jnp.maximum(place - 1, 0))), has_before)
    start(remote(hsend.at[1], hrecv.at[0], r.hal_s.at[1], r.hal_r.at[0], device_of(jnp.minimum(place + 1, last))), has_after)

    @pl.when(primary)
    def _():
        for copy in own_small:
            copy.wait()

    @pl.when(jnp.logical_not(primary))
    def _():
        for copy in mate_small:
            copy.wait_recv()

    deal_all(3, range(2, outer))
    taps, statc, stbuf = r.taps, r.statc, r.stbuf
    conv_rows = 64
    lane = lax.broadcasted_iota(jnp.int32, (conv_rows, LANES), 1)
    shift = pad - reach

    def conv_step(m, carry):
        s1 = s2 = 0.0
        for side in range(sides):
            total = jnp.zeros((conv_rows, LANES), f32)
            for residue in range(8):
                moved = gpad[side, pl.ds(m * conv_rows + residue, conv_rows + 2 * pad - 8), :]
                for j in range(KW):
                    at = j + shift - residue
                    if at % 8 == 0:
                        tap = taps[pl.ds(j, 1), pl.ds(side * LANES, LANES)]
                        total = total + tap * moved[at : at + conv_rows]
            conv[side, span(m, conv_rows), :] = total
            s1 = s1 + total
            s2 = s2 + total * total
        s1 = jnp.sum(s1, axis=-1, keepdims=True)
        s2 = jnp.sum(s2, axis=-1, keepdims=True)
        statc[span(m, conv_rows), :] = jnp.where(lane == 0, s1, jnp.where(lane == 1, s2, 0.0))
        return carry

    conv_steps = quarter // conv_rows
    lax.fori_loop(1, conv_steps // 2, conv_step, 0)
    deal_all(4, range(2))
    collect(2)
    lax.fori_loop(conv_steps // 2, conv_steps - 1, conv_step, 0)
    for edge, present, at in ((0, has_before, 0), (1, has_after, pad + quarter)):
        @pl.when(present)
        def _():
            remote(hrecv.at[edge], hrecv.at[edge], r.hal_s.at[0], r.hal_r.at[edge], (o, i, mate)).wait_recv()
            for side in range(sides):
                gpad[side, pl.ds(at, pad), :] = hrecv[edge, :, side * LANES : (side + 1) * LANES].astype(f32)

        @pl.when(jnp.logical_not(present))
        def _():
            for side in range(sides):
                gpad[side, pl.ds(at, pad), :] = jnp.zeros((pad, LANES), f32)

    lax.fori_loop(0, 2, lambda m, carry: conv_step(m * (conv_steps - 1), carry), 0)
    sums = r.sums
    two = pl.ds(0, 2)

    def sums_step(n, carry):
        sums[:, chunk(n)] = statc[chunk(n), :].T[: sums.shape[0]]
        return carry

    lax.fori_loop(0, inner, sums_step, 0)
    peers = []
    for dz in range(tp):
        for k in range(inner):
            if (dz, k) != (0, 0):
                peers.append((o if dz == 0 else twin, near[k]))
    for index, (plane_to, chip) in enumerate(peers):
        remote(sums.at[two, :], stbuf.at[head, two, :], r.sta_s, r.sta_r, (plane_to, chip, t)).start()
    deal_all(4, range(2, outer))
    gather(3, range(2))
    lax.fori_loop(0, inner, key_step, 0)
    collect(3, range(2, outer))
    lax.fori_loop(0, inner // 2, state_step, 0)

    def corner(n, d, column):
        end = block - 1 if d == 0 else 0
        at = n * block + end
        return colsv[pl.ds(at, 1), :][:, column : column + 1]

    totals = [[corner(n, d, 3 * d + 2) for n in range(inner)] for d in range(2)]
    levels = [[corner(n, d, 3 * d + 1) + totals[d][n] for n in range(inner)] for d in range(2)]
    for d in range(2):
        reaches = []
        for n in range(inner):
            later = range(n + 1, inner) if d == 0 else range(n)
            value = levels[d][n]
            for m in later:
                value = value + totals[d][m]
            reaches.append(value)
        top = functools.reduce(jnp.maximum, reaches)
        shares = [jnp.exp(v - top) for v in reaches]
        matx[d] = sum(shares[n] * cm[d, n] for n in range(inner)).astype(bf16)
        vec = sum(shares[n] * cv[d, n] for n in range(inner))
        row = lax.broadcasted_iota(jnp.int32, (8, HEAD), 0)
        decay = functools.reduce(jnp.add, totals[d])
        infox[d] = jnp.where(row == 0, vec, jnp.where(row == 1, top, decay))

    start(remote(matx, smat, r.mat_s.at[0], r.mat_r.at[0], (o, i, mate)))
    start(remote(infox, sinfo, r.inf_s.at[0], r.inf_r.at[0], (o, i, mate)))
    gather(4, range(2))
    received(stbuf.at[pl.ds(0, MEMORY_HEADS - 1), two, :], r.sta_r)
    stbuf[head] = sums[...]

    def stat_step(n, carry):
        whole = stbuf[0, :, chunk(n)]
        for k in range(1, MEMORY_HEADS):
            whole = whole + stbuf[k, :, chunk(n)]
        whole = whole * (1.0 / channels)
        mean = whole[0:1]
        rstd = lax.rsqrt(whole[1:2] - mean * mean + EPS)
        wide = jnp.concatenate([mean, rstd, jnp.zeros((LANES - 2, block), f32)], axis=0)
        statc[chunk(n), :] = wide.T
        return carry

    lax.fori_loop(0, inner, stat_step, 0)
    actb, memb, cin = r.actb, r.memb, r.cin

    def give(which, source, b):
        return remote(
            source.at[chunk(b), :], cin.at[which, i], r.ret_s.at[which, b], r.ret_r.at[which, i],
            (plane, b, par),
        )

    def give_own(which, source):
        return local(source.at[chunk(i), :], cin.at[which, i], r.rel_s.at[which])

    def give_rows(which, source, b):
        to_self = jnp.logical_and(primary, b == i)
        guarded(to_self, give_own(which, source).start)
        guarded(jnp.logical_not(to_self), give(which, source, b).start)

    order = [jnp.where(primary, near[a], near[b]) for a, b in zip((1, 2, 3, 0), (2, 1, 3, 0))]

    def act_step(n, carry):
        for half_at in range(2):
            rows = pl.ds(pl.multiple_of(n * block + half_at * (block // 2), block // 2), block // 2)
            cols = statc[rows, :]
            for side in range(sides):
                lanes = pl.ds(side * LANES, LANES)
                normal = (conv[side, rows, :] - cols[:, 0:1]) * cols[:, 1:2] * r.lng[:, lanes] + r.lnb[:, lanes]
                actb[rows, lanes] = (normal * jax.nn.sigmoid(normal)).astype(bf16)
        return carry

    lax.fori_loop(0, inner, act_step, 0)

    mat_rows = gin.at[span(t, HEAD // tp), :]
    mate_rows = gin.at[span(mate, HEAD // tp), :]
    remote(matx, smat, r.mat_s.at[0], r.mat_r.at[0], (o, i, mate)).wait_recv()
    remote(infox, sinfo, r.inf_s.at[0], r.inf_r.at[0], (o, i, mate)).wait_recv()
    ours, theirs = infox[grp], sinfo[grp]
    is_far = t == grp
    our_reach = ours[1:2, 0:1] + jnp.where(is_far, theirs[2:3, 0:1], 0.0)
    their_reach = theirs[1:2, 0:1] + jnp.where(is_far, 0.0, ours[2:3, 0:1])
    group_level = jnp.maximum(our_reach, their_reach)
    our_share, their_share = jnp.exp(our_reach - group_level), jnp.exp(their_reach - group_level)
    gmat[...] = (our_share * matx[grp].astype(f32) + their_share * smat[grp].astype(f32)).astype(bf16)
    state_row = lax.broadcasted_iota(jnp.int32, (8, HEAD), 0)
    ginfo[...] = jnp.where(state_row == 0, our_share * ours[0:1] + their_share * theirs[0:1], group_level)
    across = ((1 - grp) * tp + par, i, t)
    start(remote(gmat.at[span(t, HEAD // tp), :], mat_rows, r.mat_s.at[1], r.mat_r.at[1], across))
    start(remote(ginfo, gininfo, r.inf_s.at[1], r.inf_r.at[1], across))
    for b in order:
        give_rows(0, actb, b)
    gather(4, range(2, outer))
    nvs, levs = r.nvs, r.levs
    for d in range(2):
        by_mate = t == 1 - d
        level = jnp.where(by_mate, sinfo[d][1:2, 0:1], LOW_START)
        present = jnp.where(by_mate, 1.0, 0.0)
        mat = present * smat[d].astype(f32)
        vec = present * sinfo[d][0:1]
        for n in (range(inner) if d == 0 else range(inner - 1, -1, -1)):
            high = mat.astype(bf16)
            r.cst[d, n, pl.ds(0, HEAD), :] = high
            r.cst[d, n, pl.ds(HEAD, HEAD), :] = (mat - high.astype(f32)).astype(bf16)
            nvs[d, n] = jnp.broadcast_to(vec, (8, HEAD))
            levs[d, n] = jnp.broadcast_to(level, (8, LANES))
            carried = level + totals[d][n]
            new_level = jnp.maximum(carried, levels[d][n])
            kept, added = jnp.exp(carried - new_level), jnp.exp(levels[d][n] - new_level)
            mat = kept * mat + added * cm[d, n]
            vec = kept * vec + added * cv[d, n][0:1]
            level = new_level

    first_group = grp == 0

    def along(values):
        return jnp.concatenate([jnp.broadcast_to(v, (1, block)) for v in values], axis=1)

    kept, tops = [], []
    for d in range(2):
        running, decay = rowsv[pl.ds(3 * d + 1, 1), :], rowsv[pl.ds(3 * d + 2, 1), :]
        level = along([levs[d, n][0:1, 0:1] for n in range(inner)])
        top = jnp.maximum(running, level)
        tops.append((top, decay))
        kept.append([jnp.exp(running - top), jnp.exp(level - top), jnp.exp(-top - decay)])
    alone = [jnp.where(first_group, a, b) for a, b in zip(*kept)]
    joined = [jnp.where(first_group, b, a) for a, b in zip(*kept)]
    joined_top, joined_decay = (jnp.where(first_group, b, a) for a, b in zip(*tops))
    r.colw[:, pl.ds(0, 8)] = jnp.concatenate(alone + joined + [jnp.zeros((2, quarter), f32)], axis=0).T
    handed(4)


    def query_rows(ns):
        queries = [project(n, 4).astype(bf16) for n in ns]
        scores = [
            lax.dot_general(q, kb[chunk(n), :], (((1,), (1,)), ((), ())), preferred_element_type=f32)
            for n, q in zip(ns, queries)
        ]
        for n, q in zip(ns, queries):
            r.qb[chunk(n), :] = q
        for role, d in ((0, grp), (1, 1 - grp)):
            for n, q, score in zip(ns, queries, scores):
                cols = r.colw[chunk(n), :]
                local_weight, carry_weight = cols[:, 3 * role : 3 * role + 1], cols[:, 3 * role + 1 : 3 * role + 2]
                part = score * r.wgt[d, n]
                num = jnp.dot(part.astype(bf16), vb[chunk(n), :], preferred_element_type=f32)
                far = jnp.dot(jnp.concatenate([q, q], axis=1), r.cst[d, n], preferred_element_type=f32)
                num = local_weight * num + carry_weight * far
                far_sum = jnp.sum(q.astype(f32) * nvs[d, n][0:1], axis=-1, keepdims=True)
                den = local_weight * jnp.sum(part, axis=-1, keepdims=True) + carry_weight * far_sum
                if role == 0:
                    r.alone[chunk(n), :] = num * (1.0 / jnp.maximum(jnp.abs(den), cols[:, 2:3]))
                else:
                    r.numj[chunk(n), :] = num
                    r.denj[chunk(n), :] = jnp.broadcast_to(den, (block, LANES))

    query_rows([0, 1])
    query_rows([2])
    remote(mat_rows, mat_rows, r.mat_s.at[1], r.mat_r.at[1], (o, i, mate)).wait_recv()
    start(remote(mat_rows, mat_rows, r.mat_s.at[2], r.mat_r.at[2], (o, i, mate)))
    query_rows([3])
    remote(ginfo, gininfo, r.inf_s.at[1], r.inf_r.at[1], (o, i, mate)).wait_recv()
    remote(mate_rows, mate_rows, r.mat_s.at[2], r.mat_r.at[2], (o, i, mate)).wait_recv()

    arriving = gininfo[1:2, 0:1] + jnp.where(t == grp, sinfo[1 - grp][2:3, 0:1], 0.0)
    group_levels = []
    for n in range(inner):
        lost_f = functools.reduce(jnp.add, totals[0][:n], jnp.zeros((1, 1), f32))
        lost_b = functools.reduce(jnp.add, totals[1][n + 1 :], jnp.zeros((1, 1), f32))
        group_levels.append(arriving + jnp.where(first_group, lost_b, lost_f))
    level = along(group_levels)
    top = jnp.maximum(joined_top, level)
    kept = [jnp.exp(joined_top - top), jnp.exp(level - top), jnp.exp(-top - joined_decay)]
    r.colw[:, pl.ds(0, 8)] = jnp.concatenate(kept + [jnp.zeros((5, quarter), f32)], axis=0).T

    def memory_rows(ns):
        queries = [r.qb[chunk(n), :] for n in ns]
        fars = [jnp.dot(q, gin[...], preferred_element_type=f32) for q in queries]
        far_sums = [jnp.sum(q.astype(f32) * gininfo[0:1], axis=-1, keepdims=True) for q in queries]
        for n, far, far_sum in zip(ns, fars, far_sums):
            cols = r.colw[chunk(n), :]
            den = cols[:, 0:1] * r.denj[chunk(n), pl.ds(0, 1)] + cols[:, 1:2] * far_sum
            share_of = 1.0 / jnp.maximum(jnp.abs(den), cols[:, 2:3])
            out = r.alone[chunk(n), :] + (
                r.numj[chunk(n), :] * (cols[:, 0:1] * share_of) + far * (cols[:, 1:2] * share_of)
            )
            level = lax.rsqrt(jnp.mean(out * out, axis=-1, keepdims=True) + EPS)
            memb[chunk(n), :] = (out * level * r.mgn[...]).astype(bf16)
        for n in ns:
            give_rows(1, memb, n)

    for ns in ([order[0]], [order[1]], [order[2], order[3]]):
        memory_rows(ns)
    acc, pbuf = r.acc, r.pbuf
    tile = 512
    tiles = model // tile

    def take(which, k):
        def hear():
            rows = cin.at[which, near[k]]
            remote(rows, rows, r.ret_s.at[which, 0], r.ret_r.at[which, near[k]], (o, i, mate)).wait_recv()

        if k:
            hear()
        else:
            guarded(jnp.logical_not(primary), hear)
            guarded(primary, give_own(which, actb).wait)

    def part(which, n):
        return sum(
            jnp.dot(cin[which, k], ow[which, pl.ds(k * HEAD, HEAD), span(n, tile)], preferred_element_type=f32)
            for k in range(inner)
        )

    def conv_out_step(n, carry):
        acc[:, span(n, tile)] = part(0, n)
        return carry

    for copy in out_in:
        copy.wait()
    for k in range(inner):
        take(0, k)
    lax.fori_loop(0, tiles, conv_out_step, 0)

    def rows_part(ks, n):
        return sum(
            jnp.dot(
                cin[1, near[k]], ow[1, pl.ds(pl.multiple_of(near[k] * HEAD, HEAD), HEAD), span(n, tile)],
                preferred_element_type=f32,
            )
            for k in ks
        )

    def add_step(n, carry):
        acc[:, span(n, tile)] += rows_part((1, 2), n)
        return carry

    take(1, 1)
    take(1, 2)
    lax.fori_loop(0, tiles, add_step, 0)
    take(1, 3)
    take(1, 0)
    out_own, out_mate = r.out_own, r.out_mate

    def piece(n):
        return remote(
            pbuf.at[span(mate, hb), span(n, tile)], out_mate.at[:, span(n, tile)],
            r.fin_s, r.fin_r, (o, i, mate),
        )

    def stay(n):
        return local(pbuf.at[span(t, hb), span(n, tile)], out_own.at[:, span(n, tile)], r.fil_s)

    def mem_out_step(n, carry):
        pbuf[:, span(n, tile)] = (acc[:, span(n, tile)] + rows_part((3, 0), n)).astype(bf16)
        piece(n).start()
        stay(n).start()
        return carry

    lax.fori_loop(0, tiles, mem_out_step, 0)

    for copy, when in sends:
        if when is None:
            copy.wait_send()
        else:
            pl.when(when)(copy.wait_send)


    received(stbuf.at[pl.ds(0, MEMORY_HEADS - 1), two, :], r.sta_s)

    @pl.when(primary)
    def _():
        for copy in mate_small:
            copy.wait_send()
        for j in range(count):
            received(wst.at[j] if j in by_second else wst.at[j, pl.ds(0, inner - 1)], r.w2_s.at[j])
            if j not in by_second:
                received(wfull.at[j], r.fw_s.at[j])

    @pl.when(jnp.logical_not(primary))
    def _():
        for j in by_second:
            received(wfull.at[j], r.fw_s.at[j])

    for which, source in ((0, actb), (1, memb)):
        for b in range(inner):
            guarded(jnp.logical_not(jnp.logical_and(primary, i == b)), give(which, source, b).wait_send)
    local(out_own, out_own, r.fil_s).wait()
    received(out_mate, r.fin_s)
    received(out_mate, r.fin_r)


LANES = 128
LOW_START = -1e30


def whole_layer(outer, inner, tp, args):
    tokens = args.tokens
    block, half = tokens.shape
    depth = args.glu_value.shape[0]
    count = 5
    quarter, model = inner * block, half * tp
    hb = block // tp
    pad = 16
    f32, bf16 = jnp.float32, jnp.bfloat16
    dma = pltpu.SemaphoreType.DMA
    tiles = model // 512
    extra = args.log_decay_extra.T
    operands = dict(
        tokens=tokens, norm_gain=args.norm_gain[None],
        glu_value=args.glu_value, glu_gate=args.glu_gate,
        key_weight=args.key_weight, value_weight=args.value_weight, query_weight=args.query_weight,
        conv_taps=args.conv_taps, ln_gain=args.ln_gain[None], ln_bias=args.ln_bias[None],
        gate_weight=args.gate_weight.T, gate_bias=args.gate_bias[None],
        extra=extra, mem_gain=args.mem_gain[None],
        out_conv=args.out_conv, out_mem=args.out_mem,
    )
    scratch = dict(
        nq=pltpu.VMEM((quarter, model), bf16),
        nsrc=pltpu.VMEM((hb, model), bf16),
        xin=pltpu.VMEM((tp, hb, half), bf16),
        wst=pltpu.VMEM((count, outer, depth, half), bf16),
        wfull=pltpu.VMEM((count, model, HEAD), bf16),
        wmv=pltpu.VMEM((2, depth, half), bf16),
        ow=pltpu.VMEM((2,) + args.out_conv.shape, bf16),
        taps=pltpu.VMEM((KW, HEAD), f32), lng=pltpu.VMEM((1, HEAD), f32),
        lnb=pltpu.VMEM((1, HEAD), f32), mgn=pltpu.VMEM((1, HEAD), f32),
        ext=pltpu.VMEM((inner,) + extra.shape, f32),
        gwp=pltpu.VMEM((LANES, model), bf16),
        gain=pltpu.VMEM((1, model), f32), bias=pltpu.VMEM((1, 4 * MEMORY_HEADS), f32),
        gt=pltpu.VMEM((4 * MEMORY_HEADS, quarter), f32),
        rowsv=pltpu.VMEM((8, quarter), f32), colsv=pltpu.VMEM((quarter, LANES), f32),
        gpad=pltpu.VMEM((HEAD // LANES, quarter + 2 * pad, LANES), f32),
        conv=pltpu.VMEM((HEAD // LANES, quarter, LANES), f32), gval=pltpu.VMEM((quarter, HEAD), f32),
        hsend=pltpu.VMEM((2, pad, HEAD), bf16), hrecv=pltpu.VMEM((2, pad, HEAD), bf16),
        statc=pltpu.VMEM((quarter, LANES), f32), sums=pltpu.VMEM((8, quarter), f32),
        stbuf=pltpu.VMEM((MEMORY_HEADS, 8, quarter), f32),
        kb=pltpu.VMEM((quarter, HEAD), bf16), vb=pltpu.VMEM((quarter, HEAD), bf16),
        cm=pltpu.VMEM((2, inner, HEAD, HEAD), f32), cv=pltpu.VMEM((2, inner, 8, HEAD), f32),
        matx=pltpu.VMEM((2, HEAD, HEAD), bf16), infox=pltpu.VMEM((2, 8, HEAD), f32),
        smat=pltpu.VMEM((2, HEAD, HEAD), bf16), sinfo=pltpu.VMEM((2, 8, HEAD), f32),
        gmat=pltpu.VMEM((HEAD, HEAD), bf16), ginfo=pltpu.VMEM((8, HEAD), f32),
        gin=pltpu.VMEM((HEAD, HEAD), bf16), gininfo=pltpu.VMEM((8, HEAD), f32),
        cst=pltpu.VMEM((2, inner, 2 * HEAD, HEAD), bf16), qb=pltpu.VMEM((quarter, HEAD), bf16), kwt=pltpu.VMEM((2, HEAD, quarter), bf16),
        alone=pltpu.VMEM((quarter, HEAD), f32), numj=pltpu.VMEM((quarter, HEAD), f32), denj=pltpu.VMEM((quarter, LANES), f32),
        wgt=pltpu.VMEM((2, inner, block, block), f32), colw=pltpu.VMEM((quarter, LANES), f32),
        nvs=pltpu.VMEM((2, inner, 8, HEAD), f32), levs=pltpu.VMEM((2, inner, 8, LANES), f32),
        actb=pltpu.VMEM((quarter, HEAD), bf16), memb=pltpu.VMEM((quarter, HEAD), bf16),
        cin=pltpu.VMEM((2, inner, block, HEAD), bf16),
        acc=pltpu.VMEM((block, model), f32), pbuf=pltpu.VMEM((block, model), bf16),
        own_s=dma((count,)), mov_s=dma((2,)), mov_r=dma((2,)), mvd_s=dma((2,)), loc_s=dma((7,)), xin_s=dma, xin_r=dma,
        w1_s=dma((count, outer // tp)), w1_r=dma((count, outer)),
        sml_s=dma((4,)), prm_s=dma((4,)), prm_r=dma((4,)),
        ext_s=dma((inner,)), ext_r=dma((inner,)),
        tok_s=dma((2, 2)), tok_r=dma((inner, tp, 2)), pas_s=dma, clear=pltpu.SemaphoreType.REGULAR,
        w2_s=dma((count,)), w2_r=dma((count, outer)),
        keep_s=dma((count,)), fw_s=dma((count,)), fw_r=dma((count,)),
        hal_s=dma((2,)), hal_r=dma((2,)),
        sta_s=dma, sta_r=dma,
        mat_s=dma((3,)), mat_r=dma((3,)), inf_s=dma((2,)), inf_r=dma((2,)),
        ret_s=dma((2, inner)), ret_r=dma((2, inner)), rel_s=dma((2,)),
        fin_s=dma, fin_r=dma, fil_s=dma,
    )
    any_space = pl.BlockSpec(memory_space=pl.ANY)
    spaces = {n: any_space for n in operands}
    names = list(operands) + ["out_own", "out_mate"] + list(scratch)
    shape = pltpu.VMEM((hb, model), bf16)
    own, mate = pl.pallas_call(
        functools.partial(layer_kernel, outer, inner, tp, names),
        out_shape=(shape, shape),
        in_specs=[spaces[n] for n in operands],
        out_specs=(any_space, any_space),
        scratch_shapes=list(scratch.values()),
        compiler_params=pltpu.CompilerParams(
            collective_id=0, has_side_effects=True, vmem_limit_bytes=60 * 2**20
        ),
    )(*operands.values())
    return (own.astype(f32) + mate.astype(f32)).astype(bf16)


def gather_inputs(tokens, weights, extra, inner):
    rows, half = tokens.shape
    gathered = lax.all_gather(tokens, ("inner", "tp"), axis=0)
    tp = gathered.shape[0] // inner
    whole = jnp.transpose(gathered.reshape(inner, tp, rows, half), (0, 2, 1, 3))
    whole = whole.reshape(inner * rows, tp * half)
    depth, columns = weights[0].shape
    width = columns // inner
    packed = jnp.stack([w.reshape(depth, inner, width) for w in weights], axis=2)
    packed = jnp.transpose(packed, (1, 0, 2, 3)).reshape(inner, depth, len(weights) * width)
    if inner > 1:
        packed = lax.all_to_all(packed, "inner", split_axis=0, concat_axis=0, tiled=True)
    pieces = lax.all_gather(packed.reshape(inner * depth, -1), "outer", axis=0, tiled=True)
    pieces = pieces.reshape(-1, len(weights), width).transpose(1, 0, 2)
    extras = lax.all_gather(extra, "inner", axis=0, tiled=True) if inner > 1 else extra
    return whole, pieces, extras.T


def local_state(keys, values, shifted, level, total, scale):
    weight = jnp.exp(shifted - level[:, None]) * scale
    weighted = keys.astype(jnp.float32) * weight[:, :, None]
    mat = jnp.einsum(
        "hsd,hse->hde", weighted.astype(jnp.bfloat16), values, preferred_element_type=jnp.float32
    )
    return mat, jnp.sum(weighted, axis=1), level + total, total


def packed_state(mat, vec, level, decay):
    spread = lambda x: jnp.broadcast_to(x[:, None], vec.shape)
    rows = parts_of(vec) + parts_of(spread(level)) + parts_of(spread(decay))
    pad = [jnp.zeros_like(rows[0])] * 7
    return jnp.concatenate([mat.astype(jnp.bfloat16), jnp.stack(rows + pad, axis=1)], axis=1)


def incoming(states, reverse):
    count = states.shape[0]
    mats = states[:, :, :HEAD]
    rows = states[:, :, HEAD:]
    vecs = whole_of(rows[:, :, 0], rows[:, :, 1], rows[:, :, 2])
    levels = whole_of(rows[:, :, 3, 0], rows[:, :, 4, 0], rows[:, :, 5, 0])
    decays = whole_of(rows[:, :, 6, 0], rows[:, :, 7, 0], rows[:, :, 8, 0])
    place = lax.axis_index("outer")
    order = jnp.arange(count)
    if reverse:
        ahead = (order > place)[:, None]
        between = (order[None, :] < order[:, None]) & (order[None, :] > place)
    else:
        ahead = (order < place)[:, None]
        between = (order[None, :] > order[:, None]) & (order[None, :] < place)
    lost = jnp.sum(jnp.where(between[:, :, None], decays[None], 0.0), axis=1)
    reach = jnp.where(ahead, levels + lost, -1e30)
    level = jnp.max(reach, axis=0)
    share = jnp.where(ahead, jnp.exp(reach - level[None]), 0.0)
    mat = jnp.sum(share[:, :, None, None] * mats.astype(jnp.float32), axis=0)
    vec = jnp.sum(share[:, :, None] * vecs, axis=0)
    return mat, vec, level


def finish(query_wide, num, den, running, decay, state):
    mat, vec, level = state
    top = jnp.maximum(running, level[:, None])
    local_weight = jnp.exp(running - top)
    carry_weight = jnp.exp(level[:, None] - top)
    num = local_weight[:, :, None] * num + carry_weight[:, :, None] * jnp.einsum(
        "htd,hde->hte", query_wide, mat, precision=PRECISE
    )
    den = local_weight * den + carry_weight * jnp.einsum(
        "htd,hd->ht", query_wide, vec, precision=PRECISE
    )
    return num / jnp.maximum(jnp.abs(den), jnp.exp(-top - decay))[:, :, None]


def make_shards(inner, outer, tp):
    def own(array, dim):
        size = array.shape[dim] // inner
        return lax.dynamic_slice_in_dim(array, lax.axis_index("inner") * size, size, dim)

    def shards(
        tokens,
        norm_gain,
        glu_value,
        glu_gate,
        conv_taps,
        ln_gain,
        ln_bias,
        query_weight,
        key_weight,
        value_weight,
        gate_weight,
        gate_bias,
        log_decay_extra,
        mem_gain,
        out_conv,
        out_mem,
    ):
        fits = tp == 2 and inner == 4 and outer == 2 * tp and inner * tp == MEMORY_HEADS
        if fits and tokens.shape[1] == inner * HEAD and conv_taps.shape[1] == inner * HEAD:
            return whole_layer(outer, inner, tp, types.SimpleNamespace(
                tokens=tokens, norm_gain=norm_gain, glu_value=glu_value, glu_gate=glu_gate,
                conv_taps=conv_taps, ln_gain=ln_gain, ln_bias=ln_bias, query_weight=query_weight,
                key_weight=key_weight, value_weight=value_weight, gate_weight=gate_weight,
                gate_bias=gate_bias, log_decay_extra=log_decay_extra, mem_gain=mem_gain,
                out_conv=out_conv, out_mem=out_mem,
            ))
        taps, gain, bias, mgain = own(conv_taps, 1), own(ln_gain, 0), own(ln_bias, 0), own(mem_gain, 0)
        channels = conv_taps.shape[1] * tp
        width = gain.shape[0]
        heads = mgain.shape[0] // HEAD
        first = (lax.axis_index("tp") * inner + lax.axis_index("inner")) * heads
        stacked = (query_weight, key_weight, value_weight, glu_value, glu_gate)
        whole, weights, extras = gather_inputs(tokens, stacked, log_decay_extra, inner)
        rows = whole.shape[0]
        wide = whole.astype(jnp.float32)
        normed = (
            wide * lax.rsqrt(jnp.mean(wide * wide, axis=-1, keepdims=True) + EPS) * norm_gain
        ).astype(jnp.bfloat16)
        own_gate = lax.dynamic_slice_in_dim(
            gate_weight.reshape(-1, 4, MEMORY_HEADS), first, heads, 2
        )
        own_bias = lax.dynamic_slice_in_dim(gate_bias.reshape(4, MEMORY_HEADS), first, heads, 1)
        gates = lax.dot_general(
            own_gate.reshape(-1, 4 * heads), normed, (((0,), (1,)), ((), ())),
            preferred_element_type=jnp.float32,
        ).reshape(4, heads, rows) + own_bias[:, :, None]
        own_extra = lax.dynamic_slice_in_dim(
            extras.reshape(2, MEMORY_HEADS, rows), first, heads, 1
        )
        lf = jax.nn.log_sigmoid(gates[1::2]) + own_extra
        at = jnp.arange(rows)
        causal = at[:, None] >= at[None, :]
        anti = at[:, None] <= at[None, :]

        def total(x, mask):
            return jnp.sum(jnp.where(mask, x[:, None, :], 0.0), axis=-1)

        def highest(x, mask):
            return jnp.max(jnp.where(mask, x[:, None, :], -jnp.inf), axis=-1)

        decay_f = total(lf[0], causal)
        decay_b = total(lf[1], anti)
        shifted_f = gates[0] - decay_f
        shifted_b = gates[2] - decay_b
        running_f = highest(shifted_f, causal)
        running_b = highest(shifted_b, anti)

        def project(i):
            return jnp.dot(normed, weights[i], preferred_element_type=jnp.float32)

        def heads_first(x):
            return jnp.transpose(x.reshape(rows, heads, HEAD), (1, 0, 2)).astype(jnp.bfloat16)

        keys = heads_first(project(1))
        values = heads_first(project(2))
        scale = HEAD ** (-0.5)
        state_f = local_state(
            keys, values, shifted_f, running_f[:, -1], decay_f[:, -1], scale
        )
        state_b = local_state(keys, values, shifted_b, running_b[:, 0], decay_b[:, 0], scale)
        sent = jnp.stack([packed_state(*state_f), packed_state(*state_b)])
        states = lax.all_gather(sent, "outer", axis=0)

        glu = (project(3) * jax.nn.sigmoid(project(4))).astype(jnp.bfloat16)
        reach = KW // 2
        before = lax.ppermute(glu[rows - reach :], "outer", [(i, i + 1) for i in range(outer - 1)])
        after = lax.ppermute(glu[:reach], "outer", [(i + 1, i) for i in range(outer - 1)])
        queries = heads_first(project(0))

        scores = jnp.einsum("htd,hsd->hts", queries, keys, preferred_element_type=jnp.float32) * scale

        def local_out(shifted, running, mask):
            weight = jnp.where(
                mask, jnp.exp(jnp.minimum(shifted[:, None, :] - running[:, :, None], 0.0)), 0.0
            )
            part = scores * weight
            num = jnp.einsum(
                "hts,hse->hte", part.astype(jnp.bfloat16), values,
                preferred_element_type=jnp.float32,
            )
            return num, jnp.sum(part, axis=-1)

        num_f, den_f = local_out(shifted_f, running_f, causal)
        num_b, den_b = local_out(shifted_b, running_b, anti)

        padded = jnp.concatenate([before, glu, after], axis=0).astype(jnp.float32)
        conv = jnp.zeros(glu.shape, jnp.float32)
        for offset in range(KW):
            conv = conv + taps[offset] * padded[offset : offset + rows]
        sums = jnp.stack([jnp.sum(conv, axis=-1), jnp.sum(conv * conv, axis=-1)])
        sums = lax.psum(sums, ("inner", "tp")) / channels
        chan_mean = sums[0]
        chan_var = sums[1] - chan_mean * chan_mean
        normal = (conv - chan_mean[:, None]) * lax.rsqrt(chan_var + EPS)[:, None] * gain + bias
        act = (normal * jax.nn.sigmoid(normal)).astype(jnp.bfloat16)

        query_wide = queries.astype(jnp.float32)
        forward = finish(query_wide, num_f, den_f, running_f, decay_f, incoming(states[:, 0], False))
        backward = finish(query_wide, num_b, den_b, running_b, decay_b, incoming(states[:, 1], True))
        summed = forward + backward
        head_norm = summed * lax.rsqrt(jnp.mean(summed * summed, axis=-1, keepdims=True) + EPS)
        head_norm = head_norm * mgain.reshape(heads, HEAD)[:, None, :]
        memory = jnp.transpose(head_norm, (1, 0, 2)).reshape(rows, heads * HEAD).astype(jnp.bfloat16)

        def back(x):
            if inner == 1:
                return x
            return lax.all_to_all(x, "inner", split_axis=0, concat_axis=1, tiled=True)

        result = jnp.dot(back(act), out_conv, preferred_element_type=jnp.float32)
        result = result + jnp.dot(back(memory), out_mem, preferred_element_type=jnp.float32)
        return lax.psum_scatter(
            result.astype(jnp.bfloat16), "tp", scatter_dimension=0, tiled=True
        )

    return shards


def solution(mesh):
    sp, tp = mesh.shape["sp"], mesh.shape["tp"]
    inner = math.gcd(sp, max(MEMORY_HEADS // tp, 1))
    outer = sp // inner
    fine = Mesh(mesh.devices.reshape(outer, inner, tp), ("outer", "inner", "tp"))
    rows = ("outer", "inner")
    in_specs = (
        P(rows, "tp"),
        P(),
        P(rows, "tp"),
        P(rows, "tp"),
        P(None, "tp"),
        P("tp"),
        P("tp"),
        P(rows, "tp"),
        P(rows, "tp"),
        P(rows, "tp"),
        P(),
        P(),
        P(rows, None),
        P("tp"),
        P("tp", None),
        P("tp", None),
    )
    return jax.shard_map(
        make_shards(inner, outer, tp), mesh=fine, in_specs=in_specs,
        out_specs=P(("outer", "inner", "tp"), None), check_vma=False,
    )
```

```python
import functools
import math
import types

import jax
import jax.numpy as jnp
from jax import lax
from jax.experimental import pallas as pl
from jax.experimental.pallas import tpu as pltpu
from jax.sharding import Mesh, PartitionSpec as P

MEMORY_HEADS = 8
HEAD = 256
KW = 31

EPS = 1e-06
PRECISE = lax.Precision.HIGHEST


def parts_of(x):
    first = lax.reduce_precision(x, 8, 7)
    rest = x - first
    second = lax.reduce_precision(rest, 8, 7)
    third = rest - second
    return [p.astype(jnp.bfloat16) for p in (first, second, third)]


def whole_of(a, b, c):
    return a.astype(jnp.float32) + b.astype(jnp.float32) + c.astype(jnp.float32)


MESH = pl.DeviceIdType.MESH


def layer_kernel(outer, inner, tp, names, *refs):
    r = types.SimpleNamespace(**dict(zip(names, refs)))
    tokens, norm_gain = r.tokens, r.norm_gain
    weights = [r.glu_value, r.glu_gate, r.key_weight, r.value_weight, r.query_weight]
    count = len(weights)
    o, i, t = lax.axis_index("outer"), lax.axis_index("inner"), lax.axis_index("tp")
    block, half = tokens.shape
    depth = weights[0].shape[0]
    hb = block // tp
    quarter = inner * block
    groups = outer // tp
    model = half * tp
    channels = MEMORY_HEADS * HEAD
    scale = HEAD ** (-0.5)
    f32, bf16 = jnp.float32, jnp.bfloat16

    par, grp = lax.rem(o, tp), lax.div(o, tp)
    mate = 1 - t
    twin = o + 1 - 2 * par
    primary = t == par
    place = grp * tp + t
    last = outer - 1
    x, y = lax.rem(i, 2), lax.div(i, 2)
    near = [i, y * 2 + 1 - x, (1 - y) * 2 + x, (1 - y) * 2 + 1 - x]
    head = par * inner + i

    nq, nsrc, xin, wst, wfull, ow = r.nq, r.nsrc, r.xin, r.wst, r.wfull, r.ow

    def span(index, size):
        return pl.ds(pl.multiple_of(index * size, size), size)

    def remote(src, dst, send, recv, device):
        return pltpu.make_async_remote_copy(
            src_ref=src, dst_ref=dst, send_sem=send, recv_sem=recv,
            device_id=device, device_id_type=MESH,
        )

    sends = []

    def start(copy, when=None):
        if when is None:
            copy.start()
        else:
            pl.when(when)(copy.start)
        sends.append((copy, when))

    def guarded(when, action):
        pl.when(when)(action)

    local = pltpu.make_async_copy

    own_rows = [local(weights[j], wst.at[j, o], r.own_s.at[j]) for j in range(count)]
    tok_own = local(tokens.at[span(t, hb), :], xin.at[t], r.loc_s.at[0])
    tok_own.start()
    gain_in = local(norm_gain, r.gain, r.loc_s.at[5])
    bias_in = local(r.gate_bias, r.bias, r.loc_s.at[6])
    gain_in.start()
    bias_in.start()

    for copy in own_rows:
        copy.start()

    gate_in = local(r.gate_weight, r.gwp.at[pl.ds(0, r.gate_weight.shape[0]), :], r.loc_s.at[1])
    out_in = [
        local(source, ow.at[k], r.loc_s.at[2 + k]) for k, source in enumerate((r.out_conv, r.out_mem))
    ]

    barrier = pltpu.get_barrier_semaphore()
    greeted = []
    for dz in range(tp):
        for k in range(inner):
            for c in range(tp):
                if (dz, k, c) != (0, 0, 0):
                    greeted.append((o if dz == 0 else twin, near[k], t if c == 0 else mate))
    for step in range(1, groups):
        away = lax.rem(grp + step, groups) * tp
        for dz in range(tp):
            for c in range(tp):
                greeted.append((away + dz, i, c))
    for device in greeted:
        pl.semaphore_signal(barrier, inc=1, device_id=device, device_id_type=MESH)
    pl.semaphore_wait(barrier, len(greeted))

    start(remote(tokens.at[span(mate, hb), :], xin.at[t], r.xin_s, r.xin_r, (o, i, mate)))

    def spread(j, step):
        target = lax.rem(grp + step, groups) * tp + t
        return remote(
            wst.at[j, o], wst.at[j, o], r.w1_s.at[j, step], r.w1_r.at[j, o], (target, i, t)
        )

    moved = (1, 3)

    def plane_of(step):
        return lax.rem(grp + step, groups) * tp

    def hand_over(j):
        at = moved.index(j)
        return remote(wst.at[j, o], r.wmv.at[at], r.mov_s.at[at], r.mov_r.at[at], (o, i, mate))

    def spread_all(j, phase):
        for step in range(groups):
            target = lax.rem(grp + step, groups) * tp + t
            apart = (target - o) * (twin - o) < 0
            if phase == 0:
                when = jnp.logical_and(apart, jnp.logical_not(primary))
            elif phase == 1:
                when = jnp.logical_not(apart)
                if step == 0:
                    when = jnp.logical_and(when, jnp.logical_not(primary))
            else:
                when = jnp.logical_and(apart, primary)
            if step and phase == 1 and j in moved:
                start(spread(j, step), jnp.logical_and(when, primary))
                other = plane_of(step) + mate
                at_end = jnp.logical_and(primary, (other - o) * (twin - o) > 0)

                @pl.when(at_end)
                def _():
                    hand_over(j).wait_recv()

                start(remote(
                    r.wmv.at[moved.index(j)], wst.at[j, o], r.mvd_s.at[moved.index(j)], r.w1_r.at[j, o], (other, i, mate)
                ), at_end)
            elif step or phase == 1:
                start(spread(j, step), when)

    def arrived(j, plane):
        remote(wst.at[j, plane], wst.at[j, plane], r.w1_s.at[j, 0], r.w1_r.at[j, plane], (o, i, mate)).wait_recv()

    def row_block(owner_plane, owner):
        return pl.ds(pl.multiple_of((owner_plane * inner + owner) * depth, depth), depth)

    by_second = (4,)

    def keep(j, plane_at):
        return local(
            wst.at[j, plane_at, :, span(i, HEAD)], wfull.at[j, row_block(plane_at, i), :], r.keep_s.at[j]
        )

    def deal(j, plane_at, k):
        return remote(
            wst.at[j, plane_at, :, span(near[k], HEAD)],
            wfull.at[j, row_block(plane_at, i), :],
            r.w2_s.at[j], r.w2_r.at[j, plane_at], (o, near[k], mate if j in by_second else t),
        )

    def deal_planes(j):
        base = plane_of(1)
        nearer, farther = base + jnp.where(base < o, 1, 0), base + jnp.where(base < o, 0, 1)
        at_end = (nearer - o) * (twin - o) > 0
        return [o, jnp.where(at_end, twin, nearer), farther, jnp.where(at_end, nearer, twin)]

    def deal_all(j, which=None):
        @pl.when(primary)
        def _():
            for index, plane_at in enumerate(deal_planes(j)):
                if which is not None and index not in which:
                    continue
                if index:
                    arrived(j, plane_at)
                for k in range(0 if j in by_second else 1, inner):
                    deal(j, plane_at, k).start()
                if j not in by_second:
                    keep(j, plane_at).start()

    def share(j, plane_at):
        rows = pl.ds(pl.multiple_of(plane_at * inner * depth, inner * depth), inner * depth)
        return remote(
            wfull.at[j, rows, :], wfull.at[j, rows, :],
            r.fw_s.at[j], r.fw_r.at[j], (o, i, mate),
        )

    def received(ref, semaphore):
        remote(ref, ref, semaphore, semaphore, (o, i, mate)).wait_recv()

    def gather(j, which=None):
        second = j in by_second

        @pl.when(jnp.logical_not(primary) if second else primary)
        def _():
            if not second and (which is None or 0 in which):
                local(wst.at[j, 0], wst.at[j, 0], r.keep_s.at[j]).wait()
            for index, plane_at in enumerate(deal_planes(j)):
                if which is not None and index not in which:
                    continue
                start_row = pl.multiple_of(plane_at * inner * depth, depth)
                rows = (inner if second else inner - 1) * depth
                received(wfull.at[j, pl.ds(start_row, rows), :], r.w2_r.at[j, plane_at])
                share(j, plane_at).start()

    def handed(j):
        @pl.when(primary if j in by_second else jnp.logical_not(primary))
        def _():
            received(wfull.at[j], r.fw_r.at[j])

    def collect(j, which=None):
        gather(j, which)
        handed(j)

    small = ((r.conv_taps, r.taps), (r.ln_gain, r.lng), (r.ln_bias, r.lnb), (r.mem_gain, r.mgn))
    own_small = [
        local(a.at[:, span(i, HEAD)], b, r.sml_s.at[k]) for k, (a, b) in enumerate(small)
    ]
    mate_small = [
        remote(a.at[:, span(i, HEAD)], b, r.prm_s.at[k], r.prm_r.at[k], (o, i, mate))
        for k, (a, b) in enumerate(small)
    ]
    for j in range(count):
        own_rows[j].wait()
        spread_all(j, 0)
        if j in moved:
            at_end = (plane_of(1) + t - o) * (twin - o) > 0
            start(hand_over(j), jnp.logical_and(jnp.logical_not(primary), at_end))

    @pl.when(primary)
    def _():
        for copy in own_small:
            copy.start()
        for copy in mate_small:
            copy.start()

    ext = r.ext
    plane = jnp.where(primary, o, twin)
    own_ext = local(r.extra, ext.at[i], r.loc_s.at[4])
    guarded(primary, own_ext.start)
    for k in range(inner):
        copy = remote(r.extra, ext.at[i], r.ext_s.at[k], r.ext_r.at[i], (plane, near[k], par))
        start(copy, None if k else jnp.logical_not(primary))

    early = 2
    for j in range(early):
        deal_all(j, (0,))
    gate_in.start()
    for copy in out_in:
        copy.start()

    tok_own.wait()
    gain_in.wait()
    remote(xin.at[mate], xin.at[mate], r.xin_s, r.xin_r, (o, i, mate)).wait_recv()
    norm_rows = 32
    pieces = 2
    piece_rows = hb // pieces

    def norm_step(m, carry):
        at = span(m, norm_rows)
        parts = [xin[f, at, :].astype(f32) for f in range(tp)]
        square = sum(jnp.sum(p * p, axis=-1, keepdims=True) for p in parts)
        level = lax.rsqrt(square * (1.0 / model) + EPS)
        for f in range(tp):
            row = (parts[f] * level * r.gain[:, pl.ds(f * half, half)]).astype(bf16)
            nsrc[at, pl.ds(f * half, half)] = row

            @pl.when(primary)
            def _():
                nq[pl.ds(pl.multiple_of(i * block + t * hb + m * norm_rows, norm_rows), norm_rows), pl.ds(f * half, half)] = row
        return carry

    def rows_of(b, c, s):
        return nq.at[pl.ds(pl.multiple_of(b * block + c * hb + s * piece_rows, piece_rows), piece_rows), :]

    def tok_wait(b, c, s):
        rows = rows_of(b, c, s)
        remote(rows, rows, r.tok_s.at[0, 0], r.tok_r.at[b, c, s], (o, i, mate)).wait_recv()

    steps = piece_rows // norm_rows
    for s in range(pieces):
        lax.fori_loop(s * steps, (s + 1) * steps, norm_step, 0)
        source = nsrc.at[pl.ds(s * piece_rows, piece_rows), :]
        start(remote(source, rows_of(i, t, s), r.tok_s.at[1, s], r.tok_r.at[i, t, s], (twin, i, par)))
        start(remote(source, rows_of(i, t, s), r.tok_s.at[0, s], r.tok_r.at[i, t, s], (o, i, mate)), jnp.logical_not(primary))
    for j in range(count):
        spread_all(j, 1)

    def pass_on(b_from, c, s, k, slot):
        rows = rows_of(b_from, c, s)
        target = near[k] if isinstance(k, int) else jnp.where(k == 1, near[1], near[2])
        return remote(rows, rows, r.pas_s, r.tok_r.at[b_from, c, s], (o, target, t))

    @pl.when(primary)
    def _():
        for s in range(pieces):
            pass_on(i, t, s, 1 + t, 0).start()
        for s in range(pieces):
            tok_wait(i, mate, s)
            pass_on(i, mate, s, 1 + mate, 1).start()
        for s in range(pieces):
            pass_on(i, t, s, 1 + mate, 2).start()
            pass_on(i, mate, s, 1 + t, 3).start()

    @pl.when(jnp.logical_not(primary))
    def _():
        for s in range(pieces):
            for c, slot in ((0, 0), (1, 1)):
                tok_wait(i, c, s)
                pass_on(i, c, s, 1 + c, slot).start()
        for s in range(pieces):
            for c, slot in ((0, 2), (1, 3)):
                pass_on(i, c, s, 2 - c, slot).start()

    for s in range(pieces):
        tok_wait(near[1], 0, s)
        pass_on(near[1], 0, s, 2, 4).start()
        tok_wait(near[2], 1, s)
        pass_on(near[2], 1, s, 1, 5).start()
    for j in range(count):
        spread_all(j, 2)
    received(nq.at[pl.ds(0, (inner - 1) * block), :], r.pas_s)

    @pl.when(jnp.logical_not(primary))
    def _():
        pl.semaphore_signal(r.clear, inc=1, device_id=(o, i, mate), device_id_type=MESH)

    for s in range(pieces):
        tok_wait(near[1], 1, s)
        tok_wait(near[2], 0, s)
        tok_wait(near[3], 0, s)
        tok_wait(near[3], 1, s)

    gwp, gt, rowsv, colsv = r.gwp, r.gt, r.rowsv, r.colsv
    gate_in.wait()
    bias_in.wait()
    bias_row = jnp.concatenate([r.bias[...], jnp.zeros((1, LANES - r.bias.shape[1]), f32)], axis=1)

    def chunk(n):
        return span(n, block)

    def gate_step(n, carry):
        got = lax.dot_general(
            nq[chunk(n), :], gwp[...], (((1,), (1,)), ((), ())), preferred_element_type=f32
        )
        gt[:, chunk(n)] = (got + bias_row).T[: gt.shape[0]]
        return carry

    lax.fori_loop(0, inner, gate_step, 0)
    guarded(primary, own_ext.wait)
    for k in range(inner):
        def hear(k=k):
            remote(r.extra, ext.at[near[k]], r.ext_s.at[0], r.ext_r.at[near[k]], (o, i, mate)).wait_recv()
        if k:
            hear()
        else:
            guarded(jnp.logical_not(primary), hear)

    mine = lax.broadcasted_iota(jnp.int32, (MEMORY_HEADS, quarter), 0) == head
    mine_block = lax.broadcasted_iota(jnp.int32, (MEMORY_HEADS, block), 0) == head

    def gate_row(g):
        rows = gt[pl.ds(g * MEMORY_HEADS, MEMORY_HEADS), :]
        return jnp.sum(jnp.where(mine, rows, 0.0), axis=0, keepdims=True)

    def extra_row(d):
        pieces = [
            jnp.sum(jnp.where(mine_block, ext[b, pl.ds(d * MEMORY_HEADS, MEMORY_HEADS), :], 0.0), axis=0, keepdims=True)
            for b in range(inner)
        ]
        return jnp.concatenate(pieces, axis=1)

    def log_sigmoid(v):
        return jnp.minimum(v, 0.0) - jnp.log1p(jnp.exp(-jnp.abs(v)))

    within = lax.rem(lax.broadcasted_iota(jnp.int32, (1, quarter), 1), block)

    def scan(v, forward, join, empty):
        step = 1
        while step < block:
            if forward:
                v = join(v, jnp.where(within >= step, pltpu.roll(v, step, 1), empty))
            else:
                v = join(v, jnp.where(within < block - step, pltpu.roll(v, quarter - step, 1), empty))
            step *= 2
        return v

    table = []
    for d in range(2):
        gate_in_row = gate_row(2 * d)
        forget = log_sigmoid(gate_row(2 * d + 1)) + extra_row(d)
        decay = scan(forget, d == 0, jnp.add, 0.0)
        shifted = gate_in_row - decay
        running = scan(shifted, d == 0, jnp.maximum, -jnp.inf)
        table += [shifted, running, decay]
    table += [jnp.zeros((1, quarter), f32)] * 2
    rowsv[...] = jnp.concatenate(table, axis=0)

    def turn_step(n, carry):
        piece = rowsv[:, chunk(n)]
        wide = jnp.concatenate([piece, jnp.zeros((LANES - piece.shape[0], block), f32)], axis=0)
        colsv[chunk(n), :] = wide.T
        return carry

    lax.fori_loop(0, inner, turn_step, 0)

    @pl.when(primary)
    def _():
        pl.semaphore_wait(r.clear, 1)

    deal_all(0, range(1, outer))
    deal_all(1, range(1, outer))
    deal_all(2, range(2))

    def project(n, j):
        return jnp.dot(nq[chunk(n), :], wfull[j], preferred_element_type=f32)

    kb, vb, cm, cv = r.kb, r.vb, r.cm, r.cv
    smat, sinfo, matx, infox = r.smat, r.sinfo, r.matx, r.infox
    gmat, ginfo, gin, gininfo = r.gmat, r.ginfo, r.gin, r.gininfo

    def key_step(n, carry):
        keys = project(n, 2)
        kb[chunk(n), :] = keys.astype(bf16)
        wide = keys.astype(bf16).astype(f32)
        cols = colsv[chunk(n), :]
        for d in range(2):
            end = block - 1 if d == 0 else 0
            top = cols[end : end + 1, 3 * d + 1 : 3 * d + 2]
            weighted = wide * (jnp.exp(cols[:, 3 * d : 3 * d + 1] - top) * scale)
            r.kwt[d, :, chunk(n)] = weighted.T.astype(bf16)
            cv[d, n] = jnp.broadcast_to(jnp.sum(weighted, axis=0, keepdims=True), (8, HEAD))
        return carry

    def state_step(m, carry):
        ns = [m * 2 + p for p in range(2)]
        values = [project(n, 3).astype(bf16) for n in ns]
        for n, value in zip(ns, values):
            vb[chunk(n), :] = value
        for n, value in zip(ns, values):
            for d in range(2):
                cm[d, n] = jnp.dot(r.kwt[d, :, chunk(n)], value, preferred_element_type=f32)
        return carry

    earlier = lax.broadcasted_iota(jnp.int32, (block, block), 0) >= lax.broadcasted_iota(jnp.int32, (block, block), 1)
    later = lax.broadcasted_iota(jnp.int32, (block, block), 0) <= lax.broadcasted_iota(jnp.int32, (block, block), 1)

    def weight_step(n, carry):
        cols = colsv[chunk(n), :]
        rows = rowsv[:, chunk(n)]
        for d in range(2):
            gap = jnp.minimum(rows[3 * d : 3 * d + 1] - cols[:, 3 * d + 1 : 3 * d + 2], 0.0)
            r.wgt[d, n] = jnp.where(earlier if d == 0 else later, jnp.exp(gap) * scale, 0.0)
        return carry

    lax.fori_loop(0, inner, weight_step, 0)
    collect(0)
    gpad, conv, hsend, hrecv = r.gpad, r.conv, r.hsend, r.hrecv
    pad = hsend.shape[1]
    reach = KW // 2
    sides = HEAD // LANES

    def value_step(n, carry):
        r.gval[chunk(n), :] = project(n, 0)
        return carry

    lax.fori_loop(0, inner, value_step, 0)
    deal_all(2, range(2, outer))
    deal_all(3, range(2))
    collect(1)

    def glu_step(n, carry):
        glu = (r.gval[chunk(n), :] * jax.nn.sigmoid(project(n, 1))).astype(bf16)
        for side in range(sides):
            gpad[side, pl.ds(pl.multiple_of(n * block + pad, pad), block), :] = glu[:, side * LANES : (side + 1) * LANES].astype(f32)

        @pl.when(n == 0)
        def _():
            hsend[0] = glu[:pad]

        @pl.when(n == inner - 1)
        def _():
            hsend[1] = glu[block - pad :]

        return carry

    lax.fori_loop(0, inner, glu_step, 0)
    def device_of(q):
        return (lax.div(q, tp) * tp + par, i, lax.rem(q, tp))

    has_before, has_after = place > 0, place < last
    start(remote(hsend.at[0], hrecv.at[1], r.hal_s.at[0], r.hal_r.at[1], device_of(jnp.maximum(place - 1, 0))), has_before)
    start(remote(hsend.at[1], hrecv.at[0], r.hal_s.at[1], r.hal_r.at[0], device_of(jnp.minimum(place + 1, last))), has_after)

    @pl.when(primary)
    def _():
        for copy in own_small:
            copy.wait()

    @pl.when(jnp.logical_not(primary))
    def _():
        for copy in mate_small:
            copy.wait_recv()

    deal_all(3, range(2, outer))
    taps, statc, stbuf = r.taps, r.statc, r.stbuf
    conv_rows = 64
    lane = lax.broadcasted_iota(jnp.int32, (conv_rows, LANES), 1)
    shift = pad - reach

    def conv_step(m, carry):
        s1 = s2 = 0.0
        for side in range(sides):
            total = jnp.zeros((conv_rows, LANES), f32)
            for residue in range(8):
                moved = gpad[side, pl.ds(m * conv_rows + residue, conv_rows + 2 * pad - 8), :]
                for j in range(KW):
                    at = j + shift - residue
                    if at % 8 == 0:
                        tap = taps[pl.ds(j, 1), pl.ds(side * LANES, LANES)]
                        total = total + tap * moved[at : at + conv_rows]
            conv[side, span(m, conv_rows), :] = total
            s1 = s1 + total
            s2 = s2 + total * total
        s1 = jnp.sum(s1, axis=-1, keepdims=True)
        s2 = jnp.sum(s2, axis=-1, keepdims=True)
        statc[span(m, conv_rows), :] = jnp.where(lane == 0, s1, jnp.where(lane == 1, s2, 0.0))
        return carry

    conv_steps = quarter // conv_rows
    lax.fori_loop(1, conv_steps // 2, conv_step, 0)
    deal_all(4, range(2))
    collect(2)
    lax.fori_loop(conv_steps // 2, conv_steps - 1, conv_step, 0)
    for edge, present, at in ((0, has_before, 0), (1, has_after, pad + quarter)):
        @pl.when(present)
        def _():
            remote(hrecv.at[edge], hrecv.at[edge], r.hal_s.at[0], r.hal_r.at[edge], (o, i, mate)).wait_recv()
            for side in range(sides):
                gpad[side, pl.ds(at, pad), :] = hrecv[edge, :, side * LANES : (side + 1) * LANES].astype(f32)

        @pl.when(jnp.logical_not(present))
        def _():
            for side in range(sides):
                gpad[side, pl.ds(at, pad), :] = jnp.zeros((pad, LANES), f32)

    lax.fori_loop(0, 2, lambda m, carry: conv_step(m * (conv_steps - 1), carry), 0)
    sums = r.sums
    two = pl.ds(0, 2)

    def sums_step(n, carry):
        sums[:, chunk(n)] = statc[chunk(n), :].T[: sums.shape[0]]
        return carry

    lax.fori_loop(0, inner, sums_step, 0)
    peers = []
    for dz in range(tp):
        for k in range(inner):
            if (dz, k) != (0, 0):
                peers.append((o if dz == 0 else twin, near[k]))
    for index, (plane_to, chip) in enumerate(peers):
        remote(sums.at[two, :], stbuf.at[head, two, :], r.sta_s, r.sta_r, (plane_to, chip, t)).start()
    deal_all(4, range(2, outer))
    gather(3, range(2))
    lax.fori_loop(0, inner, key_step, 0)
    collect(3, range(2, outer))
    lax.fori_loop(0, inner // 2, state_step, 0)

    def corner(n, d, column):
        end = block - 1 if d == 0 else 0
        at = n * block + end
        return colsv[pl.ds(at, 1), :][:, column : column + 1]

    totals = [[corner(n, d, 3 * d + 2) for n in range(inner)] for d in range(2)]
    levels = [[corner(n, d, 3 * d + 1) + totals[d][n] for n in range(inner)] for d in range(2)]
    for d in range(2):
        reaches = []
        for n in range(inner):
            later = range(n + 1, inner) if d == 0 else range(n)
            value = levels[d][n]
            for m in later:
                value = value + totals[d][m]
            reaches.append(value)
        top = functools.reduce(jnp.maximum, reaches)
        shares = [jnp.exp(v - top) for v in reaches]
        matx[d] = sum(shares[n] * cm[d, n] for n in range(inner)).astype(bf16)
        vec = sum(shares[n] * cv[d, n] for n in range(inner))
        row = lax.broadcasted_iota(jnp.int32, (8, HEAD), 0)
        decay = functools.reduce(jnp.add, totals[d])
        infox[d] = jnp.where(row == 0, vec, jnp.where(row == 1, top, decay))

    start(remote(matx, smat, r.mat_s.at[0], r.mat_r.at[0], (o, i, mate)))
    start(remote(infox, sinfo, r.inf_s.at[0], r.inf_r.at[0], (o, i, mate)))
    gather(4, range(2))
    received(stbuf.at[pl.ds(0, MEMORY_HEADS - 1), two, :], r.sta_r)
    stbuf[head] = sums[...]

    def stat_step(n, carry):
        whole = stbuf[0, :, chunk(n)]
        for k in range(1, MEMORY_HEADS):
            whole = whole + stbuf[k, :, chunk(n)]
        whole = whole * (1.0 / channels)
        mean = whole[0:1]
        rstd = lax.rsqrt(whole[1:2] - mean * mean + EPS)
        wide = jnp.concatenate([mean, rstd, jnp.zeros((LANES - 2, block), f32)], axis=0)
        statc[chunk(n), :] = wide.T
        return carry

    lax.fori_loop(0, inner, stat_step, 0)
    actb, memb, cin = r.actb, r.memb, r.cin

    def give(which, source, b):
        return remote(
            source.at[chunk(b), :], cin.at[which, i], r.ret_s.at[which, b], r.ret_r.at[which, i],
            (plane, b, par),
        )

    def give_own(which, source):
        return local(source.at[chunk(i), :], cin.at[which, i], r.rel_s.at[which])

    def give_rows(which, source, b):
        to_self = jnp.logical_and(primary, b == i)
        guarded(to_self, give_own(which, source).start)
        guarded(jnp.logical_not(to_self), give(which, source, b).start)

    order = [jnp.where(primary, near[a], near[b]) for a, b in zip((1, 2, 3, 0), (2, 1, 3, 0))]

    def act_step(n, carry):
        for half_at in range(2):
            rows = pl.ds(pl.multiple_of(n * block + half_at * (block // 2), block // 2), block // 2)
            cols = statc[rows, :]
            for side in range(sides):
                lanes = pl.ds(side * LANES, LANES)
                normal = (conv[side, rows, :] - cols[:, 0:1]) * cols[:, 1:2] * r.lng[:, lanes] + r.lnb[:, lanes]
                actb[rows, lanes] = (normal * jax.nn.sigmoid(normal)).astype(bf16)
        return carry

    lax.fori_loop(0, inner, act_step, 0)

    mat_rows = gin.at[span(t, HEAD // tp), :]
    mate_rows = gin.at[span(mate, HEAD // tp), :]
    remote(matx, smat, r.mat_s.at[0], r.mat_r.at[0], (o, i, mate)).wait_recv()
    remote(infox, sinfo, r.inf_s.at[0], r.inf_r.at[0], (o, i, mate)).wait_recv()
    ours, theirs = infox[grp], sinfo[grp]
    is_far = t == grp
    our_reach = ours[1:2, 0:1] + jnp.where(is_far, theirs[2:3, 0:1], 0.0)
    their_reach = theirs[1:2, 0:1] + jnp.where(is_far, 0.0, ours[2:3, 0:1])
    group_level = jnp.maximum(our_reach, their_reach)
    our_share, their_share = jnp.exp(our_reach - group_level), jnp.exp(their_reach - group_level)
    gmat[...] = (our_share * matx[grp].astype(f32) + their_share * smat[grp].astype(f32)).astype(bf16)
    state_row = lax.broadcasted_iota(jnp.int32, (8, HEAD), 0)
    ginfo[...] = jnp.where(state_row == 0, our_share * ours[0:1] + their_share * theirs[0:1], group_level)
    across = ((1 - grp) * tp + par, i, t)
    start(remote(gmat.at[span(t, HEAD // tp), :], mat_rows, r.mat_s.at[1], r.mat_r.at[1], across))
    start(remote(ginfo, gininfo, r.inf_s.at[1], r.inf_r.at[1], across))
    for b in order:
        give_rows(0, actb, b)
    gather(4, range(2, outer))
    nvs, levs = r.nvs, r.levs
    for d in range(2):
        by_mate = t == 1 - d
        level = jnp.where(by_mate, sinfo[d][1:2, 0:1], LOW_START)
        present = jnp.where(by_mate, 1.0, 0.0)
        mat = present * smat[d].astype(f32)
        vec = present * sinfo[d][0:1]
        for n in (range(inner) if d == 0 else range(inner - 1, -1, -1)):
            high = mat.astype(bf16)
            r.cst[d, n, pl.ds(0, HEAD), :] = high
            r.cst[d, n, pl.ds(HEAD, HEAD), :] = (mat - high.astype(f32)).astype(bf16)
            nvs[d, n] = jnp.broadcast_to(vec, (8, HEAD))
            levs[d, n] = jnp.broadcast_to(level, (8, LANES))
            carried = level + totals[d][n]
            new_level = jnp.maximum(carried, levels[d][n])
            kept, added = jnp.exp(carried - new_level), jnp.exp(levels[d][n] - new_level)
            mat = kept * mat + added * cm[d, n]
            vec = kept * vec + added * cv[d, n][0:1]
            level = new_level

    first_group = grp == 0

    def along(values):
        return jnp.concatenate([jnp.broadcast_to(v, (1, block)) for v in values], axis=1)

    kept, tops = [], []
    for d in range(2):
        running, decay = rowsv[pl.ds(3 * d + 1, 1), :], rowsv[pl.ds(3 * d + 2, 1), :]
        level = along([levs[d, n][0:1, 0:1] for n in range(inner)])
        top = jnp.maximum(running, level)
        tops.append((top, decay))
        kept.append([jnp.exp(running - top), jnp.exp(level - top), jnp.exp(-top - decay)])
    alone = [jnp.where(first_group, a, b) for a, b in zip(*kept)]
    joined = [jnp.where(first_group, b, a) for a, b in zip(*kept)]
    joined_top, joined_decay = (jnp.where(first_group, b, a) for a, b in zip(*tops))
    r.colw[:, pl.ds(0, 8)] = jnp.concatenate(alone + joined + [jnp.zeros((2, quarter), f32)], axis=0).T
    handed(4)


    def query_rows(ns):
        queries = [project(n, 4).astype(bf16) for n in ns]
        scores = [
            lax.dot_general(q, kb[chunk(n), :], (((1,), (1,)), ((), ())), preferred_element_type=f32)
            for n, q in zip(ns, queries)
        ]
        for n, q in zip(ns, queries):
            r.qb[chunk(n), :] = q
        for role, d in ((0, grp), (1, 1 - grp)):
            for n, q, score in zip(ns, queries, scores):
                cols = r.colw[chunk(n), :]
                local_weight, carry_weight = cols[:, 3 * role : 3 * role + 1], cols[:, 3 * role + 1 : 3 * role + 2]
                part = score * r.wgt[d, n]
                num = jnp.dot(part.astype(bf16), vb[chunk(n), :], preferred_element_type=f32)
                far = jnp.dot(jnp.concatenate([q, q], axis=1), r.cst[d, n], preferred_element_type=f32)
                num = local_weight * num + carry_weight * far
                far_sum = jnp.sum(q.astype(f32) * nvs[d, n][0:1], axis=-1, keepdims=True)
                den = local_weight * jnp.sum(part, axis=-1, keepdims=True) + carry_weight * far_sum
                if role == 0:
                    r.alone[chunk(n), :] = num * (1.0 / jnp.maximum(jnp.abs(den), cols[:, 2:3]))
                else:
                    r.numj[chunk(n), :] = num
                    r.denj[chunk(n), :] = jnp.broadcast_to(den, (block, LANES))

    query_rows([0, 1])
    query_rows([2])
    remote(mat_rows, mat_rows, r.mat_s.at[1], r.mat_r.at[1], (o, i, mate)).wait_recv()
    start(remote(mat_rows, mat_rows, r.mat_s.at[2], r.mat_r.at[2], (o, i, mate)))
    query_rows([3])
    remote(ginfo, gininfo, r.inf_s.at[1], r.inf_r.at[1], (o, i, mate)).wait_recv()
    remote(mate_rows, mate_rows, r.mat_s.at[2], r.mat_r.at[2], (o, i, mate)).wait_recv()

    arriving = gininfo[1:2, 0:1] + jnp.where(t == grp, sinfo[1 - grp][2:3, 0:1], 0.0)
    group_levels = []
    for n in range(inner):
        lost_f = functools.reduce(jnp.add, totals[0][:n], jnp.zeros((1, 1), f32))
        lost_b = functools.reduce(jnp.add, totals[1][n + 1 :], jnp.zeros((1, 1), f32))
        group_levels.append(arriving + jnp.where(first_group, lost_b, lost_f))
    level = along(group_levels)
    top = jnp.maximum(joined_top, level)
    kept = [jnp.exp(joined_top - top), jnp.exp(level - top), jnp.exp(-top - joined_decay)]
    r.colw[:, pl.ds(0, 8)] = jnp.concatenate(kept + [jnp.zeros((5, quarter), f32)], axis=0).T

    def memory_rows(ns):
        queries = [r.qb[chunk(n), :] for n in ns]
        fars = [jnp.dot(q, gin[...], preferred_element_type=f32) for q in queries]
        far_sums = [jnp.sum(q.astype(f32) * gininfo[0:1], axis=-1, keepdims=True) for q in queries]
        for n, far, far_sum in zip(ns, fars, far_sums):
            cols = r.colw[chunk(n), :]
            den = cols[:, 0:1] * r.denj[chunk(n), pl.ds(0, 1)] + cols[:, 1:2] * far_sum
            share_of = 1.0 / jnp.maximum(jnp.abs(den), cols[:, 2:3])
            out = r.alone[chunk(n), :] + (
                r.numj[chunk(n), :] * (cols[:, 0:1] * share_of) + far * (cols[:, 1:2] * share_of)
            )
            level = lax.rsqrt(jnp.mean(out * out, axis=-1, keepdims=True) + EPS)
            memb[chunk(n), :] = (out * level * r.mgn[...]).astype(bf16)
        for n in ns:
            give_rows(1, memb, n)

    for ns in ([order[0]], [order[1]], [order[2], order[3]]):
        memory_rows(ns)
    acc, pbuf = r.acc, r.pbuf
    tile = half
    tiles = tp

    def take(which, k):
        def hear():
            rows = cin.at[which, near[k]]
            remote(rows, rows, r.ret_s.at[which, 0], r.ret_r.at[which, near[k]], (o, i, mate)).wait_recv()

        if k:
            hear()
        else:
            guarded(jnp.logical_not(primary), hear)
            guarded(primary, give_own(which, actb).wait)

    def part(which, n):
        return sum(
            jnp.dot(cin[which, k], ow[which, pl.ds(k * HEAD, HEAD), span(n, tile)], preferred_element_type=f32)
            for k in range(inner)
        )

    def conv_out_step(n, carry):
        acc[:, span(n, tile)] = part(0, n)
        return carry

    for copy in out_in:
        copy.wait()
    for k in range(inner):
        take(0, k)
    lax.fori_loop(0, tiles, conv_out_step, 0)

    def rows_part(ks, n):
        return sum(
            jnp.dot(
                cin[1, near[k]], ow[1, pl.ds(pl.multiple_of(near[k] * HEAD, HEAD), HEAD), span(n, tile)],
                preferred_element_type=f32,
            )
            for k in ks
        )

    def add_step(n, carry):
        acc[:, span(n, tile)] += rows_part((1, 2), n)
        return carry

    take(1, 1)
    take(1, 2)
    lax.fori_loop(0, tiles, add_step, 0)
    take(1, 3)
    take(1, 0)
    out_own, out_mate = r.out_own, r.out_mate

    def piece(n):
        return remote(
            pbuf.at[span(mate, hb), span(n, tile)], out_mate.at[:, span(n, tile)],
            r.fin_s, r.fin_r, (o, i, mate),
        )

    def stay(n):
        return local(pbuf.at[span(t, hb), span(n, tile)], out_own.at[:, span(n, tile)], r.fil_s)

    def mem_out_step(n, carry):
        pbuf[:, span(n, tile)] = (acc[:, span(n, tile)] + rows_part((3, 0), n)).astype(bf16)
        piece(n).start()
        stay(n).start()
        return carry

    lax.fori_loop(0, tiles, mem_out_step, 0)

    for copy, when in sends:
        if when is None:
            copy.wait_send()
        else:
            pl.when(when)(copy.wait_send)


    received(stbuf.at[pl.ds(0, MEMORY_HEADS - 1), two, :], r.sta_s)

    @pl.when(primary)
    def _():
        for copy in mate_small:
            copy.wait_send()
        for j in range(count):
            received(wst.at[j] if j in by_second else wst.at[j, pl.ds(0, inner - 1)], r.w2_s.at[j])
            if j not in by_second:
                received(wfull.at[j], r.fw_s.at[j])

    @pl.when(jnp.logical_not(primary))
    def _():
        for j in by_second:
            received(wfull.at[j], r.fw_s.at[j])

    for which, source in ((0, actb), (1, memb)):
        for b in range(inner):
            guarded(jnp.logical_not(jnp.logical_and(primary, i == b)), give(which, source, b).wait_send)
    local(out_own, out_own, r.fil_s).wait()
    received(out_mate, r.fin_s)
    received(out_mate, r.fin_r)


LANES = 128
LOW_START = -1e30


def whole_layer(outer, inner, tp, args):
    tokens = args.tokens
    block, half = tokens.shape
    depth = args.glu_value.shape[0]
    count = 5
    quarter, model = inner * block, half * tp
    hb = block // tp
    pad = 16
    f32, bf16 = jnp.float32, jnp.bfloat16
    dma = pltpu.SemaphoreType.DMA
    tiles = tp
    extra = args.log_decay_extra.T
    operands = dict(
        tokens=tokens, norm_gain=args.norm_gain[None],
        glu_value=args.glu_value, glu_gate=args.glu_gate,
        key_weight=args.key_weight, value_weight=args.value_weight, query_weight=args.query_weight,
        conv_taps=args.conv_taps, ln_gain=args.ln_gain[None], ln_bias=args.ln_bias[None],
        gate_weight=args.gate_weight.T, gate_bias=args.gate_bias[None],
        extra=extra, mem_gain=args.mem_gain[None],
        out_conv=args.out_conv, out_mem=args.out_mem,
    )
    scratch = dict(
        nq=pltpu.VMEM((quarter, model), bf16),
        nsrc=pltpu.VMEM((hb, model), bf16),
        xin=pltpu.VMEM((tp, hb, half), bf16),
        wst=pltpu.VMEM((count, outer, depth, half), bf16),
        wfull=pltpu.VMEM((count, model, HEAD), bf16),
        wmv=pltpu.VMEM((2, depth, half), bf16),
        ow=pltpu.VMEM((2,) + args.out_conv.shape, bf16),
        taps=pltpu.VMEM((KW, HEAD), f32), lng=pltpu.VMEM((1, HEAD), f32),
        lnb=pltpu.VMEM((1, HEAD), f32), mgn=pltpu.VMEM((1, HEAD), f32),
        ext=pltpu.VMEM((inner,) + extra.shape, f32),
        gwp=pltpu.VMEM((LANES, model), bf16),
        gain=pltpu.VMEM((1, model), f32), bias=pltpu.VMEM((1, 4 * MEMORY_HEADS), f32),
        gt=pltpu.VMEM((4 * MEMORY_HEADS, quarter), f32),
        rowsv=pltpu.VMEM((8, quarter), f32), colsv=pltpu.VMEM((quarter, LANES), f32),
        gpad=pltpu.VMEM((HEAD // LANES, quarter + 2 * pad, LANES), f32),
        conv=pltpu.VMEM((HEAD // LANES, quarter, LANES), f32), gval=pltpu.VMEM((quarter, HEAD), f32),
        hsend=pltpu.VMEM((2, pad, HEAD), bf16), hrecv=pltpu.VMEM((2, pad, HEAD), bf16),
        statc=pltpu.VMEM((quarter, LANES), f32), sums=pltpu.VMEM((8, quarter), f32),
        stbuf=pltpu.VMEM((MEMORY_HEADS, 8, quarter), f32),
        kb=pltpu.VMEM((quarter, HEAD), bf16), vb=pltpu.VMEM((quarter, HEAD), bf16),
        cm=pltpu.VMEM((2, inner, HEAD, HEAD), f32), cv=pltpu.VMEM((2, inner, 8, HEAD), f32),
        matx=pltpu.VMEM((2, HEAD, HEAD), bf16), infox=pltpu.VMEM((2, 8, HEAD), f32),
        smat=pltpu.VMEM((2, HEAD, HEAD), bf16), sinfo=pltpu.VMEM((2, 8, HEAD), f32),
        gmat=pltpu.VMEM((HEAD, HEAD), bf16), ginfo=pltpu.VMEM((8, HEAD), f32),
        gin=pltpu.VMEM((HEAD, HEAD), bf16), gininfo=pltpu.VMEM((8, HEAD), f32),
        cst=pltpu.VMEM((2, inner, 2 * HEAD, HEAD), bf16), qb=pltpu.VMEM((quarter, HEAD), bf16), kwt=pltpu.VMEM((2, HEAD, quarter), bf16),
        alone=pltpu.VMEM((quarter, HEAD), f32), numj=pltpu.VMEM((quarter, HEAD), f32), denj=pltpu.VMEM((quarter, LANES), f32),
        wgt=pltpu.VMEM((2, inner, block, block), f32), colw=pltpu.VMEM((quarter, LANES), f32),
        nvs=pltpu.VMEM((2, inner, 8, HEAD), f32), levs=pltpu.VMEM((2, inner, 8, LANES), f32),
        actb=pltpu.VMEM((quarter, HEAD), bf16), memb=pltpu.VMEM((quarter, HEAD), bf16),
        cin=pltpu.VMEM((2, inner, block, HEAD), bf16),
        acc=pltpu.VMEM((block, model), f32), pbuf=pltpu.VMEM((block, model), bf16),
        own_s=dma((count,)), mov_s=dma((2,)), mov_r=dma((2,)), mvd_s=dma((2,)), loc_s=dma((7,)), xin_s=dma, xin_r=dma,
        w1_s=dma((count, outer // tp)), w1_r=dma((count, outer)),
        sml_s=dma((4,)), prm_s=dma((4,)), prm_r=dma((4,)),
        ext_s=dma((inner,)), ext_r=dma((inner,)),
        tok_s=dma((2, 2)), tok_r=dma((inner, tp, 2)), pas_s=dma, clear=pltpu.SemaphoreType.REGULAR,
        w2_s=dma((count,)), w2_r=dma((count, outer)),
        keep_s=dma((count,)), fw_s=dma((count,)), fw_r=dma((count,)),
        hal_s=dma((2,)), hal_r=dma((2,)),
        sta_s=dma, sta_r=dma,
        mat_s=dma((3,)), mat_r=dma((3,)), inf_s=dma((2,)), inf_r=dma((2,)),
        ret_s=dma((2, inner)), ret_r=dma((2, inner)), rel_s=dma((2,)),
        fin_s=dma, fin_r=dma, fil_s=dma,
    )
    any_space = pl.BlockSpec(memory_space=pl.ANY)
    spaces = {n: any_space for n in operands}
    names = list(operands) + ["out_own", "out_mate"] + list(scratch)
    shape = pltpu.VMEM((hb, model), bf16)
    own, mate = pl.pallas_call(
        functools.partial(layer_kernel, outer, inner, tp, names),
        out_shape=(shape, shape),
        in_specs=[spaces[n] for n in operands],
        out_specs=(any_space, any_space),
        scratch_shapes=list(scratch.values()),
        compiler_params=pltpu.CompilerParams(
            collective_id=0, has_side_effects=True, vmem_limit_bytes=60 * 2**20
        ),
    )(*operands.values())
    return (own.astype(f32) + mate.astype(f32)).astype(bf16)


def gather_inputs(tokens, weights, extra, inner):
    rows, half = tokens.shape
    gathered = lax.all_gather(tokens, ("inner", "tp"), axis=0)
    tp = gathered.shape[0] // inner
    whole = jnp.transpose(gathered.reshape(inner, tp, rows, half), (0, 2, 1, 3))
    whole = whole.reshape(inner * rows, tp * half)
    depth, columns = weights[0].shape
    width = columns // inner
    packed = jnp.stack([w.reshape(depth, inner, width) for w in weights], axis=2)
    packed = jnp.transpose(packed, (1, 0, 2, 3)).reshape(inner, depth, len(weights) * width)
    if inner > 1:
        packed = lax.all_to_all(packed, "inner", split_axis=0, concat_axis=0, tiled=True)
    pieces = lax.all_gather(packed.reshape(inner * depth, -1), "outer", axis=0, tiled=True)
    pieces = pieces.reshape(-1, len(weights), width).transpose(1, 0, 2)
    extras = lax.all_gather(extra, "inner", axis=0, tiled=True) if inner > 1 else extra
    return whole, pieces, extras.T


def local_state(keys, values, shifted, level, total, scale):
    weight = jnp.exp(shifted - level[:, None]) * scale
    weighted = keys.astype(jnp.float32) * weight[:, :, None]
    mat = jnp.einsum(
        "hsd,hse->hde", weighted.astype(jnp.bfloat16), values, preferred_element_type=jnp.float32
    )
    return mat, jnp.sum(weighted, axis=1), level + total, total


def packed_state(mat, vec, level, decay):
    spread = lambda x: jnp.broadcast_to(x[:, None], vec.shape)
    rows = parts_of(vec) + parts_of(spread(level)) + parts_of(spread(decay))
    pad = [jnp.zeros_like(rows[0])] * 7
    return jnp.concatenate([mat.astype(jnp.bfloat16), jnp.stack(rows + pad, axis=1)], axis=1)


def incoming(states, reverse):
    count = states.shape[0]
    mats = states[:, :, :HEAD]
    rows = states[:, :, HEAD:]
    vecs = whole_of(rows[:, :, 0], rows[:, :, 1], rows[:, :, 2])
    levels = whole_of(rows[:, :, 3, 0], rows[:, :, 4, 0], rows[:, :, 5, 0])
    decays = whole_of(rows[:, :, 6, 0], rows[:, :, 7, 0], rows[:, :, 8, 0])
    place = lax.axis_index("outer")
    order = jnp.arange(count)
    if reverse:
        ahead = (order > place)[:, None]
        between = (order[None, :] < order[:, None]) & (order[None, :] > place)
    else:
        ahead = (order < place)[:, None]
        between = (order[None, :] > order[:, None]) & (order[None, :] < place)
    lost = jnp.sum(jnp.where(between[:, :, None], decays[None], 0.0), axis=1)
    reach = jnp.where(ahead, levels + lost, -1e30)
    level = jnp.max(reach, axis=0)
    share = jnp.where(ahead, jnp.exp(reach - level[None]), 0.0)
    mat = jnp.sum(share[:, :, None, None] * mats.astype(jnp.float32), axis=0)
    vec = jnp.sum(share[:, :, None] * vecs, axis=0)
    return mat, vec, level


def finish(query_wide, num, den, running, decay, state):
    mat, vec, level = state
    top = jnp.maximum(running, level[:, None])
    local_weight = jnp.exp(running - top)
    carry_weight = jnp.exp(level[:, None] - top)
    num = local_weight[:, :, None] * num + carry_weight[:, :, None] * jnp.einsum(
        "htd,hde->hte", query_wide, mat, precision=PRECISE
    )
    den = local_weight * den + carry_weight * jnp.einsum(
        "htd,hd->ht", query_wide, vec, precision=PRECISE
    )
    return num / jnp.maximum(jnp.abs(den), jnp.exp(-top - decay))[:, :, None]


def make_shards(inner, outer, tp):
    def own(array, dim):
        size = array.shape[dim] // inner
        return lax.dynamic_slice_in_dim(array, lax.axis_index("inner") * size, size, dim)

    def shards(
        tokens,
        norm_gain,
        glu_value,
        glu_gate,
        conv_taps,
        ln_gain,
        ln_bias,
        query_weight,
        key_weight,
        value_weight,
        gate_weight,
        gate_bias,
        log_decay_extra,
        mem_gain,
        out_conv,
        out_mem,
    ):
        fits = tp == 2 and inner == 4 and outer == 2 * tp and inner * tp == MEMORY_HEADS
        if fits and tokens.shape[1] == inner * HEAD and conv_taps.shape[1] == inner * HEAD:
            return whole_layer(outer, inner, tp, types.SimpleNamespace(
                tokens=tokens, norm_gain=norm_gain, glu_value=glu_value, glu_gate=glu_gate,
                conv_taps=conv_taps, ln_gain=ln_gain, ln_bias=ln_bias, query_weight=query_weight,
                key_weight=key_weight, value_weight=value_weight, gate_weight=gate_weight,
                gate_bias=gate_bias, log_decay_extra=log_decay_extra, mem_gain=mem_gain,
                out_conv=out_conv, out_mem=out_mem,
            ))
        taps, gain, bias, mgain = own(conv_taps, 1), own(ln_gain, 0), own(ln_bias, 0), own(mem_gain, 0)
        channels = conv_taps.shape[1] * tp
        width = gain.shape[0]
        heads = mgain.shape[0] // HEAD
        first = (lax.axis_index("tp") * inner + lax.axis_index("inner")) * heads
        stacked = (query_weight, key_weight, value_weight, glu_value, glu_gate)
        whole, weights, extras = gather_inputs(tokens, stacked, log_decay_extra, inner)
        rows = whole.shape[0]
        wide = whole.astype(jnp.float32)
        normed = (
            wide * lax.rsqrt(jnp.mean(wide * wide, axis=-1, keepdims=True) + EPS) * norm_gain
        ).astype(jnp.bfloat16)
        own_gate = lax.dynamic_slice_in_dim(
            gate_weight.reshape(-1, 4, MEMORY_HEADS), first, heads, 2
        )
        own_bias = lax.dynamic_slice_in_dim(gate_bias.reshape(4, MEMORY_HEADS), first, heads, 1)
        gates = lax.dot_general(
            own_gate.reshape(-1, 4 * heads), normed, (((0,), (1,)), ((), ())),
            preferred_element_type=jnp.float32,
        ).reshape(4, heads, rows) + own_bias[:, :, None]
        own_extra = lax.dynamic_slice_in_dim(
            extras.reshape(2, MEMORY_HEADS, rows), first, heads, 1
        )
        lf = jax.nn.log_sigmoid(gates[1::2]) + own_extra
        at = jnp.arange(rows)
        causal = at[:, None] >= at[None, :]
        anti = at[:, None] <= at[None, :]

        def total(x, mask):
            return jnp.sum(jnp.where(mask, x[:, None, :], 0.0), axis=-1)

        def highest(x, mask):
            return jnp.max(jnp.where(mask, x[:, None, :], -jnp.inf), axis=-1)

        decay_f = total(lf[0], causal)
        decay_b = total(lf[1], anti)
        shifted_f = gates[0] - decay_f
        shifted_b = gates[2] - decay_b
        running_f = highest(shifted_f, causal)
        running_b = highest(shifted_b, anti)

        def project(i):
            return jnp.dot(normed, weights[i], preferred_element_type=jnp.float32)

        def heads_first(x):
            return jnp.transpose(x.reshape(rows, heads, HEAD), (1, 0, 2)).astype(jnp.bfloat16)

        keys = heads_first(project(1))
        values = heads_first(project(2))
        scale = HEAD ** (-0.5)
        state_f = local_state(
            keys, values, shifted_f, running_f[:, -1], decay_f[:, -1], scale
        )
        state_b = local_state(keys, values, shifted_b, running_b[:, 0], decay_b[:, 0], scale)
        sent = jnp.stack([packed_state(*state_f), packed_state(*state_b)])
        states = lax.all_gather(sent, "outer", axis=0)

        glu = (project(3) * jax.nn.sigmoid(project(4))).astype(jnp.bfloat16)
        reach = KW // 2
        before = lax.ppermute(glu[rows - reach :], "outer", [(i, i + 1) for i in range(outer - 1)])
        after = lax.ppermute(glu[:reach], "outer", [(i + 1, i) for i in range(outer - 1)])
        queries = heads_first(project(0))

        scores = jnp.einsum("htd,hsd->hts", queries, keys, preferred_element_type=jnp.float32) * scale

        def local_out(shifted, running, mask):
            weight = jnp.where(
                mask, jnp.exp(jnp.minimum(shifted[:, None, :] - running[:, :, None], 0.0)), 0.0
            )
            part = scores * weight
            num = jnp.einsum(
                "hts,hse->hte", part.astype(jnp.bfloat16), values,
                preferred_element_type=jnp.float32,
            )
            return num, jnp.sum(part, axis=-1)

        num_f, den_f = local_out(shifted_f, running_f, causal)
        num_b, den_b = local_out(shifted_b, running_b, anti)

        padded = jnp.concatenate([before, glu, after], axis=0).astype(jnp.float32)
        conv = jnp.zeros(glu.shape, jnp.float32)
        for offset in range(KW):
            conv = conv + taps[offset] * padded[offset : offset + rows]
        sums = jnp.stack([jnp.sum(conv, axis=-1), jnp.sum(conv * conv, axis=-1)])
        sums = lax.psum(sums, ("inner", "tp")) / channels
        chan_mean = sums[0]
        chan_var = sums[1] - chan_mean * chan_mean
        normal = (conv - chan_mean[:, None]) * lax.rsqrt(chan_var + EPS)[:, None] * gain + bias
        act = (normal * jax.nn.sigmoid(normal)).astype(jnp.bfloat16)

        query_wide = queries.astype(jnp.float32)
        forward = finish(query_wide, num_f, den_f, running_f, decay_f, incoming(states[:, 0], False))
        backward = finish(query_wide, num_b, den_b, running_b, decay_b, incoming(states[:, 1], True))
        summed = forward + backward
        head_norm = summed * lax.rsqrt(jnp.mean(summed * summed, axis=-1, keepdims=True) + EPS)
        head_norm = head_norm * mgain.reshape(heads, HEAD)[:, None, :]
        memory = jnp.transpose(head_norm, (1, 0, 2)).reshape(rows, heads * HEAD).astype(jnp.bfloat16)

        def back(x):
            if inner == 1:
                return x
            return lax.all_to_all(x, "inner", split_axis=0, concat_axis=1, tiled=True)

        result = jnp.dot(back(act), out_conv, preferred_element_type=jnp.float32)
        result = result + jnp.dot(back(memory), out_mem, preferred_element_type=jnp.float32)
        return lax.psum_scatter(
            result.astype(jnp.bfloat16), "tp", scatter_dimension=0, tiled=True
        )

    return shards


def solution(mesh):
    sp, tp = mesh.shape["sp"], mesh.shape["tp"]
    inner = math.gcd(sp, max(MEMORY_HEADS // tp, 1))
    outer = sp // inner
    fine = Mesh(mesh.devices.reshape(outer, inner, tp), ("outer", "inner", "tp"))
    rows = ("outer", "inner")
    in_specs = (
        P(rows, "tp"),
        P(),
        P(rows, "tp"),
        P(rows, "tp"),
        P(None, "tp"),
        P("tp"),
        P("tp"),
        P(rows, "tp"),
        P(rows, "tp"),
        P(rows, "tp"),
        P(),
        P(),
        P(rows, None),
        P("tp"),
        P("tp", None),
        P("tp", None),
    )
    return jax.shard_map(
        make_shards(inner, outer, tp), mesh=fine, in_specs=in_specs,
        out_specs=P(("outer", "inner", "tp"), None), check_vma=False,
    )
```
